32 devices in a mesh: sp: 8 (over z, y), tp: 4 (over x, core).
Axes of the slice: x: 2, y: 2, z: 4, core: 2. Of those that a mesh axis runs over, the one named last changes fastest.
Arguments:
- query_rows: bfloat16 [2048, 2048], P('sp', 'tp'), may hold values from -5.5 to 5.5
- key_rows: bfloat16 [2048, 2048], P('sp', 'tp'), may hold values from -5.5 to 5.5
- value_rows: bfloat16 [2048, 2048], P('sp', 'tp'), may hold values from -6 to 6
- out_grad: bfloat16 [2048, 2048], P('sp', 'tp'), may hold values from -96 to 96
- rel_bias: float32 [256, 32], replicated, may hold values from -3 to 3
Outputs:
- query_grad: bfloat16 [2048, 2048], P('sp', 'tp')
- key_grad: bfloat16 [2048, 2048], P('sp', 'tp')
- value_grad: bfloat16 [2048, 2048], P('sp', 'tp')
- table_grad: float32 [256, 32], P('sp')
The draws below stay inside these ranges and needn't reach their ends.
All inputs are finite; a program needn't handle non-finite values.
Results may differ from the reference program's by a relative error of at most 0.007.
Values may be sent and summed in bfloat16 or wider, within the bound.
A program may use at most 64 MiB of HBM per device.

```python
import jax
import jax.numpy as jnp
from jax import lax

HEADS = 32
HEAD_DIM = 64
SEG = 64
LEFT = 4
CLIP = 128
TOKENS = 2048
TABLE = 256


def drawn_pair(key):
    key_queries, key_keys = jax.random.split(jax.random.fold_in(key, 11), 2)
    width_all = HEADS * HEAD_DIM
    query_draw = jnp.clip(jax.random.normal(key_queries, (TOKENS, width_all), jnp.float32), -5.5, 5.5)
    key_draw = jnp.clip(jax.random.normal(key_keys, (TOKENS, width_all), jnp.float32), -5.5, 5.5)
    return (query_draw, key_draw)


def draw_query_rows(key, part):
    return drawn_pair(key)[0].astype(jnp.bfloat16)


def draw_key_rows(key, part):
    return drawn_pair(key)[1].astype(jnp.bfloat16)


def steps_of(rng, shape, shards, low, top_value):
    def one(dim, shards_of):
        draws = jax.random.uniform(jax.random.fold_in(jax.random.fold_in(rng, 6), dim), (shards_of,), jnp.float32, low / len(shards), top_value / len(shards))
        return jnp.repeat(jnp.exp(draws), shape[dim] // shards_of).reshape((-1,) + (1,) * (len(shape) - dim - 1))

    loudness = one(*shards[0])
    for cut in shards[1:]:
        loudness = loudness * one(*cut)
    return loudness


def gaussian(rng, dims, width, limit, pieces=(), kind=jnp.bfloat16):
    factor_of = steps_of(rng, dims, pieces, -0.22, 0.18) if pieces else 1.0
    drawn = jax.random.normal(rng, dims, jnp.float32) * width * factor_of
    return jnp.minimum(jnp.maximum(drawn, -limit), limit).astype(kind)


def setup_inputs(seed: int = 0) -> dict:
    key_of = jax.random.split(jax.random.key(seed), 6)
    return {
        "query_rows": draw_query_rows(jax.random.fold_in(key_of[5], 71), 0),
        "key_rows": draw_key_rows(jax.random.fold_in(key_of[5], 71), 0),
        "value_rows": gaussian(key_of[2], (TOKENS, HEADS * HEAD_DIM), 1.0, 6.0, ((0, 8), (1, 4))),
        "out_grad": gaussian(key_of[3], (TOKENS, HEADS * HEAD_DIM), 16.0, 96.0, ((0, 8), (1, 4))),
        "rel_bias": gaussian(key_of[4], (TABLE, HEADS), 0.5, 3.0, (), jnp.float32),
    }


NEG_FILL = -1e30


def banded(extended, seg_count, seg_len, band_len):
    layers = []
    for offset in range(band_len // seg_len):
        window = lax.slice_in_dim(extended, offset * seg_len, offset * seg_len + seg_count * seg_len, axis=0)
        layers.append(window.reshape((seg_count, 1, seg_len) + extended.shape[1:]))
    return jnp.concatenate(layers, axis=1).reshape((seg_count, band_len) + extended.shape[1:])


def unbanded(band_grads, ext_len, seg_len):
    seg_count, band_len = band_grads.shape[0], band_grads.shape[1]
    trailing = band_grads.shape[2:]
    blocks = band_grads.reshape((seg_count, band_len // seg_len, seg_len) + trailing)
    summed = jnp.zeros((ext_len,) + trailing, band_grads.dtype)
    for offset in range(band_len // seg_len):
        stripe = blocks[:, offset].reshape((seg_count * seg_len,) + trailing)
        widths = [(offset * seg_len, ext_len - offset * seg_len - seg_count * seg_len)] + [(0, 0)] * len(trailing)
        summed = summed + jnp.pad(stripe, widths)
    return summed


def head_backward(inputs):
    query_head, key_head, value_head, dout_head, table_col = inputs
    reach_rows = LEFT * SEG
    band_len = reach_rows + SEG
    seg_count = TOKENS // SEG
    score_scale = HEAD_DIM ** -0.5
    key_ext = jnp.pad(key_head.astype(jnp.float32), ((reach_rows, 0), (0, 0)))
    value_ext = jnp.pad(value_head.astype(jnp.float32), ((reach_rows, 0), (0, 0)))
    key_valid = jnp.arange(reach_rows + TOKENS, dtype=jnp.int32) >= reach_rows
    key_band = banded(key_ext, seg_count, SEG, band_len)
    value_band = banded(value_ext, seg_count, SEG, band_len)
    valid_band = banded(key_valid, seg_count, SEG, band_len)
    query_segs = query_head.astype(jnp.float32).reshape(seg_count, SEG, HEAD_DIM)
    dout_segs = dout_head.astype(jnp.float32).reshape(seg_count, SEG, HEAD_DIM)
    row_pos = jnp.arange(SEG, dtype=jnp.int32)[:, None]
    col_pos = jnp.arange(band_len, dtype=jnp.int32)[None, :]
    offset_index = jnp.clip(reach_rows + row_pos - col_pos, -CLIP, CLIP - 1) + CLIP
    bias_band = table_col[offset_index]
    scores = jnp.einsum('jid,jcd->jic', query_segs, key_band) * score_scale + bias_band[None]
    scores = jnp.where(valid_band[:, None, :], scores, NEG_FILL)
    row_peak = jnp.max(scores, axis=-1)
    log_norm = row_peak + jnp.log(jnp.sum(jnp.exp(scores - row_peak[..., None]), axis=-1))
    attention = jnp.exp(scores - log_norm[..., None])
    attention_half = lax.optimization_barrier(attention.astype(jnp.bfloat16)).astype(jnp.float32)
    attention_grad = jnp.einsum('jie,jce->jic', dout_segs, value_band)
    inner_sums = jnp.sum(attention * attention_grad, axis=-1)
    dscores = attention * (attention_grad - inner_sums[..., None])
    dscore_half = lax.optimization_barrier(dscores.astype(jnp.bfloat16)).astype(jnp.float32)
    dquery = (jnp.einsum('jic,jcd->jid', dscore_half, key_band) * score_scale).reshape(TOKENS, HEAD_DIM)
    dkey_band = jnp.einsum('jic,jid->jcd', dscore_half, query_segs) * score_scale
    dvalue_band = jnp.einsum('jic,jie->jce', attention_half, dout_segs)
    key_grad_rows = unbanded(dkey_band, reach_rows + TOKENS, SEG)[reach_rows:]
    value_grad_rows = unbanded(dvalue_band, reach_rows + TOKENS, SEG)[reach_rows:]
    table_col_grad = jax.ops.segment_sum(jnp.sum(dscores, axis=0).reshape(-1), offset_index.reshape(-1), num_segments=2 * CLIP)
    return dquery.astype(jnp.bfloat16), key_grad_rows.astype(jnp.bfloat16), value_grad_rows.astype(jnp.bfloat16), table_col_grad


def split_heads(row_block):
    return jnp.transpose(row_block.reshape(TOKENS, HEADS, HEAD_DIM), (1, 0, 2))


def join_heads(stacked):
    return jnp.transpose(stacked, (1, 0, 2)).reshape(TOKENS, HEADS * HEAD_DIM)


def reference(query_rows, key_rows, value_rows, out_grad, rel_bias):
    results = lax.map(head_backward, (split_heads(query_rows), split_heads(key_rows), split_heads(value_rows), split_heads(out_grad), jnp.transpose(rel_bias)))
    return (join_heads(results[0]), join_heads(results[1]), join_heads(results[2]), jnp.transpose(results[3]))
```

```python
from functools import partial
import math

import jax
import jax.numpy as jnp
from jax import lax
from jax.experimental import pallas as pl
from jax.experimental.pallas import tpu as pltpu
from jax.sharding import PartitionSpec as P

HEAD_DIM = 64
SEG = 64
LEFT = 4
CLIP = 128

LANES = 2 * HEAD_DIM
REACH = LEFT * SEG
BLK = 2 * SEG
BAND = REACH + BLK
WRAP = 3 * BLK
NEG_FILL = -1e30
LOG2E = math.log2(math.e)
MESH = pl.DeviceIdType.MESH
F32 = jnp.float32
BF16 = jnp.bfloat16

NT = (((1,), (1,)), ((), ()))
NN = (((1,), (0,)), ((), ()))
TN = (((0,), (0,)), ((), ()))


def dot(a, b, dims):
    return lax.dot_general(a, b, dims, preferred_element_type=F32)


def turned(x, amount):
    amount %= x.shape[1]
    return pltpu.roll(x, amount, 1) if amount else x


def row_turned(x, sign):
    row = lax.broadcasted_iota(jnp.int32, x.shape, 0)
    for bit in (1, 2, 4):
        x = jnp.where((row & bit) != 0, turned(x, sign * bit), x)
    return x


def build_bias(table_row, bias_ref, pair, lane):
    last = table_row[:, 2 * CLIP - 1 :]
    flat = jnp.broadcast_to(last, (1, BLK))
    shape = (8, BLK)
    line = jnp.concatenate([table_row[:, CLIP:], flat, table_row[:, :CLIP]], axis=1)
    base = row_turned(jnp.broadcast_to(line, (8, WRAP)), 1)
    query = lax.broadcasted_iota(jnp.int32, shape, 1)
    cols = pl.ds(lane * BLK, BLK)
    flat8 = jnp.broadcast_to(last, shape)
    for group in range(BAND // 8):
        row = group * 8
        if row < BLK:
            tile = flat8
        else:
            sheared = turned(base, row % BLK)
            tile = sheared[:, BLK : 2 * BLK] if row < 2 * BLK else sheared[:, :BLK]
        if row < SEG:
            tile = jnp.where(query >= SEG, NEG_FILL, tile)
        if row >= BAND - SEG:
            tile = jnp.where(query < SEG, NEG_FILL, tile)
        bias_ref[pair, pl.ds(row, 8), cols] = tile


def diagonals(square):
    parts = []
    for group in range(BLK // 8):
        near = square[2 * BLK + group * 8 : 2 * BLK + group * 8 + 8]
        far = square[BLK + group * 8 : BLK + group * 8 + 8]
        parts.append(jnp.concatenate([near, far, jnp.zeros_like(near)], axis=1))
    step = 8
    while len(parts) > 1:
        parts = [a + turned(b, -step) for a, b in zip(parts[::2], parts[1::2])]
        step *= 2
    sums = jnp.sum(row_turned(parts[0], -1), axis=0, keepdims=True)
    return sums, jnp.sum(square[:BLK], axis=0, keepdims=True)


def kernel(
    sp_size, tp_size, moved,
    q_hbm, k_hbm, v_hbm, d_hbm, table_hbm,
    dq_ref, dk_ref, dv_ref, dt_ref,
    qd, kv, bias_ref, square_ref, grown_ref, dprob_ref, peak_ref,
    own_k, own_v, own_q, back_q, got_q, back_kv, got_kv,
    local_stats, right_stats, halo_stats, left_stats,
    table_rows, pieces, piece_got, shares,
    load_sem, hop_sem, send_sem, seq_recv, back_recv, halo_recv, misc_recv,
):
    rows, width = q_hbm.shape
    pairs = width // LANES
    heads = width // HEAD_DIM
    part = 2 * CLIP // sp_size
    me = lax.axis_index("sp")
    col = lax.axis_index("tp")
    has_left = me > 0
    has_right = me < sp_size - 1
    left = jnp.maximum(me - 1, 0)
    right = jnp.minimum(me + 1, sp_size - 1)
    first, second = pl.ds(0, rows), pl.ds(rows, rows)

    pltpu.make_async_copy(q_hbm, qd.at[0, first], load_sem.at[0]).start()
    pltpu.make_async_copy(d_hbm, qd.at[1, first], load_sem.at[0]).start()
    pltpu.make_async_copy(table_hbm, table_rows, load_sem.at[2]).start()
    pltpu.make_async_copy(k_hbm, kv.at[0, second], load_sem.at[1]).start()
    pltpu.make_async_copy(v_hbm, kv.at[1, second], load_sem.at[1]).start()

    barrier = pltpu.get_barrier_semaphore()

    def greet(sem, step):
        @pl.when(me >= step)
        def _():
            pl.semaphore_signal(sem, inc=1, device_id=(me - step, col), device_id_type=MESH)

        @pl.when(me + step < sp_size)
        def _():
            pl.semaphore_signal(sem, inc=1, device_id=(me + step, col), device_id_type=MESH)

    def greeters(step):
        return (me >= step).astype(jnp.int32) + (me + step < sp_size).astype(jnp.int32)

    greet(barrier, 1)
    for k in range(1, tp_size):
        pl.semaphore_signal(
            barrier, inc=1, device_id=(me, lax.rem(col + k, tp_size)), device_id_type=MESH
        )

    rounds = hop_sem.shape[0]

    def hop(r):
        if 0 < r <= rounds:
            pl.semaphore_wait(hop_sem.at[r - 1], greeters(1 << (r - 1)))
        if r < rounds:
            greet(hop_sem.at[r], 1 << r)

    def remote(src, dst, send, recv, target):
        return pltpu.make_async_remote_copy(
            src_ref=src,
            dst_ref=dst,
            send_sem=send_sem.at[send],
            recv_sem=recv,
            device_id=(target, col),
            device_id_type=MESH,
        )

    def query_copy(start, count):
        cols = pl.ds(start * LANES, count * LANES)
        return remote(
            qd.at[:, first, cols], qd.at[:, second, cols], 0, seq_recv.at[start], left
        )

    def key_copy(p, block):
        cols = pl.ds(p * LANES, LANES)
        return remote(
            kv.at[:, pl.ds(rows + block * BLK, BLK), cols],
            kv.at[:, pl.ds(block * BLK, BLK), cols],
            1,
            seq_recv.at[p + block * (pairs - moved)],
            right,
        )

    def all_keys():
        cols = pl.ds(moved * LANES, width - moved * LANES)
        return remote(kv.at[:, second, cols], kv.at[:, first, cols], 1, misc_recv.at[0], right)

    def local_copy():
        return remote(local_stats, right_stats, 2, misc_recv.at[0], left)

    def halo_copy(p):
        return remote(halo_stats.at[p], left_stats.at[p], 3, halo_recv.at[p], right)

    def back_copy(p):
        return remote(back_q.at[p], got_q.at[p], 4, back_recv.at[p], right)

    def key_back_copy(p):
        i = p - moved
        return remote(back_kv.at[i], got_kv.at[i], 5, back_recv.at[p], left)

    def send_pair(p):
        if p < moved:
            @pl.when(has_left)
            def _():
                query_copy(p, 1).start()
        elif p < pairs:
            @pl.when(has_right)
            def _():
                for block in (1, 0):
                    key_copy(p, block).start()

    def send_back(p):
        if p < moved:
            @pl.when(has_right)
            def _():
                back_copy(p).start()
        else:
            @pl.when(has_left)
            def _():
                key_back_copy(p).start()

    def load_wait(refs, sem):
        pltpu.make_async_copy(refs, refs, sem).wait()

    pl.semaphore_wait(barrier, greeters(1) + tp_size - 1)
    load_wait(qd.at[:, first], load_sem.at[0])
    send_pair(0)
    hop(0)

    @pl.when(jnp.logical_not(has_left))
    def _():
        spot = lax.broadcasted_iota(jnp.int32, left_stats.shape, 1)
        left_stats[...] = jnp.where((spot & 2) == 0, NEG_FILL, 0.0)
        keys = pl.ds(moved * LANES, width - moved * LANES)
        kv[:, first, keys] = jnp.zeros((2, rows, width - moved * LANES), BF16)

    load_wait(table_rows, load_sem.at[2])
    for h in range(heads):
        row = table_rows[pl.ds(col * heads + h, 1), :] * LOG2E
        build_bias(row, bias_ref, h // 2, h % 2)

    load_wait(kv.at[:, second], load_sem.at[1])

    low = lax.broadcasted_iota(jnp.int32, (BLK, LANES), 1) < HEAD_DIM
    scale = HEAD_DIM ** -0.5
    sums, tops = {}, {}

    def split(x):
        zero = jnp.zeros_like(x)
        return jnp.concatenate([jnp.where(low, x, zero), jnp.where(low, zero, x)], axis=0)

    def queries(p, mine):
        cols = pl.ds(p * LANES, LANES)
        return split(qd[0, mine, cols] * jnp.asarray(scale, BF16)), split(qd[1, mine, cols])

    def tile(p, half, halo):
        cols = pl.ds(p * LANES, LANES)
        mine = pl.ds(half * BLK + (rows if halo else 0), BLK)
        start, size, row = (
            (half * BLK, REACH - half * BLK, 0)
            if halo
            else (0, (half + 1) * BLK, REACH - half * BLK)
        )
        keys = pl.ds(rows + start, size)
        return kv[0, keys, cols], kv[1, keys, cols], *queries(p, mine), pl.ds(row, size)

    def put(stats, p, half, which, value):
        for lane in range(2):
            spot = pl.ds(half * 4 + which * 2 + lane, 1)
            stats[p, spot, :] = value[:, lane * BLK : (lane + 1) * BLK]

    def get(stats, p, half, which):
        spots = [pl.ds(half * 4 + which * 2 + lane, 1) for lane in range(2)]
        return jnp.concatenate([stats[p, spot, :] for spot in spots], axis=1)

    def partial_softmax(p, half, halo, stats):
        k_blk, v_blk, qq, dd, band = tile(p, half, halo)
        scores = dot(k_blk, qq, NT) * LOG2E + bias_ref[p, band]
        dprobs = dot(v_blk, dd, NT)
        peak = jnp.max(scores, axis=0, keepdims=True)
        grown = jnp.exp2(scores - peak)
        total = jnp.sum(grown, axis=0, keepdims=True)
        put(stats, p, half, 0, peak + jnp.log2(total))
        put(stats, p, half, 1, jnp.sum(grown * dprobs, axis=0, keepdims=True) / total)
        return grown, dprobs, peak

    def products(k_blk, qq, dd, probs, dscores):
        ds_half = dscores.astype(BF16)
        flat = dot(k_blk, ds_half, TN)
        both = jnp.concatenate([flat[:HEAD_DIM, :BLK], flat[HEAD_DIM:, BLK:]], axis=0)
        return (
            dot(ds_half, qq, NN),
            dot(probs.astype(BF16), dd, NN),
            jnp.transpose(both) * scale,
        )

    def tile_probs(p, half, grown, dprobs, peak, stats, others):
        n1, i1 = get(stats, p, half, 0), get(stats, p, half, 1)
        n2, i2 = get(others, p, half, 0), get(others, p, half, 1)
        top = jnp.maximum(n1, n2)
        a1, a2 = jnp.exp2(n1 - top), jnp.exp2(n2 - top)
        inverse = 1.0 / (a1 + a2)
        inner = (i1 * a1 + i2 * a2) * inverse
        probs = grown * (jnp.exp2(peak - top) * inverse)
        return probs, probs * (dprobs - inner)

    def tile_grads(p, half, halo, probs, dscores):
        k_blk, _, qq, dd, _ = tile(p, half, halo)
        return products(k_blk, qq, dd, probs, dscores)

    places = (pl.ds(0, BLK), pl.ds(BLK, 2 * BLK))
    for p in range(moved):
        for half in range(2):
            grown, dprobs, peak = partial_softmax(p, half, False, local_stats)
            grown_ref[p, places[half], :] = grown
            dprob_ref[p, places[half], :] = dprobs
            peak_ref[p, pl.ds(half, 1), :] = peak

    @pl.when(has_left)
    def _():
        local_copy().start()

    send_pair(1)

    def after_stats(p):
        send_pair(p + 2)
        if p == moved - 1:
            for rest in range(p + 3, pairs):
                send_pair(rest)

    def halo(p):
        @pl.when(has_right)
        def _():
            query_copy(p, 1).wait_recv()
            kept = [partial_softmax(p, half, True, halo_stats) for half in range(2)]
            halo_copy(p).start()
            after_stats(p)
            if p == 0:
                local_copy().wait_recv()
            (p0, s0), (p1, s1) = (
                tile_probs(p, half, *kept[half], halo_stats, right_stats) for half in range(2)
            )
            k0, v0, q0 = tile_grads(p, 0, True, p0, s0)
            k1, v1, q1 = tile_grads(p, 1, True, p1, s1)
            for ref, a, b in ((own_k, k0, k1), (own_v, v0, v1)):
                ref[p, :BLK, :] = a[:BLK]
                ref[p, BLK:, :] = a[BLK:] + b
            back_q[p, :BLK, :] = q0.astype(BF16)
            back_q[p, BLK:, :] = q1.astype(BF16)
            square_ref[p, :BLK, :] = s0[:BLK] + s1
            square_ref[p, BLK:REACH, :] = s0[BLK:]

        @pl.when(jnp.logical_not(has_right))
        def _():
            after_stats(p)
            own_k[p] = jnp.zeros((rows, LANES), F32)
            own_v[p] = jnp.zeros((rows, LANES), F32)
            square_ref[p, :REACH, :] = jnp.zeros((REACH, 2 * BLK), F32)

        hop(p + 1)

    def tally(p, square):
        for lane in range(2):
            sums[2 * p + lane], tops[2 * p + lane] = diagonals(
                square[:, lane * BLK : (lane + 1) * BLK]
            )

    def local(p, between=None):
        cols = pl.ds(p * LANES, LANES)

        @pl.when(has_left)
        def _():
            halo_copy(p).wait_recv()

        (p0, s0), (p1, s1) = (
            tile_probs(
                p, half,
                grown_ref[p, places[half], :], dprob_ref[p, places[half], :],
                peak_ref[p, pl.ds(half, 1), :],
                local_stats, left_stats,
            )
            for half in range(2)
        )
        square = jnp.concatenate(
            [
                square_ref[p, :BLK, :],
                square_ref[p, BLK:REACH, :] + s1[:BLK],
                s0 + s1[BLK:],
            ],
            axis=0,
        )
        tally(p, square)
        if between is not None:
            between()
        k0, v0, q0 = tile_grads(p, 0, False, p0, s0)
        k1, v1, q1 = tile_grads(p, 1, False, p1, s1)
        for out, ref, a, b in ((dk_ref, own_k, k0, k1), (dv_ref, own_v, v0, v1)):
            out[:BLK, cols] = (ref[p, :BLK, :] + a + b[:BLK]).astype(BF16)
            out[BLK:, cols] = (ref[p, BLK:, :] + b[BLK:]).astype(BF16)
        own_q[p, :BLK, :] = q0
        own_q[p, BLK:, :] = q1

    gate = jnp.where(has_left, 0.0, NEG_FILL)

    def full(p, between=None):
        cols = pl.ds(p * LANES, LANES)
        i = p - moved

        def half_probs(half):
            @pl.when(has_left)
            def _():
                key_copy(p, half).wait_recv()

            keys = pl.ds(half * BLK, BAND)
            qq, dd = queries(p, pl.ds(half * BLK, BLK))
            scores = dot(kv[0, keys, cols], qq, NT) * LOG2E + bias_ref[p]
            before = REACH - half * BLK
            scores = jnp.concatenate([scores[:before] + gate, scores[before:]], axis=0)
            dprobs = dot(kv[1, keys, cols], dd, NT)
            peak = jnp.max(scores, axis=0, keepdims=True)
            grown = jnp.exp2(scores - peak)
            inverse = 1.0 / jnp.sum(grown, axis=0, keepdims=True)
            inner = jnp.sum(grown * dprobs, axis=0, keepdims=True) * inverse
            probs = grown * inverse
            return probs, probs * (dprobs - inner)

        def half_grads(half, probs, dscores):
            qq, dd = queries(p, pl.ds(half * BLK, BLK))
            return products(kv[0, pl.ds(half * BLK, BAND), cols], qq, dd, probs, dscores)

        p1, s1 = half_probs(1)
        k1, v1, q1 = half_grads(1, p1, s1)
        p0, s0 = half_probs(0)
        tally(p, s0 + s1)
        if between is not None:
            between()
        k0, v0, q0 = half_grads(0, p0, s0)
        for which, ref, a, b in ((0, own_k, k0, k1), (1, own_v, v0, v1)):
            back_kv[i, which, :BLK, :] = a[:BLK].astype(BF16)
            back_kv[i, which, BLK:, :] = (a[BLK:REACH] + b[:BLK]).astype(BF16)
            ref[p, :BLK, :] = a[REACH:] + b[BLK:REACH]
            ref[p, BLK:, :] = b[REACH:]
        dq_ref[:BLK, cols] = q0.astype(BF16)
        dq_ref[BLK:, cols] = q1.astype(BF16)

    def piece_copy(k):
        target = lax.rem(me + k, sp_size)
        return remote(
            pieces.at[target * part // CLIP], piece_got.at[k - 1], 6, misc_recv.at[1], target
        )

    def all_pieces():
        return remote(piece_got, piece_got, 6, misc_recv.at[1], left)

    def share_copy(k):
        return pltpu.make_async_remote_copy(
            src_ref=shares.at[0],
            dst_ref=shares.at[k],
            send_sem=send_sem.at[7],
            recv_sem=misc_recv.at[2],
            device_id=(me, lax.rem(col + k, tp_size)),
            device_id_type=MESH,
        )

    def all_shares():
        rest = shares.at[pl.ds(1, tp_size - 1)]
        return remote(rest, rest, 7, misc_recv.at[2], left)

    def send_pieces():
        for r in range(moved + 1, rounds + 1):
            hop(r)
        y = jnp.concatenate([sums[h] for h in range(heads)], axis=0)
        beyond = jnp.sum(
            y[:, BLK : 2 * BLK] + jnp.concatenate([tops[h] for h in range(heads)], axis=0),
            axis=1, keepdims=True,
        )
        spot = lax.broadcasted_iota(jnp.int32, (heads, BLK), 1)
        pieces[0] = y[:, 2 * BLK :]
        pieces[1] = y[:, :BLK] + jnp.where(spot == BLK - 1, beyond, 0.0)
        for k in range(1, sp_size):
            piece_copy(k).start()
        for p in range(pairs - 1):
            send_back(p)

    for p in range(moved):
        halo(p)
        if p:
            local(p - 1)
    last = pairs - 1
    for p in range(moved, last):
        full(p)
        if p == moved:
            local(moved - 1)
    if moved < last:
        full(last, send_pieces)
    else:
        full(last, lambda: local(moved - 1, send_pieces))
    send_back(last)

    all_pieces().wait_recv()
    total = pieces[me * part // CLIP]
    for k in range(1, sp_size):
        total = total + piece_got[k - 1]
    shares[0] = pltpu.roll(total, lax.rem(CLIP - lax.rem(me * part, CLIP), CLIP), 1)
    for k in range(1, tp_size):
        share_copy(k).start()

    def finish(p):
        cols = pl.ds(p * LANES, LANES)
        if p < moved:
            @pl.when(has_left)
            def _():
                back_copy(p).wait_recv()
                dq_ref[:, cols] = (own_q[p] + got_q[p].astype(F32)).astype(BF16)

            @pl.when(jnp.logical_not(has_left))
            def _():
                dq_ref[:, cols] = own_q[p].astype(BF16)
        else:
            i = p - moved

            @pl.when(has_right)
            def _():
                key_back_copy(p).wait_recv()
                dk_ref[:, cols] = (own_k[p] + got_kv[i, 0].astype(F32)).astype(BF16)
                dv_ref[:, cols] = (own_v[p] + got_kv[i, 1].astype(F32)).astype(BF16)

            @pl.when(jnp.logical_not(has_right))
            def _():
                dk_ref[:, cols] = own_k[p].astype(BF16)
                dv_ref[:, cols] = own_v[p].astype(BF16)

    for p in range(pairs):
        finish(p)
    all_shares().wait_recv()
    stacked = jnp.concatenate(
        [shares[lax.rem(col + tp_size - t, tp_size)] for t in range(tp_size)], axis=0
    )
    dt_ref[...] = jnp.transpose(stacked)[:part]

    all_pieces().wait_send()
    all_shares().wait_send()

    @pl.when(has_left)
    def _():
        query_copy(0, moved).wait_send()
        local_copy().wait_send()
        remote(back_kv, got_kv, 5, misc_recv.at[0], left).wait_send()

    @pl.when(has_right)
    def _():
        all_keys().wait_send()
        remote(halo_stats, left_stats, 3, misc_recv.at[0], right).wait_send()
        remote(back_q, got_q, 4, misc_recv.at[0], right).wait_send()


def shards(sp_size, tp_size, query_rows, key_rows, value_rows, out_grad, rel_bias):
    rows, width = query_rows.shape
    pairs = width // LANES
    heads = width // HEAD_DIM
    part = 2 * CLIP // sp_size
    moved = pairs - 1
    rounds = max(sp_size - 2, 0).bit_length()
    assert rows == REACH and REACH == 2 * BLK and CLIP == BLK
    like = jax.ShapeDtypeStruct((rows, width), BF16)
    dma = pltpu.SemaphoreType.DMA
    shapes = (like, like, like, jax.ShapeDtypeStruct((part, heads * tp_size), F32))
    results = pl.pallas_call(
        partial(kernel, sp_size, tp_size, moved),
        out_shape=shapes,
        in_specs=[pl.BlockSpec(memory_space=pltpu.HBM)] * 5,
        out_specs=tuple([pl.BlockSpec(memory_space=pltpu.VMEM)] * 4),
        scratch_shapes=[
            pltpu.VMEM((2, 2 * rows, width), BF16),
            pltpu.VMEM((2, 2 * rows, width), BF16),
            pltpu.VMEM((pairs, BAND, 2 * BLK), F32),
            pltpu.VMEM((moved, REACH, 2 * BLK), F32),
            pltpu.VMEM((moved, BAND, 2 * BLK), F32),
            pltpu.VMEM((moved, BAND, 2 * BLK), F32),
            pltpu.VMEM((moved, 8, 2 * BLK), F32),
            pltpu.VMEM((pairs, rows, LANES), F32),
            pltpu.VMEM((pairs, rows, LANES), F32),
            pltpu.VMEM((moved, rows, LANES), F32),
            pltpu.VMEM((moved, rows, LANES), BF16),
            pltpu.VMEM((moved, rows, LANES), BF16),
            pltpu.VMEM((pairs - moved, 2, rows, LANES), BF16),
            pltpu.VMEM((pairs - moved, 2, rows, LANES), BF16),
            pltpu.VMEM((moved, 8, BLK), F32),
            pltpu.VMEM((moved, 8, BLK), F32),
            pltpu.VMEM((moved, 8, BLK), F32),
            pltpu.VMEM((moved, 8, BLK), F32),
            pltpu.VMEM(rel_bias.shape[::-1], F32),
            pltpu.VMEM((2, heads, BLK), F32),
            pltpu.VMEM((sp_size - 1, heads, BLK), F32),
            pltpu.VMEM((tp_size, heads, BLK), F32),
            dma((3,)),
            pltpu.SemaphoreType.REGULAR((rounds,)),
            dma((8,)),
            dma((2 * pairs - moved,)),
            dma((pairs,)),
            dma((moved,)),
            dma((3,)),
        ],
        compiler_params=pltpu.CompilerParams(
            collective_id=0, has_side_effects=True, vmem_limit_bytes=48 * 1024 * 1024
        ),
    )(*[pltpu.with_memory_space_constraint(x, pltpu.HBM) for x in (query_rows, key_rows, value_rows, out_grad, jnp.transpose(rel_bias))])
    return pl.pallas_call(
        write_out,
        out_shape=shapes,
        in_specs=[pl.BlockSpec(memory_space=pl.ANY)] * 4,
        out_specs=tuple([pl.BlockSpec(memory_space=pltpu.HBM)] * 4),
        scratch_shapes=[dma((4,))],
        compiler_params=pltpu.CompilerParams(vmem_limit_bytes=1024 * 1024),
    )(*results)


def write_out(*refs):
    sem = refs[-1]
    copies = [pltpu.make_async_copy(refs[i], refs[4 + i], sem.at[i]) for i in range(4)]
    for copy in copies:
        copy.start()
    for copy in copies:
        copy.wait()


def solution(mesh):
    return jax.shard_map(
        partial(shards, mesh.shape["sp"], mesh.shape["tp"]),
        mesh=mesh,
        in_specs=(P("sp", "tp"), P("sp", "tp"), P("sp", "tp"), P("sp", "tp"), P()),
        out_specs=(P("sp", "tp"), P("sp", "tp"), P("sp", "tp"), P("sp", None)),
        check_vma=False,
    )
```

```python
from functools import partial
import math

import jax
import jax.numpy as jnp
from jax import lax
from jax.experimental import pallas as pl
from jax.experimental.pallas import tpu as pltpu
from jax.sharding import PartitionSpec as P

HEAD_DIM = 64
SEG = 64
LEFT = 4
CLIP = 128

LANES = 2 * HEAD_DIM
REACH = LEFT * SEG
BLK = 2 * SEG
BAND = REACH + BLK
WRAP = 3 * BLK
NEG_FILL = -1e30
LOG2E = math.log2(math.e)
MESH = pl.DeviceIdType.MESH
F32 = jnp.float32
BF16 = jnp.bfloat16

NT = (((1,), (1,)), ((), ()))
NN = (((1,), (0,)), ((), ()))
TN = (((0,), (0,)), ((), ()))


def dot(a, b, dims):
    return lax.dot_general(a, b, dims, preferred_element_type=F32)


def turned(x, amount):
    amount %= x.shape[1]
    return pltpu.roll(x, amount, 1) if amount else x


def grid(axis):
    return lax.broadcasted_iota(jnp.int32, (BLK, BLK), axis)


def build_bias(table_row, bias_ref, pair, lane):
    def shear(half):
        return pltpu.roll(
            jnp.broadcast_to(half, (BLK, BLK)), 0, 1, stride=1, stride_axis=0
        )

    ahead, behind = shear(table_row[:, CLIP:]), shear(table_row[:, :CLIP])
    flat = jnp.broadcast_to(table_row[:, 2 * CLIP - 1 :], (BLK, BLK))
    key, query = grid(0), grid(1)
    later = query >= key
    cols = pl.ds(lane * BLK, BLK)
    bias_ref[pair, :BLK, cols] = jnp.where((key < SEG) & (query >= SEG), NEG_FILL, flat)
    bias_ref[pair, BLK : 2 * BLK, cols] = jnp.where(later, flat, ahead)
    bias_ref[pair, 2 * BLK :, cols] = jnp.where(
        (key >= SEG) & (query < SEG), NEG_FILL, jnp.where(later, ahead, behind)
    )


def unshear(square):
    parts = [turned(square[8 * g : 8 * g + 8], -8 * g) for g in range(BLK // 8)]
    while len(parts) > 1:
        parts = [a + b for a, b in zip(parts[::2], parts[1::2])]
    row = lax.broadcasted_iota(jnp.int32, (8, BLK), 0)
    result = parts[0]
    for i in range(1, 8):
        result = jnp.where(row == i, turned(parts[0], -i), result)
    return jnp.sum(result, axis=0, keepdims=True)


def diagonals(square):
    top, far, near = square[:BLK], square[BLK : 2 * BLK], square[2 * BLK :]
    later = grid(1) >= grid(0)
    beyond = jnp.sum(top + jnp.where(later, far, 0.0), axis=0, keepdims=True)
    return (
        unshear(jnp.where(later, 0.0, near)),
        unshear(jnp.where(later, near, far)),
        beyond,
    )


def kernel(
    sp_size, tp_size, moved, direct,
    q_hbm, k_hbm, v_hbm, d_hbm, table_hbm,
    dq_ref, dk_ref, dv_ref, dt_ref,
    qd, got_qd, kv, bias_ref, square_ref, grown_ref, dprob_ref, peak_ref,
    own_k, own_v, own_q, back_q, got_q, back_kv, got_kv,
    local_stats, right_stats, halo_stats, left_stats,
    table_rows, pieces, exchange_a, exchange_b, exchange_c, exchange_d,
    load_sem, hop_sem, send_sem, seq_recv, back_recv, halo_recv, misc_recv,
):
    if direct:
        packs, pack_got, turns, stack = exchange_a, exchange_b, exchange_c, exchange_d
    else:
        piece_got, shares = exchange_a, exchange_b
    rows, width = q_hbm.shape
    pairs = width // LANES
    heads = width // HEAD_DIM
    part = 2 * CLIP // sp_size
    me = lax.axis_index("sp")
    col = lax.axis_index("tp")
    has_left = me > 0
    has_right = me < sp_size - 1
    left = jnp.maximum(me - 1, 0)
    right = jnp.minimum(me + 1, sp_size - 1)
    prev, own = pl.ds(0, rows), pl.ds(rows, rows)

    def columns(p):
        return pl.ds(p * LANES, LANES)

    for p in range(pairs):
        for i, src in enumerate((q_hbm, d_hbm)):
            pltpu.make_async_copy(src.at[:, columns(p)], qd.at[p, i], load_sem.at[2 + p]).start()
    pltpu.make_async_copy(table_hbm, table_rows, load_sem.at[0]).start()
    for p in range(pairs):
        for i, src in enumerate((k_hbm, v_hbm)):
            pltpu.make_async_copy(src.at[:, columns(p)], kv.at[p, i, own], load_sem.at[1]).start()

    barrier = pltpu.get_barrier_semaphore()

    def greet(sem, step):
        @pl.when(me >= step)
        def _():
            pl.semaphore_signal(sem, inc=1, device_id=(me - step, col), device_id_type=MESH)

        @pl.when(me + step < sp_size)
        def _():
            pl.semaphore_signal(sem, inc=1, device_id=(me + step, col), device_id_type=MESH)

    def greeters(step):
        return (me >= step).astype(jnp.int32) + (me + step < sp_size).astype(jnp.int32)

    greet(barrier, 1)
    for k in range(1, tp_size):
        pl.semaphore_signal(
            barrier, inc=1, device_id=(me, lax.rem(col + k, tp_size)), device_id_type=MESH
        )

    rounds = hop_sem.shape[0] - 1

    def hop(r):
        if 0 < r <= rounds:
            pl.semaphore_wait(hop_sem.at[r - 1], greeters(1 << (r - 1)))
        if r < rounds:
            greet(hop_sem.at[r], 1 << r)

    def remote(src, dst, send, recv, target):
        return pltpu.make_async_remote_copy(
            src_ref=src,
            dst_ref=dst,
            send_sem=send_sem.at[send],
            recv_sem=recv,
            device_id=(target, col),
            device_id_type=MESH,
        )

    def query_copy(p):
        return remote(qd.at[p], got_qd.at[p], 0, seq_recv.at[p], left)

    def all_queries():
        return remote(qd.at[pl.ds(0, moved)], got_qd, 0, misc_recv.at[0], left)

    def key_copy(p, block):
        return remote(
            kv.at[p, :, pl.ds(rows + block * BLK, BLK)],
            kv.at[p, :, pl.ds(block * BLK, BLK)],
            1,
            seq_recv.at[p + block * (pairs - moved)],
            right,
        )

    def all_keys():
        keyed = pl.ds(moved, pairs - moved)
        return remote(kv.at[keyed, :, own], kv.at[keyed, :, prev], 1, misc_recv.at[0], right)

    def local_copy():
        return remote(local_stats, right_stats, 2, misc_recv.at[0], left)

    def halo_copy(p):
        return remote(halo_stats.at[p], left_stats.at[p], 3, halo_recv.at[p], right)

    def back_copy(p):
        return remote(back_q.at[p], got_q.at[p], 4, back_recv.at[p], right)

    def key_back_copy(p):
        i = p - moved
        return remote(back_kv.at[i], got_kv.at[i], 5, back_recv.at[p], left)

    def send_queries(p):
        @pl.when(has_left)
        def _():
            query_copy(p).start()

    def send_back(p):
        if p < moved:
            @pl.when(has_right)
            def _():
                back_copy(p).start()
        else:
            @pl.when(has_left)
            def _():
                key_back_copy(p).start()

    def load_wait(refs, sem):
        pltpu.make_async_copy(refs, refs, sem).wait()

    pl.semaphore_wait(barrier, greeters(1) + tp_size - 1)
    load_wait(qd.at[0], load_sem.at[2])
    send_queries(0)
    hop(0)

    @pl.when(jnp.logical_not(has_left))
    def _():
        spot = lax.broadcasted_iota(jnp.int32, left_stats.shape, 1)
        left_stats[...] = jnp.where((spot & 2) == 0, NEG_FILL, 0.0)
        kv[moved:, :, prev] = jnp.zeros((pairs - moved, 2, rows, LANES), BF16)

    load_wait(table_rows, load_sem.at[0])
    for h in range(heads):
        row = table_rows[pl.ds(col * heads + h, 1), :] * LOG2E
        build_bias(row, bias_ref, h // 2, h % 2)

    for p in range(1, pairs):
        load_wait(qd.at[p], load_sem.at[2 + p])
    load_wait(kv.at[:, :, own], load_sem.at[1])

    low = lax.broadcasted_iota(jnp.int32, (BLK, LANES), 1) < HEAD_DIM
    scale = HEAD_DIM ** -0.5
    sums = {}

    def split(x):
        zero = jnp.zeros_like(x)
        return jnp.concatenate([jnp.where(low, x, zero), jnp.where(low, zero, x)], axis=0)

    def queries(ref, p, half):
        mine = pl.ds(half * BLK, BLK)
        return split(ref[p, 0, mine] * jnp.asarray(scale, BF16)), split(ref[p, 1, mine])

    def tile(p, half, halo):
        start, size, row = (
            (half * BLK, REACH - half * BLK, 0)
            if halo
            else (0, (half + 1) * BLK, REACH - half * BLK)
        )
        keys = pl.ds(rows + start, size)
        ref = got_qd if halo else qd
        return kv[p, 0, keys], kv[p, 1, keys], *queries(ref, p, half), pl.ds(row, size)

    def put(stats, p, half, which, value):
        for lane in range(2):
            spot = pl.ds(half * 4 + which * 2 + lane, 1)
            stats[p, spot, :] = value[:, lane * BLK : (lane + 1) * BLK]

    def get(stats, p, half, which):
        spots = [pl.ds(half * 4 + which * 2 + lane, 1) for lane in range(2)]
        return jnp.concatenate([stats[p, spot, :] for spot in spots], axis=1)

    def partial_softmax(p, half, halo, stats):
        k_blk, v_blk, qq, dd, band = tile(p, half, halo)
        scores = dot(k_blk, qq, NT) * LOG2E + bias_ref[p, band]
        dprobs = dot(v_blk, dd, NT)
        peak = jnp.max(scores, axis=0, keepdims=True)
        grown = jnp.exp2(scores - peak)
        total = jnp.sum(grown, axis=0, keepdims=True)
        put(stats, p, half, 0, peak + jnp.log2(total))
        put(stats, p, half, 1, jnp.sum(grown * dprobs, axis=0, keepdims=True) / total)
        return grown, dprobs, peak

    def products(k_blk, qq, dd, probs, dscores):
        ds_half = dscores.astype(BF16)
        flat = dot(k_blk, ds_half, TN)
        both = jnp.concatenate([flat[:HEAD_DIM, :BLK], flat[HEAD_DIM:, BLK:]], axis=0)
        return (
            dot(ds_half, qq, NN),
            dot(probs.astype(BF16), dd, NN),
            jnp.transpose(both) * scale,
        )

    def tile_probs(p, half, grown, dprobs, peak, stats, others):
        n1, i1 = get(stats, p, half, 0), get(stats, p, half, 1)
        n2, i2 = get(others, p, half, 0), get(others, p, half, 1)
        top = jnp.maximum(n1, n2)
        a1, a2 = jnp.exp2(n1 - top), jnp.exp2(n2 - top)
        inverse = 1.0 / (a1 + a2)
        inner = (i1 * a1 + i2 * a2) * inverse
        probs = grown * (jnp.exp2(peak - top) * inverse)
        return probs, probs * (dprobs - inner)

    def tile_grads(p, half, halo, probs, dscores):
        k_blk, _, qq, dd, _ = tile(p, half, halo)
        return products(k_blk, qq, dd, probs, dscores)

    places = (pl.ds(0, BLK), pl.ds(BLK, 2 * BLK))
    for p in range(moved):
        for half in range(2):
            grown, dprobs, peak = partial_softmax(p, half, False, local_stats)
            grown_ref[p, places[half], :] = grown
            dprob_ref[p, places[half], :] = dprobs
            peak_ref[p, pl.ds(half, 1), :] = peak

    @pl.when(has_left)
    def _():
        local_copy().start()

    if moved > 1:
        send_queries(1)

    even = lax.rem(me, 2) == 0
    core = lax.rem(col, 2)
    early = has_right & (even | (core == 0))
    keyed = [(p, block) for p in range(moved, pairs) for block in (1, 0)]
    turn = moved - 2 if moved > 1 else 0

    def send_keys():
        for p, block in keyed:
            key_copy(p, block).start()

    def after_stats(p):
        if p + 2 < moved:
            send_queries(p + 2)
        if p == turn:
            @pl.when(has_right & jnp.logical_not(even) & (core == 0))
            def _():
                pl.semaphore_signal(
                    hop_sem.at[rounds], inc=1, device_id=(me, col + 1), device_id_type=MESH
                )

            @pl.when(early)
            def _():
                send_keys()

        if p == moved - 1:
            for done in range(p):
                send_back(done)

    def late_keys():
        @pl.when(has_right & jnp.logical_not(early))
        def _():
            pl.semaphore_wait(hop_sem.at[rounds], 1)
            send_keys()

    def halo(p):
        @pl.when(has_right)
        def _():
            query_copy(p).wait_recv()
            kept = [partial_softmax(p, half, True, halo_stats) for half in range(2)]
            halo_copy(p).start()
            after_stats(p)
            if p == 0:
                local_copy().wait_recv()
            (p0, s0), (p1, s1) = (
                tile_probs(p, half, *kept[half], halo_stats, right_stats) for half in range(2)
            )
            k0, v0, q0 = tile_grads(p, 0, True, p0, s0)
            k1, v1, q1 = tile_grads(p, 1, True, p1, s1)
            for ref, a, b in ((own_k, k0, k1), (own_v, v0, v1)):
                ref[p, :BLK, :] = a[:BLK]
                ref[p, BLK:, :] = a[BLK:] + b
            back_q[p, :BLK, :] = q0.astype(BF16)
            back_q[p, BLK:, :] = q1.astype(BF16)
            square_ref[p, :BLK, :] = s0[:BLK] + s1
            square_ref[p, BLK:REACH, :] = s0[BLK:]

        @pl.when(jnp.logical_not(has_right))
        def _():
            after_stats(p)
            own_k[p] = jnp.zeros((rows, LANES), F32)
            own_v[p] = jnp.zeros((rows, LANES), F32)
            square_ref[p, :REACH, :] = jnp.zeros((REACH, 2 * BLK), F32)

        hop(p + 1)

    def tally(p, square):
        for lane in range(2):
            sums[2 * p + lane] = diagonals(square[:, lane * BLK : (lane + 1) * BLK])

    def local(p):
        cols = pl.ds(p * LANES, LANES)

        @pl.when(has_left)
        def _():
            halo_copy(p).wait_recv()

        (p0, s0), (p1, s1) = (
            tile_probs(
                p, half,
                grown_ref[p, places[half], :], dprob_ref[p, places[half], :],
                peak_ref[p, pl.ds(half, 1), :],
                local_stats, left_stats,
            )
            for half in range(2)
        )
        square = jnp.concatenate(
            [
                square_ref[p, :BLK, :],
                square_ref[p, BLK:REACH, :] + s1[:BLK],
                s0 + s1[BLK:],
            ],
            axis=0,
        )
        tally(p, square)
        k0, v0, q0 = tile_grads(p, 0, False, p0, s0)
        k1, v1, q1 = tile_grads(p, 1, False, p1, s1)
        for out, ref, a, b in ((dk_ref, own_k, k0, k1), (dv_ref, own_v, v0, v1)):
            out[:BLK, cols] = (ref[p, :BLK, :] + a + b[:BLK]).astype(BF16)
            out[BLK:, cols] = (ref[p, BLK:, :] + b[BLK:]).astype(BF16)
        own_q[p, :BLK, :] = q0
        own_q[p, BLK:, :] = q1

    gate = jnp.where(has_left, 0.0, NEG_FILL)

    def full(p, before=None, between=None):
        cols = pl.ds(p * LANES, LANES)
        i = p - moved

        def half_probs(half):
            @pl.when(has_left)
            def _():
                key_copy(p, half).wait_recv()

            keys = pl.ds(half * BLK, BAND)
            qq, dd = queries(qd, p, half)
            scores = dot(kv[p, 0, keys], qq, NT) * LOG2E + bias_ref[p]
            before = REACH - half * BLK
            scores = jnp.concatenate([scores[:before] + gate, scores[before:]], axis=0)
            dprobs = dot(kv[p, 1, keys], dd, NT)
            peak = jnp.max(scores, axis=0, keepdims=True)
            grown = jnp.exp2(scores - peak)
            inverse = 1.0 / jnp.sum(grown, axis=0, keepdims=True)
            inner = jnp.sum(grown * dprobs, axis=0, keepdims=True) * inverse
            probs = grown * inverse
            return probs, probs * (dprobs - inner)

        def half_grads(half, probs, dscores):
            qq, dd = queries(qd, p, half)
            return products(kv[p, 0, pl.ds(half * BLK, BAND)], qq, dd, probs, dscores)

        p1, s1 = half_probs(1)
        k1, v1, q1 = half_grads(1, p1, s1)
        if before is not None:
            before()
        p0, s0 = half_probs(0)
        if p == pairs - 1:
            send_back(moved - 1)
        tally(p, s0 + s1)
        if between is not None:
            between()
        k0, v0, q0 = half_grads(0, p0, s0)
        for which, ref, a, b in ((0, own_k, k0, k1), (1, own_v, v0, v1)):
            back_kv[i, which, :BLK, :] = a[:BLK].astype(BF16)
            back_kv[i, which, BLK:, :] = (a[BLK:REACH] + b[:BLK]).astype(BF16)
            ref[p, :BLK, :] = a[REACH:] + b[BLK:REACH]
            ref[p, BLK:, :] = b[REACH:]
        dq_ref[:BLK, cols] = q0.astype(BF16)
        dq_ref[BLK:, cols] = q1.astype(BF16)

    def piece_copy(k, t):
        target = lax.rem(me + k, sp_size)
        if direct:
            src, dst = packs.at[target], pack_got.at[col * sp_size + me]
        else:
            src, dst = pieces.at[target * part // CLIP], piece_got.at[k - 1]
        return pltpu.make_async_remote_copy(
            src_ref=src,
            dst_ref=dst,
            send_sem=send_sem.at[6],
            recv_sem=misc_recv.at[1],
            device_id=(target, lax.rem(col + t, tp_size)),
            device_id_type=MESH,
        )

    def all_pieces():
        ref = pack_got.at[pl.ds(1, sp_size * tp_size - 1)] if direct else piece_got
        return remote(ref, ref, 6, misc_recv.at[1], left)

    def share_copy(k):
        return pltpu.make_async_remote_copy(
            src_ref=shares.at[0],
            dst_ref=shares.at[k],
            send_sem=send_sem.at[7],
            recv_sem=misc_recv.at[2],
            device_id=(me, lax.rem(col + k, tp_size)),
            device_id_type=MESH,
        )

    def all_shares():
        rest = shares.at[pl.ds(1, tp_size - 1)]
        return remote(rest, rest, 7, misc_recv.at[2], left)

    groups = CLIP // part
    folded = exchange_a.shape[1]
    wide = heads // folded

    def fold():
        block = lax.broadcasted_iota(jnp.int32, (folded, CLIP), 1) // part
        for side in range(2):
            for a in range(groups):
                turns[a] = turned(pieces[side], part * a)
            for m in range(groups):
                pack = jnp.zeros((folded, CLIP), F32)
                for j in range(wide):
                    line = turns[(j - m) % groups, pl.ds(j, folded, stride=wide), :]
                    pack = jnp.where(block == j, line, pack)
                packs[side * groups + m] = pack

    def unfold():
        total = []
        for t in range(tp_size):
            line = pack_got[t * sp_size]
            for k in range(1, sp_size):
                line = line + pack_got[t * sp_size + k]
            total.append(line)
        total = jnp.concatenate(total, axis=0)
        for j in range(wide):
            stack[pl.ds(j, folded * tp_size, stride=wide), :] = turned(total, -part * j)
        dt_ref[...] = jnp.transpose(stack[...])[:part]

    def send_pieces():
        for r in range(moved + 1, rounds + 1):
            hop(r)
        behind, ahead, beyond = (
            jnp.concatenate([sums[h][i] for h in range(heads)], axis=0) for i in range(3)
        )
        beyond = jnp.sum(beyond, axis=1, keepdims=True)
        spot = lax.broadcasted_iota(jnp.int32, (heads, BLK), 1)
        pieces[0] = behind
        pieces[1] = ahead + jnp.where(spot == BLK - 1, beyond, 0.0)
        if direct:
            fold()
            pack_got[col * sp_size + me] = packs[me]
        for k in range(sp_size):
            for t in range(tp_size if direct else 1):
                if k or t:
                    piece_copy(k, t).start()

    for p in range(moved):
        halo(p)
        if p:
            local(p - 1)
        if p == turn:
            late_keys()
    last = pairs - 1
    for p in range(moved, last):
        full(p)
        send_back(p)
        if p == moved:
            local(moved - 1)
    if moved < last:
        full(last, None, send_pieces)
    else:
        full(last, lambda: local(moved - 1), send_pieces)
    send_back(last)

    def finish(p):
        cols = pl.ds(p * LANES, LANES)
        if p < moved:
            @pl.when(has_left)
            def _():
                back_copy(p).wait_recv()
                dq_ref[:, cols] = (own_q[p] + got_q[p].astype(F32)).astype(BF16)

            @pl.when(jnp.logical_not(has_left))
            def _():
                dq_ref[:, cols] = own_q[p].astype(BF16)
        else:
            i = p - moved

            @pl.when(has_right)
            def _():
                key_back_copy(p).wait_recv()
                dk_ref[:, cols] = (own_k[p] + got_kv[i, 0].astype(F32)).astype(BF16)
                dv_ref[:, cols] = (own_v[p] + got_kv[i, 1].astype(F32)).astype(BF16)

            @pl.when(jnp.logical_not(has_right))
            def _():
                dk_ref[:, cols] = own_k[p].astype(BF16)
                dv_ref[:, cols] = own_v[p].astype(BF16)

    for p in range(moved - 1):
        finish(p)
    all_pieces().wait_recv()
    if direct:
        unfold()
    else:
        total = pieces[me * part // CLIP]
        for k in range(1, sp_size):
            total = total + piece_got[k - 1]
        shares[0] = pltpu.roll(total, lax.rem(CLIP - lax.rem(me * part, CLIP), CLIP), 1)
        for k in range(1, tp_size):
            share_copy(k).start()
    for p in range(moved - 1, pairs):
        finish(p)
    if not direct:
        all_shares().wait_recv()
        stacked = jnp.concatenate(
            [shares[lax.rem(col + tp_size - t, tp_size)] for t in range(tp_size)], axis=0
        )
        dt_ref[...] = jnp.transpose(stacked)[:part]
        all_shares().wait_send()

    all_pieces().wait_send()

    @pl.when(has_left)
    def _():
        all_queries().wait_send()
        local_copy().wait_send()
        remote(back_kv, got_kv, 5, misc_recv.at[0], left).wait_send()

    @pl.when(has_right)
    def _():
        all_keys().wait_send()
        remote(halo_stats, left_stats, 3, misc_recv.at[0], right).wait_send()
        remote(back_q, got_q, 4, misc_recv.at[0], right).wait_send()


def shards(sp_size, tp_size, query_rows, key_rows, value_rows, out_grad, rel_bias):
    rows, width = query_rows.shape
    pairs = width // LANES
    heads = width // HEAD_DIM
    part = 2 * CLIP // sp_size
    moved = pairs - 1
    rounds = (sp_size - 1).bit_length()
    direct = sp_size * tp_size <= 64 and part <= CLIP and heads % (CLIP // part) == 0
    folded = heads * part // CLIP
    exchange = [
        pltpu.VMEM(shape, F32)
        for shape in (
            (
                (sp_size, folded, CLIP),
                (sp_size * tp_size, folded, CLIP),
                (CLIP // part, heads, CLIP),
                (tp_size * heads, CLIP),
            )
            if direct
            else ((sp_size - 1, heads, CLIP), (tp_size, heads, CLIP), (8, CLIP), (8, CLIP))
        )
    ]
    assert rows == REACH and REACH == 2 * BLK and CLIP == BLK
    like = jax.ShapeDtypeStruct((rows, width), BF16)
    dma = pltpu.SemaphoreType.DMA
    shapes = (like, like, like, jax.ShapeDtypeStruct((part, heads * tp_size), F32))
    results = pl.pallas_call(
        partial(kernel, sp_size, tp_size, moved, direct),
        out_shape=shapes,
        in_specs=[pl.BlockSpec(memory_space=pltpu.HBM)] * 5,
        out_specs=tuple([pl.BlockSpec(memory_space=pltpu.VMEM)] * 4),
        scratch_shapes=[
            pltpu.VMEM((pairs, 2, rows, LANES), BF16),
            pltpu.VMEM((moved, 2, rows, LANES), BF16),
            pltpu.VMEM((pairs, 2, 2 * rows, LANES), BF16),
            pltpu.VMEM((pairs, BAND, 2 * BLK), F32),
            pltpu.VMEM((moved, REACH, 2 * BLK), F32),
            pltpu.VMEM((moved, BAND, 2 * BLK), F32),
            pltpu.VMEM((moved, BAND, 2 * BLK), F32),
            pltpu.VMEM((moved, 8, 2 * BLK), F32),
            pltpu.VMEM((pairs, rows, LANES), F32),
            pltpu.VMEM((pairs, rows, LANES), F32),
            pltpu.VMEM((moved, rows, LANES), F32),
            pltpu.VMEM((moved, rows, LANES), BF16),
            pltpu.VMEM((moved, rows, LANES), BF16),
            pltpu.VMEM((pairs - moved, 2, rows, LANES), BF16),
            pltpu.VMEM((pairs - moved, 2, rows, LANES), BF16),
            pltpu.VMEM((moved, 8, BLK), F32),
            pltpu.VMEM((moved, 8, BLK), F32),
            pltpu.VMEM((moved, 8, BLK), F32),
            pltpu.VMEM((moved, 8, BLK), F32),
            pltpu.VMEM(rel_bias.shape[::-1], F32),
            pltpu.VMEM((2, heads, BLK), F32),
            *exchange,
            dma((2 + pairs,)),
            pltpu.SemaphoreType.REGULAR((rounds + 1,)),
            dma((8,)),
            dma((2 * pairs - moved,)),
            dma((pairs,)),
            dma((moved,)),
            dma((3,)),
        ],
        compiler_params=pltpu.CompilerParams(
            collective_id=0, has_side_effects=True, vmem_limit_bytes=48 * 1024 * 1024
        ),
    )(*[pltpu.with_memory_space_constraint(x, pltpu.HBM) for x in (query_rows, key_rows, value_rows, out_grad, jnp.transpose(rel_bias))])
    return pl.pallas_call(
        write_out,
        out_shape=shapes,
        in_specs=[pl.BlockSpec(memory_space=pl.ANY)] * 4,
        out_specs=tuple([pl.BlockSpec(memory_space=pltpu.HBM)] * 4),
        scratch_shapes=[dma((4,))],
        compiler_params=pltpu.CompilerParams(vmem_limit_bytes=1024 * 1024),
    )(*results)


def write_out(*refs):
    sem = refs[-1]
    copies = [pltpu.make_async_copy(refs[i], refs[4 + i], sem.at[i]) for i in range(4)]
    for copy in copies:
        copy.start()
    for copy in copies:
        copy.wait()


def solution(mesh):
    return jax.shard_map(
        partial(shards, mesh.shape["sp"], mesh.shape["tp"]),
        mesh=mesh,
        in_specs=(P("sp", "tp"), P("sp", "tp"), P("sp", "tp"), P("sp", "tp"), P()),
        out_specs=(P("sp", "tp"), P("sp", "tp"), P("sp", "tp"), P("sp", None)),
        check_vma=False,
    )
```

```python
from functools import partial
import math

import jax
import jax.numpy as jnp
from jax import lax
from jax.experimental import pallas as pl
from jax.experimental.pallas import tpu as pltpu
from jax.sharding import PartitionSpec as P

HEAD_DIM = 64
SEG = 64
LEFT = 4
CLIP = 128

LANES = 2 * HEAD_DIM
REACH = LEFT * SEG
BLK = 2 * SEG
BAND = REACH + BLK
WRAP = 3 * BLK
NEG_FILL = -1e30
LOG2E = math.log2(math.e)
MESH = pl.DeviceIdType.MESH
LEFTWARD, RIGHTWARD = 0, 1
F32 = jnp.float32
BF16 = jnp.bfloat16

NT = (((1,), (1,)), ((), ()))
NN = (((1,), (0,)), ((), ()))
TN = (((0,), (0,)), ((), ()))


def dot(a, b, dims):
    return lax.dot_general(a, b, dims, preferred_element_type=F32)


def turned(x, amount):
    amount %= x.shape[1]
    return pltpu.roll(x, amount, 1) if amount else x


def grid(axis):
    return lax.broadcasted_iota(jnp.int32, (BLK, BLK), axis)


def build_bias(table_row, bias_ref, pair, lane):
    def shear(half):
        return pltpu.roll(
            jnp.broadcast_to(half, (BLK, BLK)), 0, 1, stride=1, stride_axis=0
        )

    ahead, behind = shear(table_row[:, CLIP:]), shear(table_row[:, :CLIP])
    flat = jnp.broadcast_to(table_row[:, 2 * CLIP - 1 :], (BLK, BLK))
    key, query = grid(0), grid(1)
    later = query >= key
    cols = pl.ds(lane * BLK, BLK)
    bias_ref[pair, :BLK, cols] = jnp.where((key < SEG) & (query >= SEG), NEG_FILL, flat)
    bias_ref[pair, BLK : 2 * BLK, cols] = jnp.where(later, flat, ahead)
    bias_ref[pair, 2 * BLK :, cols] = jnp.where(
        (key >= SEG) & (query < SEG), NEG_FILL, jnp.where(later, ahead, behind)
    )


def unshear(square, shift):
    parts = [turned(square[8 * g : 8 * g + 8], -8 * g) for g in range(BLK // 8)]
    while len(parts) > 1:
        parts = [a + b for a, b in zip(parts[::2], parts[1::2])]
    row = lax.broadcasted_iota(jnp.int32, (8, BLK), 0)
    result = turned(parts[0], shift)
    for i in range(1, 8):
        result = jnp.where(row == i, turned(parts[0], shift - i), result)
    return jnp.sum(result, axis=0, keepdims=True)


def diagonals(square, shift):
    top, far, near = square[:BLK], square[BLK : 2 * BLK], square[2 * BLK :]
    later = grid(1) >= grid(0)
    beyond = jnp.sum(top + jnp.where(later, far, 0.0), axis=0, keepdims=True)
    spot = lax.broadcasted_iota(jnp.int32, (1, BLK), 1)
    clipped = jnp.where(
        spot == (BLK - 1 + shift) % BLK, jnp.sum(beyond, axis=1, keepdims=True), 0.0
    )
    return (
        unshear(jnp.where(later, 0.0, near), shift),
        unshear(jnp.where(later, near, far), shift) + clipped,
    )


def kernel(
    sp_size, tp_size, moved, direct,
    q_hbm, k_hbm, v_hbm, d_hbm, table_hbm,
    dq_ref, dk_ref, dv_ref, dt_ref,
    qd, got_qd, kv, bias_ref, square_ref, grown_ref, dprob_ref, peak_ref,
    own_k, own_v, own_q, back_q, got_q, back_kv, got_kv,
    local_stats, right_stats, halo_stats, left_stats,
    table_rows, pieces, exchange_a, exchange_b, exchange_c,
    load_sem, hop_sem, send_sem, seq_recv, back_recv, halo_recv, misc_recv,
):
    if direct:
        packs, pack_got, stack = exchange_a, exchange_b, exchange_c
    else:
        piece_got, shares = exchange_a, exchange_b
    rows, width = q_hbm.shape
    pairs = width // LANES
    heads = width // HEAD_DIM
    part = 2 * CLIP // sp_size
    me = lax.axis_index("sp")
    col = lax.axis_index("tp")
    has_left = me > 0
    has_right = me < sp_size - 1
    left = jnp.maximum(me - 1, 0)
    right = jnp.minimum(me + 1, sp_size - 1)
    prev, own = pl.ds(0, rows), pl.ds(rows, rows)

    def columns(p):
        return pl.ds(p * LANES, LANES)

    for p in range(pairs):
        for i, src in enumerate((q_hbm, d_hbm)):
            pltpu.make_async_copy(src.at[:, columns(p)], qd.at[p, i], load_sem.at[2 + (p > 0)]).start()
    pltpu.make_async_copy(table_hbm, table_rows, load_sem.at[0]).start()
    for p in range(pairs):
        for i, src in enumerate((k_hbm, v_hbm)):
            pltpu.make_async_copy(src.at[:, columns(p)], kv.at[p, i, own], load_sem.at[1]).start()

    barrier = pltpu.get_barrier_semaphore()

    def greet(sem, step):
        @pl.when(me >= step)
        def _():
            pl.semaphore_signal(sem, inc=1, device_id=(me - step, col), device_id_type=MESH)

        @pl.when(me + step < sp_size)
        def _():
            pl.semaphore_signal(sem, inc=1, device_id=(me + step, col), device_id_type=MESH)

    def greeters(step):
        return (me >= step).astype(jnp.int32) + (me + step < sp_size).astype(jnp.int32)

    greet(barrier, 1)
    for k in range(1, tp_size):
        pl.semaphore_signal(
            barrier, inc=1, device_id=(me, lax.rem(col + k, tp_size)), device_id_type=MESH
        )

    rounds = hop_sem.shape[0] - 1

    def hop(r):
        if 0 < r <= rounds:
            pl.semaphore_wait(hop_sem.at[r - 1], greeters(1 << (r - 1)))
        if r < rounds:
            greet(hop_sem.at[r], 1 << r)

    def remote(src, dst, send, recv, target):
        return pltpu.make_async_remote_copy(
            src_ref=src,
            dst_ref=dst,
            send_sem=send_sem.at[send],
            recv_sem=recv,
            device_id=(target, col),
            device_id_type=MESH,
        )

    def query_copy(p):
        return remote(qd.at[p], got_qd.at[p], LEFTWARD, seq_recv.at[p], left)

    def all_queries():
        return remote(qd.at[pl.ds(0, moved)], got_qd, LEFTWARD, misc_recv.at[0], left)

    def key_copy(p, block):
        return remote(
            kv.at[p, :, pl.ds(rows + block * BLK, BLK)],
            kv.at[p, :, pl.ds(block * BLK, BLK)],
            RIGHTWARD,
            seq_recv.at[p + block * (pairs - moved)],
            right,
        )

    def all_keys():
        keyed = pl.ds(moved, pairs - moved)
        return remote(kv.at[keyed, :, own], kv.at[keyed, :, prev], RIGHTWARD, misc_recv.at[0], right)

    def local_copy():
        return remote(local_stats, right_stats, LEFTWARD, misc_recv.at[0], left)

    def halo_copy(p):
        return remote(halo_stats.at[p], left_stats.at[p], RIGHTWARD, halo_recv.at[p], right)

    def back_copy(p):
        recv = back_recv.at[int(p == moved - 1)]
        return remote(back_q.at[p], got_q.at[p], RIGHTWARD, recv, right)

    def early_back():
        some = pl.ds(0, max(moved - 1, 1))
        return remote(back_q.at[some], got_q.at[some], RIGHTWARD, back_recv.at[0], right)

    def key_back_copy(p):
        i = p - moved
        return remote(back_kv.at[i], got_kv.at[i], LEFTWARD, back_recv.at[2 + i], left)

    def send_queries(p):
        @pl.when(has_left)
        def _():
            query_copy(p).start()

    def send_back(p):
        if p < moved:
            @pl.when(has_right)
            def _():
                back_copy(p).start()
        else:
            @pl.when(has_left)
            def _():
                key_back_copy(p).start()

    def load_wait(refs, sem):
        pltpu.make_async_copy(refs, refs, sem).wait()

    pl.semaphore_wait(barrier, greeters(1) + tp_size - 1)
    load_wait(qd.at[0], load_sem.at[2])
    send_queries(0)
    hop(0)

    @pl.when(jnp.logical_not(has_left))
    def _():
        spot = lax.broadcasted_iota(jnp.int32, left_stats.shape, 1)
        left_stats[...] = jnp.where((spot & 2) == 0, NEG_FILL, 0.0)
        kv[moved:, :, prev] = jnp.zeros((pairs - moved, 2, rows, LANES), BF16)

    load_wait(table_rows, load_sem.at[0])
    for h in range(heads):
        row = table_rows[pl.ds(col * heads + h, 1), :] * LOG2E
        build_bias(row, bias_ref, h // 2, h % 2)

    load_wait(qd.at[pl.ds(1, pairs - 1)], load_sem.at[3])
    load_wait(kv.at[:, :, own], load_sem.at[1])

    low = lax.broadcasted_iota(jnp.int32, (BLK, LANES), 1) < HEAD_DIM
    scale = HEAD_DIM ** -0.5
    groups = CLIP // part
    folded = exchange_a.shape[1]
    wide = heads // folded

    def split(x):
        zero = jnp.zeros_like(x)
        return jnp.concatenate([jnp.where(low, x, zero), jnp.where(low, zero, x)], axis=0)

    def queries(ref, p, half):
        mine = pl.ds(half * BLK, BLK)
        return split(ref[p, 0, mine] * jnp.asarray(scale, BF16)), split(ref[p, 1, mine])

    def tile(p, half, halo):
        start, size, row = (
            (half * BLK, REACH - half * BLK, 0)
            if halo
            else (0, (half + 1) * BLK, REACH - half * BLK)
        )
        keys = pl.ds(rows + start, size)
        ref = got_qd if halo else qd
        return kv[p, 0, keys], kv[p, 1, keys], *queries(ref, p, half), pl.ds(row, size)

    def put(stats, p, half, which, value):
        for lane in range(2):
            spot = pl.ds(half * 4 + which * 2 + lane, 1)
            stats[p, spot, :] = value[:, lane * BLK : (lane + 1) * BLK]

    def get(stats, p, half, which):
        spots = [pl.ds(half * 4 + which * 2 + lane, 1) for lane in range(2)]
        return jnp.concatenate([stats[p, spot, :] for spot in spots], axis=1)

    def partial_softmax(p, half, halo, stats):
        k_blk, v_blk, qq, dd, band = tile(p, half, halo)
        scores = dot(k_blk, qq, NT) * LOG2E + bias_ref[p, band]
        dprobs = dot(v_blk, dd, NT)
        peak = jnp.max(scores, axis=0, keepdims=True)
        grown = jnp.exp2(scores - peak)
        total = jnp.sum(grown, axis=0, keepdims=True)
        put(stats, p, half, 0, peak + jnp.log2(total))
        put(stats, p, half, 1, jnp.sum(grown * dprobs, axis=0, keepdims=True) / total)
        return grown, dprobs, peak

    def products(k_blk, qq, dd, probs, dscores):
        ds_half = dscores.astype(BF16)
        flat = dot(k_blk, ds_half, TN)
        both = jnp.concatenate([flat[:HEAD_DIM, :BLK], flat[HEAD_DIM:, BLK:]], axis=0)
        return (
            dot(ds_half, qq, NN),
            dot(probs.astype(BF16), dd, NN),
            jnp.transpose(both) * scale,
        )

    def tile_probs(p, half, grown, dprobs, peak, stats, others):
        n1, i1 = get(stats, p, half, 0), get(stats, p, half, 1)
        n2, i2 = get(others, p, half, 0), get(others, p, half, 1)
        top = jnp.maximum(n1, n2)
        a1, a2 = jnp.exp2(n1 - top), jnp.exp2(n2 - top)
        inverse = 1.0 / (a1 + a2)
        inner = (i1 * a1 + i2 * a2) * inverse
        probs = grown * (jnp.exp2(peak - top) * inverse)
        return probs, probs * (dprobs - inner)

    def tile_grads(p, half, halo, probs, dscores):
        k_blk, _, qq, dd, _ = tile(p, half, halo)
        return products(k_blk, qq, dd, probs, dscores)

    places = (pl.ds(0, BLK), pl.ds(BLK, 2 * BLK))
    for p in range(moved):
        for half in range(2):
            grown, dprobs, peak = partial_softmax(p, half, False, local_stats)
            grown_ref[p, places[half], :] = grown
            dprob_ref[p, places[half], :] = dprobs
            peak_ref[p, pl.ds(half, 1), :] = peak

    @pl.when(has_left)
    def _():
        local_copy().start()

    if moved > 1:
        send_queries(1)

    even = lax.rem(me, 2) == 0
    core = lax.rem(col, 2)
    early = has_right & (even | (core == 0))
    keyed = [(p, block) for p in range(moved, pairs) for block in (1, 0)]
    turn = moved - 2 if moved > 1 else 0

    def send_keys():
        for p, block in keyed:
            key_copy(p, block).start()

    def after_stats(p):
        if p + 2 < moved:
            send_queries(p + 2)
        if p == turn:
            @pl.when(has_right & jnp.logical_not(even) & (core == 0))
            def _():
                pl.semaphore_signal(
                    hop_sem.at[rounds], inc=1, device_id=(me, col + 1), device_id_type=MESH
                )

            @pl.when(early)
            def _():
                send_keys()

        if p == moved - 1:
            for done in range(p):
                send_back(done)

    def late_keys():
        @pl.when(has_right & jnp.logical_not(early))
        def _():
            pl.semaphore_wait(hop_sem.at[rounds], 1)
            send_keys()

    def halo(p):
        @pl.when(has_right)
        def _():
            query_copy(p).wait_recv()
            kept = [partial_softmax(p, half, True, halo_stats) for half in range(2)]
            halo_copy(p).start()
            after_stats(p)
            if p == 0:
                local_copy().wait_recv()
            (p0, s0), (p1, s1) = (
                tile_probs(p, half, *kept[half], halo_stats, right_stats) for half in range(2)
            )
            k0, v0, q0 = tile_grads(p, 0, True, p0, s0)
            k1, v1, q1 = tile_grads(p, 1, True, p1, s1)
            for ref, a, b in ((own_k, k0, k1), (own_v, v0, v1)):
                ref[p, :BLK, :] = a[:BLK]
                ref[p, BLK:, :] = a[BLK:] + b
            back_q[p, :BLK, :] = q0.astype(BF16)
            back_q[p, BLK:, :] = q1.astype(BF16)
            square_ref[p, :BLK, :] = s0[:BLK] + s1
            square_ref[p, BLK:REACH, :] = s0[BLK:]

        @pl.when(jnp.logical_not(has_right))
        def _():
            after_stats(p)
            own_k[p] = jnp.zeros((rows, LANES), F32)
            own_v[p] = jnp.zeros((rows, LANES), F32)
            square_ref[p, :REACH, :] = jnp.zeros((REACH, 2 * BLK), F32)

        hop(p + 1)

    def tally(p, square):
        for lane in range(2):
            head = 2 * p + lane
            sides = diagonals(
                square[:, lane * BLK : (lane + 1) * BLK],
                part * (head % wide) if direct else 0,
            )
            for side in range(2):
                pieces[side, head : head + 1] = sides[side]

    def local_probs(p):
        @pl.when(has_left)
        def _():
            halo_copy(p).wait_recv()

        (p0, s0), (p1, s1) = (
            tile_probs(
                p, half,
                grown_ref[p, places[half], :], dprob_ref[p, places[half], :],
                peak_ref[p, pl.ds(half, 1), :],
                local_stats, left_stats,
            )
            for half in range(2)
        )
        square = jnp.concatenate(
            [
                square_ref[p, :BLK, :],
                square_ref[p, BLK:REACH, :] + s1[:BLK],
                s0 + s1[BLK:],
            ],
            axis=0,
        )
        tally(p, square)
        return p0, s0, p1, s1

    def local_grads(p, p0, s0, p1, s1):
        cols = columns(p)
        k0, v0, q0 = tile_grads(p, 0, False, p0, s0)
        k1, v1, q1 = tile_grads(p, 1, False, p1, s1)
        for out, ref, a, b in ((dk_ref, own_k, k0, k1), (dv_ref, own_v, v0, v1)):
            out[:BLK, cols] = (ref[p, :BLK, :] + a + b[:BLK]).astype(BF16)
            out[BLK:, cols] = (ref[p, BLK:, :] + b[BLK:]).astype(BF16)
        own_q[p, :BLK, :] = q0
        own_q[p, BLK:, :] = q1

    def local(p):
        local_grads(p, *local_probs(p))

    gate = jnp.where(has_left, 0.0, NEG_FILL)

    def full(p, between=None):
        cols = columns(p)
        i = p - moved

        def arrived(block):
            @pl.when(has_left)
            def _():
                key_copy(p, block).wait_recv()

        def part_of(half, row, size, before):
            keys = pl.ds(half * BLK + row, size)
            qq, dd = queries(qd, p, half)
            scores = dot(kv[p, 0, keys], qq, NT) * LOG2E + bias_ref[p, pl.ds(row, size)]
            scores = (
                jnp.concatenate([scores[:before] + gate, scores[before:]], axis=0)
                if before < size
                else scores + gate
            )
            peak = jnp.max(scores, axis=0, keepdims=True)
            return scores, dot(kv[p, 1, keys], dd, NT), peak

        def moments(grown, dprobs):
            return (
                jnp.sum(grown, axis=0, keepdims=True),
                jnp.sum(grown * dprobs, axis=0, keepdims=True),
            )

        def half_grads(half, probs, dscores):
            qq, dd = queries(qd, p, half)
            return products(kv[p, 0, pl.ds(half * BLK, BAND)], qq, dd, probs, dscores)

        arrived(1)
        scores, dprobs, peak = part_of(1, 0, BAND, BLK)
        grown = jnp.exp2(scores - peak)
        total, inner = moments(grown, dprobs)
        inverse = 1.0 / total
        probs = grown * inverse
        s1 = probs * (dprobs - inner * inverse)
        k1, v1, q1 = half_grads(1, probs, s1)
        scores_a, dprobs_a, peak_a = part_of(0, BLK, 2 * BLK, BLK)
        grown_a = jnp.exp2(scores_a - peak_a)
        total_a, inner_a = moments(grown_a, dprobs_a)

        arrived(0)
        scores_b, dprobs_b, peak_b = part_of(0, 0, BLK, BLK)
        peak = jnp.maximum(peak_a, peak_b)
        grown_b = jnp.exp2(scores_b - peak)
        total_b, inner_b = moments(grown_b, dprobs_b)
        factor = jnp.exp2(peak_a - peak)
        inverse = 1.0 / (total_a * factor + total_b)
        inner = (inner_a * factor + inner_b) * inverse
        probs_a, probs_b = grown_a * (factor * inverse), grown_b * inverse
        p0 = jnp.concatenate([probs_b, probs_a], axis=0)
        s0 = jnp.concatenate(
            [probs_b * (dprobs_b - inner), probs_a * (dprobs_a - inner)], axis=0
        )
        tally(p, s0 + s1)
        if p == pairs - 1:
            send_back(moved - 1)
        if between is not None:
            between()
        k0, v0, q0 = half_grads(0, p0, s0)
        for which, ref, a, b in ((0, own_k, k0, k1), (1, own_v, v0, v1)):
            back_kv[i, which, :BLK, :] = a[:BLK].astype(BF16)
            back_kv[i, which, BLK:, :] = (a[BLK:REACH] + b[:BLK]).astype(BF16)
            ref[p, :BLK, :] = a[REACH:] + b[BLK:REACH]
            ref[p, BLK:, :] = b[REACH:]
        dq_ref[:BLK, cols] = q0.astype(BF16)
        dq_ref[BLK:, cols] = q1.astype(BF16)

    def piece_copy(k, t):
        target = lax.rem(me + k, sp_size)
        if direct:
            src, dst = packs.at[target], pack_got.at[col * sp_size + me]
        else:
            src, dst = pieces.at[target * part // CLIP], piece_got.at[k - 1]
        return pltpu.make_async_remote_copy(
            src_ref=src,
            dst_ref=dst,
            send_sem=send_sem.at[2],
            recv_sem=misc_recv.at[1],
            device_id=(target, lax.rem(col + t, tp_size)),
            device_id_type=MESH,
        )

    def all_pieces():
        ref = pack_got.at[pl.ds(1, sp_size * tp_size - 1)] if direct else piece_got
        return remote(ref, ref, 2, misc_recv.at[1], left)

    def share_copy(k):
        return pltpu.make_async_remote_copy(
            src_ref=shares.at[0],
            dst_ref=shares.at[k],
            send_sem=send_sem.at[3],
            recv_sem=misc_recv.at[2],
            device_id=(me, lax.rem(col + k, tp_size)),
            device_id_type=MESH,
        )

    def all_shares():
        rest = shares.at[pl.ds(1, tp_size - 1)]
        return remote(rest, rest, 3, misc_recv.at[2], left)

    def fold():
        block = lax.broadcasted_iota(jnp.int32, (folded, CLIP), 1) // part
        for side in range(2):
            lines = [pieces[side, pl.ds(j, folded, stride=wide), :] for j in range(wide)]
            for m in range(groups):
                pack = jnp.zeros((folded, CLIP), F32)
                for j in range(wide):
                    pack = jnp.where(block == (m + j) % groups, lines[j], pack)
                packs[side * groups + m] = pack

    def unfold():
        total = []
        for t in range(tp_size):
            line = pack_got[t * sp_size]
            for k in range(1, sp_size):
                line = line + pack_got[t * sp_size + k]
            total.append(line)
        total = jnp.concatenate(total, axis=0)
        for j in range(wide):
            away = lax.rem(me + j, groups) * part
            stack[pl.ds(j, folded * tp_size, stride=wide), :] = pltpu.roll(
                total, lax.rem(CLIP - away, CLIP), 1
            )
        dt_ref[...] = jnp.transpose(stack[...])[:part]

    def send_pieces():
        for r in range(moved + 1, rounds + 1):
            hop(r)
        if direct:
            fold()
            pack_got[col * sp_size + me] = packs[me]
        for k in range(sp_size):
            for t in range(tp_size if direct else 1):
                if k or t:
                    piece_copy(k, t).start()

    for p in range(moved):
        halo(p)
        if p:
            local(p - 1)
        if p == turn:
            late_keys()
    last = pairs - 1
    for p in range(moved, last):
        full(p)
        send_back(p)
        if p == moved:
            local(moved - 1)
    kept = []

    def finish_pieces():
        if moved == last:
            kept.extend(local_probs(moved - 1))
        send_pieces()

    full(last, finish_pieces)
    send_back(last)
    if kept:
        local_grads(moved - 1, *kept)

    def finish(p):
        cols = pl.ds(p * LANES, LANES)
        if p < moved:
            @pl.when(has_left)
            def _():
                if p == moved - 1:
                    back_copy(p).wait_recv()
                elif p == 0:
                    early_back().wait_recv()
                dq_ref[:, cols] = (own_q[p] + got_q[p].astype(F32)).astype(BF16)

            @pl.when(jnp.logical_not(has_left))
            def _():
                dq_ref[:, cols] = own_q[p].astype(BF16)
        else:
            i = p - moved

            @pl.when(has_right)
            def _():
                key_back_copy(p).wait_recv()
                dk_ref[:, cols] = (own_k[p] + got_kv[i, 0].astype(F32)).astype(BF16)
                dv_ref[:, cols] = (own_v[p] + got_kv[i, 1].astype(F32)).astype(BF16)

            @pl.when(jnp.logical_not(has_right))
            def _():
                dk_ref[:, cols] = own_k[p].astype(BF16)
                dv_ref[:, cols] = own_v[p].astype(BF16)

    if direct:
        for p in range(pairs):
            finish(p)
    all_pieces().wait_recv()
    if direct:
        unfold()
    else:
        total = pieces[me * part // CLIP]
        for k in range(1, sp_size):
            total = total + piece_got[k - 1]
        shares[0] = pltpu.roll(total, lax.rem(CLIP - lax.rem(me * part, CLIP), CLIP), 1)
        for k in range(1, tp_size):
            share_copy(k).start()
    if not direct:
        for p in range(pairs):
            finish(p)
        all_shares().wait_recv()
        stacked = jnp.concatenate(
            [shares[lax.rem(col + tp_size - t, tp_size)] for t in range(tp_size)], axis=0
        )
        dt_ref[...] = jnp.transpose(stacked)[:part]
        all_shares().wait_send()

    all_pieces().wait_send()

    @pl.when(has_left)
    def _():
        all_queries().wait_send()
        local_copy().wait_send()
        remote(back_kv, got_kv, LEFTWARD, misc_recv.at[0], left).wait_send()

    @pl.when(has_right)
    def _():
        all_keys().wait_send()
        remote(halo_stats, left_stats, RIGHTWARD, misc_recv.at[0], right).wait_send()
        remote(back_q, got_q, RIGHTWARD, misc_recv.at[0], right).wait_send()


def shards(sp_size, tp_size, query_rows, key_rows, value_rows, out_grad, rel_bias):
    rows, width = query_rows.shape
    pairs = width // LANES
    heads = width // HEAD_DIM
    part = 2 * CLIP // sp_size
    moved = pairs - 1
    rounds = (sp_size - 1).bit_length()
    direct = sp_size * tp_size <= 64 and part <= CLIP and heads % (CLIP // part) == 0
    folded = heads * part // CLIP
    exchange = [
        pltpu.VMEM(shape, F32)
        for shape in (
            (
                (sp_size, folded, CLIP),
                (sp_size * tp_size, folded, CLIP),
                (tp_size * heads, CLIP),
            )
            if direct
            else ((sp_size - 1, heads, CLIP), (tp_size, heads, CLIP), (8, CLIP))
        )
    ]
    assert rows == REACH and REACH == 2 * BLK and CLIP == BLK
    like = jax.ShapeDtypeStruct((rows, width), BF16)
    dma = pltpu.SemaphoreType.DMA
    shapes = (like, like, like, jax.ShapeDtypeStruct((part, heads * tp_size), F32))
    results = pl.pallas_call(
        partial(kernel, sp_size, tp_size, moved, direct),
        out_shape=shapes,
        in_specs=[pl.BlockSpec(memory_space=pltpu.HBM)] * 5,
        out_specs=tuple([pl.BlockSpec(memory_space=pltpu.VMEM)] * 4),
        scratch_shapes=[
            pltpu.VMEM((pairs, 2, rows, LANES), BF16),
            pltpu.VMEM((moved, 2, rows, LANES), BF16),
            pltpu.VMEM((pairs, 2, 2 * rows, LANES), BF16),
            pltpu.VMEM((pairs, BAND, 2 * BLK), F32),
            pltpu.VMEM((moved, REACH, 2 * BLK), F32),
            pltpu.VMEM((moved, BAND, 2 * BLK), F32),
            pltpu.VMEM((moved, BAND, 2 * BLK), F32),
            pltpu.VMEM((moved, 8, 2 * BLK), F32),
            pltpu.VMEM((pairs, rows, LANES), F32),
            pltpu.VMEM((pairs, rows, LANES), F32),
            pltpu.VMEM((moved, rows, LANES), F32),
            pltpu.VMEM((moved, rows, LANES), BF16),
            pltpu.VMEM((moved, rows, LANES), BF16),
            pltpu.VMEM((pairs - moved, 2, rows, LANES), BF16),
            pltpu.VMEM((pairs - moved, 2, rows, LANES), BF16),
            pltpu.VMEM((moved, 8, BLK), F32),
            pltpu.VMEM((moved, 8, BLK), F32),
            pltpu.VMEM((moved, 8, BLK), F32),
            pltpu.VMEM((moved, 8, BLK), F32),
            pltpu.VMEM(rel_bias.shape[::-1], F32),
            pltpu.VMEM((2, heads, BLK), F32),
            *exchange,
            dma((4,)),
            pltpu.SemaphoreType.REGULAR((rounds + 1,)),
            dma((3 if direct else 4,)),
            dma((2 * pairs - moved,)),
            dma((2 + pairs - moved,)),
            dma((moved,)),
            dma((2 if direct else 3,)),
        ],
        compiler_params=pltpu.CompilerParams(
            collective_id=0, has_side_effects=True, vmem_limit_bytes=48 * 1024 * 1024
        ),
    )(*[pltpu.with_memory_space_constraint(x, pltpu.HBM) for x in (query_rows, key_rows, value_rows, out_grad, jnp.transpose(rel_bias))])
    return pl.pallas_call(
        write_out,
        out_shape=shapes,
        in_specs=[pl.BlockSpec(memory_space=pl.ANY)] * 4,
        out_specs=tuple([pl.BlockSpec(memory_space=pltpu.HBM)] * 4),
        scratch_shapes=[dma((4,))],
        compiler_params=pltpu.CompilerParams(vmem_limit_bytes=1024 * 1024),
    )(*results)


def write_out(*refs):
    sem = refs[-1]
    copies = [pltpu.make_async_copy(refs[i], refs[4 + i], sem.at[i]) for i in range(4)]
    for copy in copies:
        copy.start()
    for copy in copies:
        copy.wait()


def solution(mesh):
    return jax.shard_map(
        partial(shards, mesh.shape["sp"], mesh.shape["tp"]),
        mesh=mesh,
        in_specs=(P("sp", "tp"), P("sp", "tp"), P("sp", "tp"), P("sp", "tp"), P()),
        out_specs=(P("sp", "tp"), P("sp", "tp"), P("sp", "tp"), P("sp", None)),
        check_vma=False,
    )
```

```python
from functools import partial
import math

import jax
import jax.numpy as jnp
from jax import lax
from jax.experimental import pallas as pl
from jax.experimental.pallas import tpu as pltpu
from jax.sharding import PartitionSpec as P

HEAD_DIM = 64
SEG = 64
LEFT = 4
CLIP = 128

LANES = 2 * HEAD_DIM
REACH = LEFT * SEG
BLK = 2 * SEG
BAND = REACH + BLK
WRAP = 3 * BLK
NEG_FILL = -1e30
LOG2E = math.log2(math.e)
MESH = pl.DeviceIdType.MESH
LEFTWARD, RIGHTWARD = 0, 1
F32 = jnp.float32
BF16 = jnp.bfloat16

NT = (((1,), (1,)), ((), ()))
NN = (((1,), (0,)), ((), ()))
TN = (((0,), (0,)), ((), ()))


def dot(a, b, dims):
    return lax.dot_general(a, b, dims, preferred_element_type=F32)


def turned(x, amount):
    amount %= x.shape[1]
    return pltpu.roll(x, amount, 1) if amount else x


def grid(axis):
    return lax.broadcasted_iota(jnp.int32, (BLK, BLK), axis)


def build_bias(table_row, bias_ref, pair, lane):
    def shear(half):
        return pltpu.roll(
            jnp.broadcast_to(half, (BLK, BLK)), 0, 1, stride=1, stride_axis=0
        )

    ahead, behind = shear(table_row[:, CLIP:]), shear(table_row[:, :CLIP])
    flat = jnp.broadcast_to(table_row[:, 2 * CLIP - 1 :], (BLK, BLK))
    key, query = grid(0), grid(1)
    later = query >= key
    cols = pl.ds(lane * BLK, BLK)
    bias_ref[pair, :BLK, cols] = jnp.where((key < SEG) & (query >= SEG), NEG_FILL, flat)
    bias_ref[pair, BLK : 2 * BLK, cols] = jnp.where(later, flat, ahead)
    bias_ref[pair, 2 * BLK :, cols] = jnp.where(
        (key >= SEG) & (query < SEG), NEG_FILL, jnp.where(later, ahead, behind)
    )


def unshear(square, shift):
    parts = [turned(square[8 * g : 8 * g + 8], -8 * g) for g in range(BLK // 8)]
    while len(parts) > 1:
        parts = [a + b for a, b in zip(parts[::2], parts[1::2])]
    row = lax.broadcasted_iota(jnp.int32, (8, BLK), 0)
    result = turned(parts[0], shift)
    for i in range(1, 8):
        result = jnp.where(row == i, turned(parts[0], shift - i), result)
    return jnp.sum(result, axis=0, keepdims=True)


def diagonals(square, shift):
    top, far, near = square[:BLK], square[BLK : 2 * BLK], square[2 * BLK :]
    later = grid(1) >= grid(0)
    beyond = jnp.sum(top + jnp.where(later, far, 0.0), axis=0, keepdims=True)
    spot = lax.broadcasted_iota(jnp.int32, (1, BLK), 1)
    clipped = jnp.where(
        spot == (BLK - 1 + shift) % BLK, jnp.sum(beyond, axis=1, keepdims=True), 0.0
    )
    return (
        unshear(jnp.where(later, 0.0, near), shift),
        unshear(jnp.where(later, near, far), shift) + clipped,
    )


def kernel(
    sp_size, tp_size, moved, direct,
    q_hbm, k_hbm, v_hbm, d_hbm, table_hbm,
    dq_ref, dk_ref, dv_ref, dt_ref,
    qd, got_qd, kv, bias_ref, square_ref, grown_ref, dprob_ref, peak_ref,
    own_k, own_v, own_q, back_q, got_q, back_kv, got_kv,
    local_stats, right_stats, halo_stats, left_stats,
    table_rows, pieces, exchange_a, exchange_b, exchange_c,
    load_sem, hop_sem, send_sem, seq_recv, back_recv, halo_recv, misc_recv,
):
    if direct:
        packs, pack_got, stack = exchange_a, exchange_b, exchange_c
    else:
        piece_got, shares = exchange_a, exchange_b
    rows, width = q_hbm.shape
    pairs = width // LANES
    heads = width // HEAD_DIM
    part = 2 * CLIP // sp_size
    me = lax.axis_index("sp")
    col = lax.axis_index("tp")
    has_left = me > 0
    has_right = me < sp_size - 1
    left = jnp.maximum(me - 1, 0)
    right = jnp.minimum(me + 1, sp_size - 1)
    prev, own = pl.ds(0, rows), pl.ds(rows, rows)

    def columns(p):
        return pl.ds(p * LANES, LANES)

    barrier = pltpu.get_barrier_semaphore()

    def greet(sem, step):
        @pl.when(me >= step)
        def _():
            pl.semaphore_signal(sem, inc=1, device_id=(me - step, col), device_id_type=MESH)

        @pl.when(me + step < sp_size)
        def _():
            pl.semaphore_signal(sem, inc=1, device_id=(me + step, col), device_id_type=MESH)

    def greeters(step):
        return (me >= step).astype(jnp.int32) + (me + step < sp_size).astype(jnp.int32)

    @pl.when(has_right)
    def _():
        pl.semaphore_signal(barrier, inc=1, device_id=(me + 1, col), device_id_type=MESH)

    for k in range(1, tp_size):
        pl.semaphore_signal(
            barrier, inc=1, device_id=(me, lax.rem(col + k, tp_size)), device_id_type=MESH
        )

    for p in range(pairs):
        for i, src in enumerate((q_hbm, d_hbm)):
            pltpu.make_async_copy(src.at[:, columns(p)], qd.at[p, i], load_sem.at[2 + (p > 0)]).start()
    pltpu.make_async_copy(table_hbm, table_rows, load_sem.at[0]).start()
    for p in range(pairs):
        for i, src in enumerate((k_hbm, v_hbm)):
            pltpu.make_async_copy(src.at[:, columns(p)], kv.at[p, i, own], load_sem.at[1]).start()

    rounds = hop_sem.shape[0] - 1

    def hop(r):
        if 0 < r <= rounds:
            pl.semaphore_wait(hop_sem.at[r - 1], greeters(1 << (r - 1)))
        if r < rounds:
            greet(hop_sem.at[r], 1 << r)

    def remote(src, dst, send, recv, target):
        return pltpu.make_async_remote_copy(
            src_ref=src,
            dst_ref=dst,
            send_sem=send_sem.at[send],
            recv_sem=recv,
            device_id=(target, col),
            device_id_type=MESH,
        )

    def query_copy(p):
        return remote(qd.at[p], got_qd.at[p], LEFTWARD, seq_recv.at[p], left)

    turn = max(moved - 2, 0)

    def query_part(half):
        mine = pl.ds(half * BLK, BLK)
        recv = seq_recv.at[2 * pairs - moved if half == 0 else turn]
        return remote(qd.at[turn, :, mine], got_qd.at[turn, :, mine], LEFTWARD, recv, left)

    def all_queries():
        return remote(qd.at[pl.ds(0, moved)], got_qd, LEFTWARD, misc_recv.at[0], left)

    def key_copy(p, block):
        return remote(
            kv.at[p, :, pl.ds(rows + block * BLK, BLK)],
            kv.at[p, :, pl.ds(block * BLK, BLK)],
            RIGHTWARD,
            seq_recv.at[p + block * (pairs - moved)],
            right,
        )

    def all_keys():
        keyed = pl.ds(moved, pairs - moved)
        return remote(kv.at[keyed, :, own], kv.at[keyed, :, prev], RIGHTWARD, misc_recv.at[0], right)

    def local_copy():
        return remote(local_stats, right_stats, LEFTWARD, misc_recv.at[0], left)

    def halo_copy(p):
        return remote(halo_stats.at[p], left_stats.at[p], RIGHTWARD, halo_recv.at[p], right)

    def back_copy(p):
        recv = back_recv.at[int(p == moved - 1)]
        return remote(back_q.at[p], got_q.at[p], RIGHTWARD, recv, right)

    def early_back():
        some = pl.ds(0, max(moved - 1, 1))
        return remote(back_q.at[some], got_q.at[some], RIGHTWARD, back_recv.at[0], right)

    def key_back_copy(p):
        i = p - moved
        return remote(back_kv.at[i], got_kv.at[i], LEFTWARD, back_recv.at[2 + i], left)

    def send_queries(p):
        @pl.when(has_left)
        def _():
            if p == turn:
                query_part(1).start()
                query_part(0).start()
            else:
                query_copy(p).start()

    def send_back(p):
        if p < moved:
            @pl.when(has_right)
            def _():
                back_copy(p).start()
        else:
            @pl.when(has_left)
            def _():
                key_back_copy(p).start()

    def load_wait(refs, sem):
        pltpu.make_async_copy(refs, refs, sem).wait()

    pl.semaphore_wait(barrier, has_left.astype(jnp.int32) + tp_size - 1)
    load_wait(qd.at[0], load_sem.at[2])
    send_queries(0)

    @pl.when(jnp.logical_not(has_left))
    def _():
        spot = lax.broadcasted_iota(jnp.int32, left_stats.shape, 1)
        left_stats[...] = jnp.where((spot & 2) == 0, NEG_FILL, 0.0)
        kv[moved:, :, prev] = jnp.zeros((pairs - moved, 2, rows, LANES), BF16)

    load_wait(table_rows, load_sem.at[0])
    for h in range(heads):
        row = table_rows[pl.ds(col * heads + h, 1), :] * LOG2E
        build_bias(row, bias_ref, h // 2, h % 2)

    load_wait(qd.at[pl.ds(1, pairs - 1)], load_sem.at[3])
    load_wait(kv.at[:, :, own], load_sem.at[1])

    low = lax.broadcasted_iota(jnp.int32, (BLK, LANES), 1) < HEAD_DIM
    scale = HEAD_DIM ** -0.5
    groups = CLIP // part
    folded = exchange_a.shape[1]
    wide = heads // folded

    def split(x):
        zero = jnp.zeros_like(x)
        return jnp.concatenate([jnp.where(low, x, zero), jnp.where(low, zero, x)], axis=0)

    def queries(ref, p, half):
        mine = pl.ds(half * BLK, BLK)
        return split(ref[p, 0, mine] * jnp.asarray(scale, BF16)), split(ref[p, 1, mine])

    def tile(p, half, halo):
        start, size, row = (
            (half * BLK, REACH - half * BLK, 0)
            if halo
            else (0, (half + 1) * BLK, REACH - half * BLK)
        )
        keys = pl.ds(rows + start, size)
        ref = got_qd if halo else qd
        return kv[p, 0, keys], kv[p, 1, keys], *queries(ref, p, half), pl.ds(row, size)

    def put(stats, p, half, which, value):
        for lane in range(2):
            spot = pl.ds(half * 4 + which * 2 + lane, 1)
            stats[p, spot, :] = value[:, lane * BLK : (lane + 1) * BLK]

    def get(stats, p, half, which):
        spots = [pl.ds(half * 4 + which * 2 + lane, 1) for lane in range(2)]
        return jnp.concatenate([stats[p, spot, :] for spot in spots], axis=1)

    def partial_softmax(p, half, halo, stats):
        k_blk, v_blk, qq, dd, band = tile(p, half, halo)
        scores = dot(k_blk, qq, NT) * LOG2E + bias_ref[p, band]
        dprobs = dot(v_blk, dd, NT)
        peak = jnp.max(scores, axis=0, keepdims=True)
        grown = jnp.exp2(scores - peak)
        total = jnp.sum(grown, axis=0, keepdims=True)
        put(stats, p, half, 0, peak + jnp.log2(total))
        put(stats, p, half, 1, jnp.sum(grown * dprobs, axis=0, keepdims=True) / total)
        return grown, dprobs, peak

    def products(k_blk, qq, dd, probs, dscores):
        ds_half = dscores.astype(BF16)
        flat = dot(k_blk, ds_half, TN)
        both = jnp.concatenate([flat[:HEAD_DIM, :BLK], flat[HEAD_DIM:, BLK:]], axis=0)
        return (
            dot(ds_half, qq, NN),
            dot(probs.astype(BF16), dd, NN),
            jnp.transpose(both) * scale,
        )

    def tile_probs(p, half, grown, dprobs, peak, stats, others):
        n1, i1 = get(stats, p, half, 0), get(stats, p, half, 1)
        n2, i2 = get(others, p, half, 0), get(others, p, half, 1)
        top = jnp.maximum(n1, n2)
        a1, a2 = jnp.exp2(n1 - top), jnp.exp2(n2 - top)
        inverse = 1.0 / (a1 + a2)
        inner = (i1 * a1 + i2 * a2) * inverse
        probs = grown * (jnp.exp2(peak - top) * inverse)
        return probs, probs * (dprobs - inner)

    def tile_grads(p, half, halo, probs, dscores):
        k_blk, _, qq, dd, _ = tile(p, half, halo)
        return products(k_blk, qq, dd, probs, dscores)

    places = (pl.ds(0, BLK), pl.ds(BLK, 2 * BLK))
    for p in range(moved):
        for half in range(2):
            grown, dprobs, peak = partial_softmax(p, half, False, local_stats)
            grown_ref[p, places[half], :] = grown
            dprob_ref[p, places[half], :] = dprobs
            peak_ref[p, pl.ds(half, 1), :] = peak

    @pl.when(has_left)
    def _():
        local_copy().start()

    if moved > 1:
        send_queries(1)

    even = lax.rem(me, 2) == 0
    core = lax.rem(col, 2)
    early = has_right & (even | (core == 0))
    keyed = [(p, block) for p in range(moved, pairs) for block in (1, 0)]

    def send_keys(blocks):
        for p, block in blocks:
            key_copy(p, block).start()

    def first_keys():
        @pl.when(has_right & jnp.logical_not(even) & (core == 0))
        def _():
            pl.semaphore_signal(
                hop_sem.at[rounds], inc=1, device_id=(me, col + 1), device_id_type=MESH
            )

        @pl.when(early)
        def _():
            send_keys(keyed[:1])

    def after_stats(p):
        if p + 2 < moved:
            send_queries(p + 2)
        if p == turn:
            @pl.when(early)
            def _():
                send_keys(keyed[1:])

            @pl.when(has_right & jnp.logical_not(early))
            def _():
                pl.semaphore_wait(hop_sem.at[rounds], 1)
                send_keys(keyed)

        if p == moved - 1:
            for done in range(p):
                send_back(done)

    def halo(p):
        @pl.when(has_right)
        def _():
            if p == turn:
                query_part(1).wait_recv()
                kept = [partial_softmax(p, 1, True, halo_stats)]
                query_part(0).wait_recv()
                first_keys()
                kept.insert(0, partial_softmax(p, 0, True, halo_stats))
            else:
                query_copy(p).wait_recv()
                kept = [partial_softmax(p, half, True, halo_stats) for half in range(2)]
            halo_copy(p).start()
            after_stats(p)
            if p == 0:
                local_copy().wait_recv()
            (p0, s0), (p1, s1) = (
                tile_probs(p, half, *kept[half], halo_stats, right_stats) for half in range(2)
            )
            k0, v0, q0 = tile_grads(p, 0, True, p0, s0)
            k1, v1, q1 = tile_grads(p, 1, True, p1, s1)
            for ref, a, b in ((own_k, k0, k1), (own_v, v0, v1)):
                ref[p, :BLK, :] = a[:BLK]
                ref[p, BLK:, :] = a[BLK:] + b
            back_q[p, :BLK, :] = q0.astype(BF16)
            back_q[p, BLK:, :] = q1.astype(BF16)
            square_ref[p, :BLK, :] = s0[:BLK] + s1
            square_ref[p, BLK:REACH, :] = s0[BLK:]

        @pl.when(jnp.logical_not(has_right))
        def _():
            after_stats(p)
            own_k[p] = jnp.zeros((rows, LANES), F32)
            own_v[p] = jnp.zeros((rows, LANES), F32)
            square_ref[p, :REACH, :] = jnp.zeros((REACH, 2 * BLK), F32)

        hop(p)

    def tally(p, square):
        for lane in range(2):
            head = 2 * p + lane
            sides = diagonals(
                square[:, lane * BLK : (lane + 1) * BLK],
                part * (head % wide) if direct else 0,
            )
            for side in range(2):
                pieces[side, head : head + 1] = sides[side]

    def local_probs(p):
        @pl.when(has_left)
        def _():
            halo_copy(p).wait_recv()

        (p0, s0), (p1, s1) = (
            tile_probs(
                p, half,
                grown_ref[p, places[half], :], dprob_ref[p, places[half], :],
                peak_ref[p, pl.ds(half, 1), :],
                local_stats, left_stats,
            )
            for half in range(2)
        )
        square = jnp.concatenate(
            [
                square_ref[p, :BLK, :],
                square_ref[p, BLK:REACH, :] + s1[:BLK],
                s0 + s1[BLK:],
            ],
            axis=0,
        )
        tally(p, square)
        return p0, s0, p1, s1

    def local_grads(p, p0, s0, p1, s1):
        cols = columns(p)
        k0, v0, q0 = tile_grads(p, 0, False, p0, s0)
        k1, v1, q1 = tile_grads(p, 1, False, p1, s1)
        for out, ref, a, b in ((dk_ref, own_k, k0, k1), (dv_ref, own_v, v0, v1)):
            out[:BLK, cols] = (ref[p, :BLK, :] + a + b[:BLK]).astype(BF16)
            out[BLK:, cols] = (ref[p, BLK:, :] + b[BLK:]).astype(BF16)
        own_q[p, :BLK, :] = q0
        own_q[p, BLK:, :] = q1

    def local(p):
        local_grads(p, *local_probs(p))

    gate = jnp.where(has_left, 0.0, NEG_FILL)

    def full(p, between=None):
        cols = columns(p)
        i = p - moved

        def arrived(block):
            @pl.when(has_left)
            def _():
                key_copy(p, block).wait_recv()

        def part_of(half, row, size, before):
            keys = pl.ds(half * BLK + row, size)
            qq, dd = queries(qd, p, half)
            scores = dot(kv[p, 0, keys], qq, NT) * LOG2E + bias_ref[p, pl.ds(row, size)]
            scores = (
                jnp.concatenate([scores[:before] + gate, scores[before:]], axis=0)
                if before < size
                else scores + gate
            )
            peak = jnp.max(scores, axis=0, keepdims=True)
            return scores, dot(kv[p, 1, keys], dd, NT), peak

        def moments(grown, dprobs):
            return (
                jnp.sum(grown, axis=0, keepdims=True),
                jnp.sum(grown * dprobs, axis=0, keepdims=True),
            )

        def half_grads(half, probs, dscores):
            qq, dd = queries(qd, p, half)
            return products(kv[p, 0, pl.ds(half * BLK, BAND)], qq, dd, probs, dscores)

        arrived(1)
        scores, dprobs, peak = part_of(1, 0, BAND, BLK)
        grown = jnp.exp2(scores - peak)
        total, inner = moments(grown, dprobs)
        inverse = 1.0 / total
        probs = grown * inverse
        s1 = probs * (dprobs - inner * inverse)
        k1, v1, q1 = half_grads(1, probs, s1)
        scores_a, dprobs_a, peak_a = part_of(0, BLK, 2 * BLK, BLK)
        grown_a = jnp.exp2(scores_a - peak_a)
        total_a, inner_a = moments(grown_a, dprobs_a)

        arrived(0)
        scores_b, dprobs_b, peak_b = part_of(0, 0, BLK, BLK)
        peak = jnp.maximum(peak_a, peak_b)
        grown_b = jnp.exp2(scores_b - peak)
        total_b, inner_b = moments(grown_b, dprobs_b)
        factor = jnp.exp2(peak_a - peak)
        inverse = 1.0 / (total_a * factor + total_b)
        inner = (inner_a * factor + inner_b) * inverse
        probs_a, probs_b = grown_a * (factor * inverse), grown_b * inverse
        p0 = jnp.concatenate([probs_b, probs_a], axis=0)
        s0 = jnp.concatenate(
            [probs_b * (dprobs_b - inner), probs_a * (dprobs_a - inner)], axis=0
        )
        tally(p, s0 + s1)
        if p == pairs - 1:
            send_back(moved - 1)
        if between is not None:
            between()
        k0, v0, q0 = half_grads(0, p0, s0)
        for which, ref, a, b in ((0, own_k, k0, k1), (1, own_v, v0, v1)):
            back_kv[i, which, :BLK, :] = a[:BLK].astype(BF16)
            back_kv[i, which, BLK:, :] = (a[BLK:REACH] + b[:BLK]).astype(BF16)
            ref[p, :BLK, :] = a[REACH:] + b[BLK:REACH]
            ref[p, BLK:, :] = b[REACH:]
        dq_ref[:BLK, cols] = q0.astype(BF16)
        dq_ref[BLK:, cols] = q1.astype(BF16)

    def piece_copy(k, t):
        target = lax.rem(me + k, sp_size)
        if direct:
            src, dst = packs.at[target], pack_got.at[col * sp_size + me]
        else:
            src, dst = pieces.at[target * part // CLIP], piece_got.at[k - 1]
        return pltpu.make_async_remote_copy(
            src_ref=src,
            dst_ref=dst,
            send_sem=send_sem.at[2],
            recv_sem=misc_recv.at[1],
            device_id=(target, lax.rem(col + t, tp_size)),
            device_id_type=MESH,
        )

    def all_pieces():
        ref = pack_got.at[pl.ds(1, sp_size * tp_size - 1)] if direct else piece_got
        return remote(ref, ref, 2, misc_recv.at[1], left)

    def share_copy(k):
        return pltpu.make_async_remote_copy(
            src_ref=shares.at[0],
            dst_ref=shares.at[k],
            send_sem=send_sem.at[3],
            recv_sem=misc_recv.at[2],
            device_id=(me, lax.rem(col + k, tp_size)),
            device_id_type=MESH,
        )

    def all_shares():
        rest = shares.at[pl.ds(1, tp_size - 1)]
        return remote(rest, rest, 3, misc_recv.at[2], left)

    def fold():
        block = lax.broadcasted_iota(jnp.int32, (folded, CLIP), 1) // part
        for side in range(2):
            lines = [pieces[side, pl.ds(j, folded, stride=wide), :] for j in range(wide)]
            for m in range(groups):
                pack = jnp.zeros((folded, CLIP), F32)
                for j in range(wide):
                    pack = jnp.where(block == (m + j) % groups, lines[j], pack)
                packs[side * groups + m] = pack

    def unfold():
        total = []
        for t in range(tp_size):
            line = pack_got[t * sp_size]
            for k in range(1, sp_size):
                line = line + pack_got[t * sp_size + k]
            total.append(line)
        total = jnp.concatenate(total, axis=0)
        for j in range(wide):
            away = lax.rem(me + j, groups) * part
            stack[pl.ds(j, folded * tp_size, stride=wide), :] = pltpu.roll(
                total, lax.rem(CLIP - away, CLIP), 1
            )
        dt_ref[...] = jnp.transpose(stack[...])[:part]

    def send_pieces():
        for r in range(moved, rounds + 1):
            hop(r)
        if direct:
            fold()
            pack_got[col * sp_size + me] = packs[me]
        for k in range(sp_size):
            for t in range(tp_size if direct else 1):
                if k or t:
                    piece_copy(k, t).start()

    for p in range(moved):
        halo(p)
        if p:
            local(p - 1)
    last = pairs - 1
    for p in range(moved, last):
        full(p)
        send_back(p)
        if p == moved:
            local(moved - 1)
    kept = []

    def finish_pieces():
        if moved == last:
            kept.extend(local_probs(moved - 1))
        send_pieces()

    full(last, finish_pieces)
    send_back(last)
    if kept:
        local_grads(moved - 1, *kept)

    def finish(p):
        cols = pl.ds(p * LANES, LANES)
        if p < moved:
            @pl.when(has_left)
            def _():
                if p == moved - 1:
                    back_copy(p).wait_recv()
                elif p == 0:
                    early_back().wait_recv()
                dq_ref[:, cols] = (own_q[p] + got_q[p].astype(F32)).astype(BF16)

            @pl.when(jnp.logical_not(has_left))
            def _():
                dq_ref[:, cols] = own_q[p].astype(BF16)
        else:
            i = p - moved

            @pl.when(has_right)
            def _():
                key_back_copy(p).wait_recv()
                dk_ref[:, cols] = (own_k[p] + got_kv[i, 0].astype(F32)).astype(BF16)
                dv_ref[:, cols] = (own_v[p] + got_kv[i, 1].astype(F32)).astype(BF16)

            @pl.when(jnp.logical_not(has_right))
            def _():
                dk_ref[:, cols] = own_k[p].astype(BF16)
                dv_ref[:, cols] = own_v[p].astype(BF16)

    if direct:
        for p in range(pairs):
            finish(p)
    all_pieces().wait_recv()
    if direct:
        unfold()
    else:
        total = pieces[me * part // CLIP]
        for k in range(1, sp_size):
            total = total + piece_got[k - 1]
        shares[0] = pltpu.roll(total, lax.rem(CLIP - lax.rem(me * part, CLIP), CLIP), 1)
        for k in range(1, tp_size):
            share_copy(k).start()
    if not direct:
        for p in range(pairs):
            finish(p)
        all_shares().wait_recv()
        stacked = jnp.concatenate(
            [shares[lax.rem(col + tp_size - t, tp_size)] for t in range(tp_size)], axis=0
        )
        dt_ref[...] = jnp.transpose(stacked)[:part]
        all_shares().wait_send()

    all_pieces().wait_send()

    @pl.when(has_left)
    def _():
        all_queries().wait_send()
        local_copy().wait_send()
        remote(back_kv, got_kv, LEFTWARD, misc_recv.at[0], left).wait_send()

    @pl.when(has_right)
    def _():
        all_keys().wait_send()
        remote(halo_stats, left_stats, RIGHTWARD, misc_recv.at[0], right).wait_send()
        remote(back_q, got_q, RIGHTWARD, misc_recv.at[0], right).wait_send()


def shards(sp_size, tp_size, query_rows, key_rows, value_rows, out_grad, rel_bias):
    rows, width = query_rows.shape
    pairs = width // LANES
    heads = width // HEAD_DIM
    part = 2 * CLIP // sp_size
    moved = pairs - 1
    rounds = (sp_size - 1).bit_length()
    direct = sp_size * tp_size <= 64 and part <= CLIP and heads % (CLIP // part) == 0
    folded = heads * part // CLIP
    exchange = [
        pltpu.VMEM(shape, F32)
        for shape in (
            (
                (sp_size, folded, CLIP),
                (sp_size * tp_size, folded, CLIP),
                (tp_size * heads, CLIP),
            )
            if direct
            else ((sp_size - 1, heads, CLIP), (tp_size, heads, CLIP), (8, CLIP))
        )
    ]
    assert rows == REACH and REACH == 2 * BLK and CLIP == BLK
    like = jax.ShapeDtypeStruct((rows, width), BF16)
    dma = pltpu.SemaphoreType.DMA
    shapes = (like, like, like, jax.ShapeDtypeStruct((part, heads * tp_size), F32))
    results = pl.pallas_call(
        partial(kernel, sp_size, tp_size, moved, direct),
        out_shape=shapes,
        in_specs=[pl.BlockSpec(memory_space=pltpu.HBM)] * 5,
        out_specs=tuple([pl.BlockSpec(memory_space=pltpu.VMEM)] * 4),
        scratch_shapes=[
            pltpu.VMEM((pairs, 2, rows, LANES), BF16),
            pltpu.VMEM((moved, 2, rows, LANES), BF16),
            pltpu.VMEM((pairs, 2, 2 * rows, LANES), BF16),
            pltpu.VMEM((pairs, BAND, 2 * BLK), F32),
            pltpu.VMEM((moved, REACH, 2 * BLK), F32),
            pltpu.VMEM((moved, BAND, 2 * BLK), F32),
            pltpu.VMEM((moved, BAND, 2 * BLK), F32),
            pltpu.VMEM((moved, 8, 2 * BLK), F32),
            pltpu.VMEM((pairs, rows, LANES), F32),
            pltpu.VMEM((pairs, rows, LANES), F32),
            pltpu.VMEM((moved, rows, LANES), F32),
            pltpu.VMEM((moved, rows, LANES), BF16),
            pltpu.VMEM((moved, rows, LANES), BF16),
            pltpu.VMEM((pairs - moved, 2, rows, LANES), BF16),
            pltpu.VMEM((pairs - moved, 2, rows, LANES), BF16),
            pltpu.VMEM((moved, 8, BLK), F32),
            pltpu.VMEM((moved, 8, BLK), F32),
            pltpu.VMEM((moved, 8, BLK), F32),
            pltpu.VMEM((moved, 8, BLK), F32),
            pltpu.VMEM(rel_bias.shape[::-1], F32),
            pltpu.VMEM((2, heads, BLK), F32),
            *exchange,
            dma((4,)),
            pltpu.SemaphoreType.REGULAR((rounds + 1,)),
            dma((3 if direct else 4,)),
            dma((2 * pairs - moved + 1,)),
            dma((2 + pairs - moved,)),
            dma((moved,)),
            dma((2 if direct else 3,)),
        ],
        compiler_params=pltpu.CompilerParams(
            collective_id=0, has_side_effects=True, vmem_limit_bytes=48 * 1024 * 1024
        ),
    )(*[pltpu.with_memory_space_constraint(x, pltpu.HBM) for x in (query_rows, key_rows, value_rows, out_grad, jnp.transpose(rel_bias))])
    return pl.pallas_call(
        write_out,
        out_shape=shapes,
        in_specs=[pl.BlockSpec(memory_space=pl.ANY)] * 4,
        out_specs=tuple([pl.BlockSpec(memory_space=pltpu.HBM)] * 4),
        scratch_shapes=[dma((4,))],
        compiler_params=pltpu.CompilerParams(vmem_limit_bytes=1024 * 1024),
    )(*results)


def write_out(*refs):
    sem = refs[-1]
    copies = [pltpu.make_async_copy(refs[i], refs[4 + i], sem.at[i]) for i in range(4)]
    for copy in copies:
        copy.start()
    for copy in copies:
        copy.wait()


def solution(mesh):
    return jax.shard_map(
        partial(shards, mesh.shape["sp"], mesh.shape["tp"]),
        mesh=mesh,
        in_specs=(P("sp", "tp"), P("sp", "tp"), P("sp", "tp"), P("sp", "tp"), P()),
        out_specs=(P("sp", "tp"), P("sp", "tp"), P("sp", "tp"), P("sp", None)),
        check_vma=False,
    )
```

```python
from functools import partial
import math

import jax
import jax.numpy as jnp
from jax import lax
from jax.experimental import pallas as pl
from jax.experimental.pallas import tpu as pltpu
from jax.sharding import PartitionSpec as P

HEAD_DIM = 64
SEG = 64
LEFT = 4
CLIP = 128

LANES = 2 * HEAD_DIM
REACH = LEFT * SEG
BLK = 2 * SEG
BAND = REACH + BLK
WRAP = 3 * BLK
NEG_FILL = -1e30
LOG2E = math.log2(math.e)
MESH = pl.DeviceIdType.MESH
LEFTWARD, RIGHTWARD = 0, 1
F32 = jnp.float32
BF16 = jnp.bfloat16

NT = (((1,), (1,)), ((), ()))
NN = (((1,), (0,)), ((), ()))
TN = (((0,), (0,)), ((), ()))


def dot(a, b, dims):
    return lax.dot_general(a, b, dims, preferred_element_type=F32)


def turned(x, amount):
    amount %= x.shape[1]
    return pltpu.roll(x, amount, 1) if amount else x


def grid(axis):
    return lax.broadcasted_iota(jnp.int32, (BLK, BLK), axis)


def build_bias(table_row, bias_ref, pair, lane):
    def shear(half):
        return pltpu.roll(
            jnp.broadcast_to(half, (BLK, BLK)), 0, 1, stride=1, stride_axis=0
        )

    ahead, behind = shear(table_row[:, CLIP:]), shear(table_row[:, :CLIP])
    flat = jnp.broadcast_to(table_row[:, 2 * CLIP - 1 :], (BLK, BLK))
    key, query = grid(0), grid(1)
    later = query >= key
    cols = pl.ds(lane * BLK, BLK)
    bias_ref[pair, :BLK, cols] = jnp.where((key < SEG) & (query >= SEG), NEG_FILL, flat)
    bias_ref[pair, BLK : 2 * BLK, cols] = jnp.where(later, flat, ahead)
    bias_ref[pair, 2 * BLK :, cols] = jnp.where(
        (key >= SEG) & (query < SEG), NEG_FILL, jnp.where(later, ahead, behind)
    )


def unshear(square, shift):
    parts = [turned(square[8 * g : 8 * g + 8], -8 * g) for g in range(BLK // 8)]
    while len(parts) > 1:
        parts = [a + b for a, b in zip(parts[::2], parts[1::2])]
    row = lax.broadcasted_iota(jnp.int32, (8, BLK), 0)
    result = turned(parts[0], shift)
    for i in range(1, 8):
        result = jnp.where(row == i, turned(parts[0], shift - i), result)
    return jnp.sum(result, axis=0, keepdims=True)


def diagonals(square, shift):
    top, far, near = square[:BLK], square[BLK : 2 * BLK], square[2 * BLK :]
    later = grid(1) >= grid(0)
    beyond = jnp.sum(top + jnp.where(later, far, 0.0), axis=0, keepdims=True)
    spot = lax.broadcasted_iota(jnp.int32, (1, BLK), 1)
    clipped = jnp.where(
        spot == (BLK - 1 + shift) % BLK, jnp.sum(beyond, axis=1, keepdims=True), 0.0
    )
    return (
        unshear(jnp.where(later, 0.0, near), shift),
        unshear(jnp.where(later, near, far), shift) + clipped,
    )


def kernel(
    sp_size, tp_size, moved, direct,
    q_hbm, k_hbm, v_hbm, d_hbm, table_hbm,
    dq_ref, dk_ref, dv_ref, dt_ref,
    qd, got_qd, kv, bias_ref, square_ref, grown_ref, dprob_ref, peak_ref,
    own_k, own_v, own_q, back_q, got_q, back_kv, got_kv,
    local_stats, right_stats, halo_stats, left_stats,
    table_rows, pieces, exchange_a, exchange_b, exchange_c,
    load_sem, hop_sem, send_sem, seq_recv, back_recv, halo_recv, misc_recv,
):
    if direct:
        packs, pack_got, stack = exchange_a, exchange_b, exchange_c
    else:
        piece_got, shares = exchange_a, exchange_b
    rows, width = q_hbm.shape
    pairs = width // LANES
    heads = width // HEAD_DIM
    part = 2 * CLIP // sp_size
    me = lax.axis_index("sp")
    col = lax.axis_index("tp")
    has_left = me > 0
    has_right = me < sp_size - 1
    left = jnp.maximum(me - 1, 0)
    right = jnp.minimum(me + 1, sp_size - 1)
    prev, own = pl.ds(0, rows), pl.ds(rows, rows)

    def columns(p):
        return pl.ds(p * LANES, LANES)

    barrier = pltpu.get_barrier_semaphore()

    def greet(sem, step):
        @pl.when(me >= step)
        def _():
            pl.semaphore_signal(sem, inc=1, device_id=(me - step, col), device_id_type=MESH)

        @pl.when(me + step < sp_size)
        def _():
            pl.semaphore_signal(sem, inc=1, device_id=(me + step, col), device_id_type=MESH)

    def greeters(step):
        return (me >= step).astype(jnp.int32) + (me + step < sp_size).astype(jnp.int32)

    @pl.when(has_right)
    def _():
        pl.semaphore_signal(barrier, inc=1, device_id=(me + 1, col), device_id_type=MESH)

    for k in range(1, tp_size):
        pl.semaphore_signal(
            barrier, inc=1, device_id=(me, lax.rem(col + k, tp_size)), device_id_type=MESH
        )

    for p in range(pairs):
        for i, src in enumerate((q_hbm, d_hbm)):
            pltpu.make_async_copy(src.at[:, columns(p)], qd.at[p, i], load_sem.at[2 + (p > 0)]).start()
    pltpu.make_async_copy(table_hbm, table_rows, load_sem.at[0]).start()
    for p in range(pairs):
        for i, src in enumerate((k_hbm, v_hbm)):
            pltpu.make_async_copy(src.at[:, columns(p)], kv.at[p, i, own], load_sem.at[1]).start()

    rounds = hop_sem.shape[0] - 1

    def hop(r):
        if 0 < r <= rounds:
            pl.semaphore_wait(hop_sem.at[r - 1], greeters(1 << (r - 1)))
        if r < rounds:
            greet(hop_sem.at[r], 1 << r)

    def remote(src, dst, send, recv, target):
        return pltpu.make_async_remote_copy(
            src_ref=src,
            dst_ref=dst,
            send_sem=send_sem.at[send],
            recv_sem=recv,
            device_id=(target, col),
            device_id_type=MESH,
        )

    def query_copy(p):
        return remote(qd.at[p], got_qd.at[p], LEFTWARD, seq_recv.at[p], left)

    turn, last = max(moved - 2, 0), pairs - 1

    def query_part(half):
        mine = pl.ds(SEG, rows - SEG) if half else pl.ds(0, SEG)
        recv = seq_recv.at[turn if half else 2 * pairs - moved]
        return remote(qd.at[turn, :, mine], got_qd.at[turn, :, mine], LEFTWARD, recv, left)

    def all_queries():
        return remote(qd.at[pl.ds(0, moved)], got_qd, LEFTWARD, misc_recv.at[0], left)

    def key_copy(p, block):
        return remote(
            kv.at[p, :, pl.ds(rows + block * BLK, BLK)],
            kv.at[p, :, pl.ds(block * BLK, BLK)],
            RIGHTWARD,
            seq_recv.at[p + block * (pairs - moved)],
            right,
        )

    def all_keys():
        keyed = pl.ds(moved, pairs - moved)
        return remote(kv.at[keyed, :, own], kv.at[keyed, :, prev], RIGHTWARD, misc_recv.at[0], right)

    def local_copy():
        return remote(local_stats, right_stats, LEFTWARD, misc_recv.at[0], left)

    def halo_copy(p):
        return remote(halo_stats.at[p], left_stats.at[p], RIGHTWARD, halo_recv.at[p], right)

    def back_copy(p):
        recv = back_recv.at[int(p == moved - 1)]
        return remote(back_q.at[p], got_q.at[p], RIGHTWARD, recv, right)

    def early_back():
        some = pl.ds(0, max(moved - 1, 1))
        return remote(back_q.at[some], got_q.at[some], RIGHTWARD, back_recv.at[0], right)

    def key_back_copy(p):
        i = p - moved
        return remote(back_kv.at[i], got_kv.at[i], LEFTWARD, back_recv.at[2 + i], left)

    def send_queries(p):
        @pl.when(has_left)
        def _():
            if p == turn:
                query_part(1).start()
                query_part(0).start()
            else:
                query_copy(p).start()

    def send_back(p):
        if p < moved:
            @pl.when(has_right)
            def _():
                back_copy(p).start()
        else:
            @pl.when(has_left)
            def _():
                key_back_copy(p).start()

    def load_wait(refs, sem):
        pltpu.make_async_copy(refs, refs, sem).wait()

    pl.semaphore_wait(barrier, has_left.astype(jnp.int32) + tp_size - 1)
    load_wait(qd.at[0], load_sem.at[2])
    send_queries(0)

    @pl.when(jnp.logical_not(has_left))
    def _():
        spot = lax.broadcasted_iota(jnp.int32, left_stats.shape, 1)
        left_stats[...] = jnp.where((spot & 2) == 0, NEG_FILL, 0.0)
        kv[moved:, :, prev] = jnp.zeros((pairs - moved, 2, rows, LANES), BF16)

    load_wait(table_rows, load_sem.at[0])
    for h in range(heads):
        row = table_rows[pl.ds(col * heads + h, 1), :] * LOG2E
        build_bias(row, bias_ref, h // 2, h % 2)

    load_wait(qd.at[pl.ds(1, pairs - 1)], load_sem.at[3])
    load_wait(kv.at[:, :, own], load_sem.at[1])

    low = lax.broadcasted_iota(jnp.int32, (BLK, LANES), 1) < HEAD_DIM
    scale = HEAD_DIM ** -0.5
    groups = CLIP // part
    folded = exchange_a.shape[1]
    wide = heads // folded

    def split(x):
        zero = jnp.zeros_like(x)
        return jnp.concatenate([jnp.where(low, x, zero), jnp.where(low, zero, x)], axis=0)

    def queries(ref, p, half):
        mine = pl.ds(half * BLK, BLK)
        return split(ref[p, 0, mine] * jnp.asarray(scale, BF16)), split(ref[p, 1, mine])

    def tile(p, half, halo):
        start, size, row = (
            (half * BLK, REACH - half * BLK, 0)
            if halo
            else (0, (half + 1) * BLK, REACH - half * BLK)
        )
        keys = pl.ds(rows + start, size)
        ref = got_qd if halo else qd
        return kv[p, 0, keys], kv[p, 1, keys], *queries(ref, p, half), pl.ds(row, size)

    def put(stats, p, half, which, value):
        for lane in range(2):
            spot = pl.ds(half * 4 + which * 2 + lane, 1)
            stats[p, spot, :] = value[:, lane * BLK : (lane + 1) * BLK]

    def get(stats, p, half, which):
        spots = [pl.ds(half * 4 + which * 2 + lane, 1) for lane in range(2)]
        return jnp.concatenate([stats[p, spot, :] for spot in spots], axis=1)

    def partial_softmax(p, half, halo, stats):
        k_blk, v_blk, qq, dd, band = tile(p, half, halo)
        scores = dot(k_blk, qq, NT) * LOG2E + bias_ref[p, band]
        dprobs = dot(v_blk, dd, NT)
        peak = jnp.max(scores, axis=0, keepdims=True)
        grown = jnp.exp2(scores - peak)
        total = jnp.sum(grown, axis=0, keepdims=True)
        put(stats, p, half, 0, peak + jnp.log2(total))
        put(stats, p, half, 1, jnp.sum(grown * dprobs, axis=0, keepdims=True) / total)
        return grown, dprobs, peak

    def products(k_blk, qq, dd, probs, dscores):
        ds_half = dscores.astype(BF16)
        flat = dot(k_blk, ds_half, TN)
        both = jnp.concatenate([flat[:HEAD_DIM, :BLK], flat[HEAD_DIM:, BLK:]], axis=0)
        return (
            dot(ds_half, qq, NN),
            dot(probs.astype(BF16), dd, NN),
            jnp.transpose(both) * scale,
        )

    def tile_probs(p, half, grown, dprobs, peak, stats, others):
        n1, i1 = get(stats, p, half, 0), get(stats, p, half, 1)
        n2, i2 = get(others, p, half, 0), get(others, p, half, 1)
        top = jnp.maximum(n1, n2)
        a1, a2 = jnp.exp2(n1 - top), jnp.exp2(n2 - top)
        inverse = 1.0 / (a1 + a2)
        inner = (i1 * a1 + i2 * a2) * inverse
        probs = grown * (jnp.exp2(peak - top) * inverse)
        return probs, probs * (dprobs - inner)

    def tile_grads(p, half, halo, probs, dscores):
        k_blk, _, qq, dd, _ = tile(p, half, halo)
        return products(k_blk, qq, dd, probs, dscores)

    places = (pl.ds(0, BLK), pl.ds(BLK, 2 * BLK))
    for p in range(moved):
        for half in range(2):
            grown, dprobs, peak = partial_softmax(p, half, False, local_stats)
            grown_ref[p, places[half], :] = grown
            dprob_ref[p, places[half], :] = dprobs
            peak_ref[p, pl.ds(half, 1), :] = peak

    @pl.when(has_left)
    def _():
        local_copy().start()

    if moved > 1:
        send_queries(1)

    even = lax.rem(me, 2) == 0
    core = lax.rem(col, 2)
    early = has_right & (even | (core == 0))
    keyed = [(p, block) for p in range(moved, pairs) for block in (1, 0)]

    def send_keys(blocks):
        for p, block in blocks:
            key_copy(p, block).start()

    def first_keys():
        @pl.when(has_right & jnp.logical_not(even) & (core == 0))
        def _():
            pl.semaphore_signal(
                hop_sem.at[rounds], inc=1, device_id=(me, col + 1), device_id_type=MESH
            )

        @pl.when(early)
        def _():
            send_keys(keyed[:1])

    def after_stats(p):
        if p + 2 < moved:
            send_queries(p + 2)
        if p == turn:
            @pl.when(early)
            def _():
                send_keys(keyed[1:])

            @pl.when(has_right & jnp.logical_not(early))
            def _():
                pl.semaphore_wait(hop_sem.at[rounds], 1)
                send_keys(keyed)

        if p == moved - 1:
            for done in range(p):
                send_back(done)

    def halo(p):
        @pl.when(has_right)
        def _():
            if p == turn:
                query_part(1).wait_recv()
                kept = [partial_softmax(p, 1, True, halo_stats)]
                first_keys()
                query_part(0).wait_recv()
                kept.insert(0, partial_softmax(p, 0, True, halo_stats))
            else:
                query_copy(p).wait_recv()
                kept = [partial_softmax(p, half, True, halo_stats) for half in range(2)]
            halo_copy(p).start()
            after_stats(p)
            hop(p)
            if p == 0:
                local_copy().wait_recv()
            (p0, s0), (p1, s1) = (
                tile_probs(p, half, *kept[half], halo_stats, right_stats) for half in range(2)
            )
            k0, v0, q0 = tile_grads(p, 0, True, p0, s0)
            k1, v1, q1 = tile_grads(p, 1, True, p1, s1)
            for ref, a, b in ((own_k, k0, k1), (own_v, v0, v1)):
                ref[p, :BLK, :] = a[:BLK]
                ref[p, BLK:, :] = a[BLK:] + b
            back_q[p, :BLK, :] = q0.astype(BF16)
            back_q[p, BLK:, :] = q1.astype(BF16)
            square_ref[p, :BLK, :] = s0[:BLK] + s1
            square_ref[p, BLK:REACH, :] = s0[BLK:]

        @pl.when(jnp.logical_not(has_right))
        def _():
            after_stats(p)
            hop(p)
            own_k[p] = jnp.zeros((rows, LANES), F32)
            own_v[p] = jnp.zeros((rows, LANES), F32)
            square_ref[p, :REACH, :] = jnp.zeros((REACH, 2 * BLK), F32)

    def tally(p, square):
        for lane in range(2):
            head = 2 * p + lane
            sides = diagonals(
                square[:, lane * BLK : (lane + 1) * BLK],
                part * (head % wide) if direct else 0,
            )
            for side in range(2):
                pieces[side, head : head + 1] = sides[side]

    def local_probs(p):
        @pl.when(has_left)
        def _():
            halo_copy(p).wait_recv()

        (p0, s0), (p1, s1) = (
            tile_probs(
                p, half,
                grown_ref[p, places[half], :], dprob_ref[p, places[half], :],
                peak_ref[p, pl.ds(half, 1), :],
                local_stats, left_stats,
            )
            for half in range(2)
        )
        square = jnp.concatenate(
            [
                square_ref[p, :BLK, :],
                square_ref[p, BLK:REACH, :] + s1[:BLK],
                s0 + s1[BLK:],
            ],
            axis=0,
        )
        tally(p, square)
        return p0, s0, p1, s1

    def local_grads(p, p0, s0, p1, s1):
        cols = columns(p)
        k0, v0, q0 = tile_grads(p, 0, False, p0, s0)
        k1, v1, q1 = tile_grads(p, 1, False, p1, s1)
        for out, ref, a, b in ((dk_ref, own_k, k0, k1), (dv_ref, own_v, v0, v1)):
            out[:BLK, cols] = (ref[p, :BLK, :] + a + b[:BLK]).astype(BF16)
            out[BLK:, cols] = (ref[p, BLK:, :] + b[BLK:]).astype(BF16)
        own_q[p, :BLK, :] = q0
        own_q[p, BLK:, :] = q1

    def local(p):
        local_grads(p, *local_probs(p))

    gate = jnp.where(has_left, 0.0, NEG_FILL)

    def full(p, between=None):
        cols = columns(p)
        i = p - moved

        def arrived(block):
            @pl.when(has_left)
            def _():
                key_copy(p, block).wait_recv()

        def part_of(half, row, size, before):
            keys = pl.ds(half * BLK + row, size)
            qq, dd = queries(qd, p, half)
            scores = dot(kv[p, 0, keys], qq, NT) * LOG2E + bias_ref[p, pl.ds(row, size)]
            scores = (
                jnp.concatenate([scores[:before] + gate, scores[before:]], axis=0)
                if before < size
                else scores + gate
            )
            peak = jnp.max(scores, axis=0, keepdims=True)
            return scores, dot(kv[p, 1, keys], dd, NT), peak

        def moments(grown, dprobs):
            return (
                jnp.sum(grown, axis=0, keepdims=True),
                jnp.sum(grown * dprobs, axis=0, keepdims=True),
            )

        def half_grads(half, probs, dscores):
            qq, dd = queries(qd, p, half)
            return products(kv[p, 0, pl.ds(half * BLK, BAND)], qq, dd, probs, dscores)

        arrived(1)
        scores, dprobs, peak = part_of(1, 0, BAND, BLK)
        grown = jnp.exp2(scores - peak)
        total, inner = moments(grown, dprobs)
        inverse = 1.0 / total
        probs = grown * inverse
        s1 = probs * (dprobs - inner * inverse)
        k1, v1, q1 = half_grads(1, probs, s1)
        scores_a, dprobs_a, peak_a = part_of(0, BLK, 2 * BLK, BLK)
        grown_a = jnp.exp2(scores_a - peak_a)
        total_a, inner_a = moments(grown_a, dprobs_a)

        arrived(0)
        scores_b, dprobs_b, peak_b = part_of(0, 0, BLK, BLK)
        peak = jnp.maximum(peak_a, peak_b)
        grown_b = jnp.exp2(scores_b - peak)
        total_b, inner_b = moments(grown_b, dprobs_b)
        factor = jnp.exp2(peak_a - peak)
        inverse = 1.0 / (total_a * factor + total_b)
        inner = (inner_a * factor + inner_b) * inverse
        probs_a, probs_b = grown_a * (factor * inverse), grown_b * inverse
        p0 = jnp.concatenate([probs_b, probs_a], axis=0)
        s0 = jnp.concatenate(
            [probs_b * (dprobs_b - inner), probs_a * (dprobs_a - inner)], axis=0
        )
        tally(p, s0 + s1)
        if p == pairs - 1:
            send_back(moved - 1)
        if between is not None:
            between()
        k0, v0, q0 = half_grads(0, p0, s0)
        for which, ref, a, b in ((0, own_k, k0, k1), (1, own_v, v0, v1)):
            back_kv[i, which, :BLK, :] = a[:BLK].astype(BF16)
            back_kv[i, which, BLK:, :] = (a[BLK:REACH] + b[:BLK]).astype(BF16)
            ref[p, :BLK, :] = a[REACH:] + b[BLK:REACH]
            ref[p, BLK:, :] = b[REACH:]
        dq_ref[:BLK, cols] = q0.astype(BF16)
        dq_ref[BLK:, cols] = q1.astype(BF16)

    def piece_copy(k, t):
        target = lax.rem(me + k, sp_size)
        if direct:
            src, dst = packs.at[target], pack_got.at[col * sp_size + me]
        else:
            src, dst = pieces.at[target * part // CLIP], piece_got.at[k - 1]
        return pltpu.make_async_remote_copy(
            src_ref=src,
            dst_ref=dst,
            send_sem=send_sem.at[2],
            recv_sem=misc_recv.at[1],
            device_id=(target, lax.rem(col + t, tp_size)),
            device_id_type=MESH,
        )

    def all_pieces():
        ref = pack_got.at[pl.ds(1, sp_size * tp_size - 1)] if direct else piece_got
        return remote(ref, ref, 2, misc_recv.at[1], left)

    def share_copy(k):
        return pltpu.make_async_remote_copy(
            src_ref=shares.at[0],
            dst_ref=shares.at[k],
            send_sem=send_sem.at[3],
            recv_sem=misc_recv.at[2],
            device_id=(me, lax.rem(col + k, tp_size)),
            device_id_type=MESH,
        )

    def all_shares():
        rest = shares.at[pl.ds(1, tp_size - 1)]
        return remote(rest, rest, 3, misc_recv.at[2], left)

    def fold():
        block = lax.broadcasted_iota(jnp.int32, (folded, CLIP), 1) // part
        for side in range(2):
            lines = [pieces[side, pl.ds(j, folded, stride=wide), :] for j in range(wide)]
            for m in range(groups):
                pack = jnp.zeros((folded, CLIP), F32)
                for j in range(wide):
                    pack = jnp.where(block == (m + j) % groups, lines[j], pack)
                packs[side * groups + m] = pack

    def unfold():
        total = []
        for t in range(tp_size):
            line = pack_got[t * sp_size]
            for k in range(1, sp_size):
                line = line + pack_got[t * sp_size + k]
            total.append(line)
        total = jnp.concatenate(total, axis=0)
        for j in range(wide):
            away = lax.rem(me + j, groups) * part
            stack[pl.ds(j, folded * tp_size, stride=wide), :] = pltpu.roll(
                total, lax.rem(CLIP - away, CLIP), 1
            )
        dt_ref[...] = jnp.transpose(stack[...])[:part]

    def send_pieces():
        for r in range(moved, rounds + 1):
            hop(r)
        if direct:
            fold()
            pack_got[col * sp_size + me] = packs[me]
        for k in range(sp_size):
            for t in range(tp_size if direct else 1):
                if k or t:
                    piece_copy(k, t).start()

    for p in range(moved):
        halo(p)
        if p:
            local(p - 1)
    for p in range(moved, last):
        full(p)
        send_back(p)
        if p == moved:
            local(moved - 1)
    kept = []

    def finish_pieces():
        if moved == last:
            kept.extend(local_probs(moved - 1))
        send_pieces()

    full(last, finish_pieces)
    send_back(last)
    if kept:
        local_grads(moved - 1, *kept)

    def finish(p):
        cols = pl.ds(p * LANES, LANES)
        if p < moved:
            @pl.when(has_left)
            def _():
                if p == moved - 1:
                    back_copy(p).wait_recv()
                elif p == 0:
                    early_back().wait_recv()
                dq_ref[:, cols] = (own_q[p] + got_q[p].astype(F32)).astype(BF16)

            @pl.when(jnp.logical_not(has_left))
            def _():
                dq_ref[:, cols] = own_q[p].astype(BF16)
        else:
            i = p - moved

            @pl.when(has_right)
            def _():
                key_back_copy(p).wait_recv()
                dk_ref[:, cols] = (own_k[p] + got_kv[i, 0].astype(F32)).astype(BF16)
                dv_ref[:, cols] = (own_v[p] + got_kv[i, 1].astype(F32)).astype(BF16)

            @pl.when(jnp.logical_not(has_right))
            def _():
                dk_ref[:, cols] = own_k[p].astype(BF16)
                dv_ref[:, cols] = own_v[p].astype(BF16)

    if direct:
        for p in range(pairs):
            finish(p)
    all_pieces().wait_recv()
    if direct:
        unfold()
    else:
        total = pieces[me * part // CLIP]
        for k in range(1, sp_size):
            total = total + piece_got[k - 1]
        shares[0] = pltpu.roll(total, lax.rem(CLIP - lax.rem(me * part, CLIP), CLIP), 1)
        for k in range(1, tp_size):
            share_copy(k).start()
    if not direct:
        for p in range(pairs):
            finish(p)
        all_shares().wait_recv()
        stacked = jnp.concatenate(
            [shares[lax.rem(col + tp_size - t, tp_size)] for t in range(tp_size)], axis=0
        )
        dt_ref[...] = jnp.transpose(stacked)[:part]
        all_shares().wait_send()

    all_pieces().wait_send()

    @pl.when(has_left)
    def _():
        all_queries().wait_send()
        local_copy().wait_send()
        remote(back_kv, got_kv, LEFTWARD, misc_recv.at[0], left).wait_send()

    @pl.when(has_right)
    def _():
        all_keys().wait_send()
        remote(halo_stats, left_stats, RIGHTWARD, misc_recv.at[0], right).wait_send()
        remote(back_q, got_q, RIGHTWARD, misc_recv.at[0], right).wait_send()


def shards(sp_size, tp_size, query_rows, key_rows, value_rows, out_grad, rel_bias):
    rows, width = query_rows.shape
    pairs = width // LANES
    heads = width // HEAD_DIM
    part = 2 * CLIP // sp_size
    moved = pairs - 1
    rounds = (sp_size - 1).bit_length()
    direct = sp_size * tp_size <= 64 and part <= CLIP and heads % (CLIP // part) == 0
    folded = heads * part // CLIP
    exchange = [
        pltpu.VMEM(shape, F32)
        for shape in (
            (
                (sp_size, folded, CLIP),
                (sp_size * tp_size, folded, CLIP),
                (tp_size * heads, CLIP),
            )
            if direct
            else ((sp_size - 1, heads, CLIP), (tp_size, heads, CLIP), (8, CLIP))
        )
    ]
    assert rows == REACH and REACH == 2 * BLK and CLIP == BLK
    like = jax.ShapeDtypeStruct((rows, width), BF16)
    dma = pltpu.SemaphoreType.DMA
    shapes = (like, like, like, jax.ShapeDtypeStruct((part, heads * tp_size), F32))
    results = pl.pallas_call(
        partial(kernel, sp_size, tp_size, moved, direct),
        out_shape=shapes,
        in_specs=[pl.BlockSpec(memory_space=pltpu.HBM)] * 5,
        out_specs=tuple([pl.BlockSpec(memory_space=pltpu.VMEM)] * 4),
        scratch_shapes=[
            pltpu.VMEM((pairs, 2, rows, LANES), BF16),
            pltpu.VMEM((moved, 2, rows, LANES), BF16),
            pltpu.VMEM((pairs, 2, 2 * rows, LANES), BF16),
            pltpu.VMEM((pairs, BAND, 2 * BLK), F32),
            pltpu.VMEM((moved, REACH, 2 * BLK), F32),
            pltpu.VMEM((moved, BAND, 2 * BLK), F32),
            pltpu.VMEM((moved, BAND, 2 * BLK), F32),
            pltpu.VMEM((moved, 8, 2 * BLK), F32),
            pltpu.VMEM((pairs, rows, LANES), F32),
            pltpu.VMEM((pairs, rows, LANES), F32),
            pltpu.VMEM((moved, rows, LANES), F32),
            pltpu.VMEM((moved, rows, LANES), BF16),
            pltpu.VMEM((moved, rows, LANES), BF16),
            pltpu.VMEM((pairs - moved, 2, rows, LANES), BF16),
            pltpu.VMEM((pairs - moved, 2, rows, LANES), BF16),
            pltpu.VMEM((moved, 8, BLK), F32),
            pltpu.VMEM((moved, 8, BLK), F32),
            pltpu.VMEM((moved, 8, BLK), F32),
            pltpu.VMEM((moved, 8, BLK), F32),
            pltpu.VMEM(rel_bias.shape[::-1], F32),
            pltpu.VMEM((2, heads, BLK), F32),
            *exchange,
            dma((4,)),
            pltpu.SemaphoreType.REGULAR((rounds + 1,)),
            dma((3 if direct else 4,)),
            dma((2 * pairs - moved + 1,)),
            dma((2 + pairs - moved,)),
            dma((moved,)),
            dma((2 if direct else 3,)),
        ],
        compiler_params=pltpu.CompilerParams(
            collective_id=0, has_side_effects=True, vmem_limit_bytes=48 * 1024 * 1024
        ),
    )(*[pltpu.with_memory_space_constraint(x, pltpu.HBM) for x in (query_rows, key_rows, value_rows, out_grad, jnp.transpose(rel_bias))])
    return pl.pallas_call(
        write_out,
        out_shape=shapes,
        in_specs=[pl.BlockSpec(memory_space=pl.ANY)] * 4,
        out_specs=tuple([pl.BlockSpec(memory_space=pltpu.HBM)] * 4),
        scratch_shapes=[dma((4,))],
        compiler_params=pltpu.CompilerParams(vmem_limit_bytes=1024 * 1024),
    )(*results)


def write_out(*refs):
    sem = refs[-1]
    copies = [pltpu.make_async_copy(refs[i], refs[4 + i], sem.at[i]) for i in range(4)]
    for copy in copies:
        copy.start()
    for copy in copies:
        copy.wait()


def solution(mesh):
    return jax.shard_map(
        partial(shards, mesh.shape["sp"], mesh.shape["tp"]),
        mesh=mesh,
        in_specs=(P("sp", "tp"), P("sp", "tp"), P("sp", "tp"), P("sp", "tp"), P()),
        out_specs=(P("sp", "tp"), P("sp", "tp"), P("sp", "tp"), P("sp", None)),
        check_vma=False,
    )
```

```python
from functools import partial
import math

import jax
import jax.numpy as jnp
from jax import lax
from jax.experimental import pallas as pl
from jax.experimental.pallas import tpu as pltpu
from jax.sharding import PartitionSpec as P

HEAD_DIM = 64
SEG = 64
LEFT = 4
CLIP = 128

LANES = 2 * HEAD_DIM
REACH = LEFT * SEG
BLK = 2 * SEG
BAND = REACH + BLK
WRAP = 3 * BLK
NEG_FILL = -1e30
LOG2E = math.log2(math.e)
MESH = pl.DeviceIdType.MESH
LEFTWARD, RIGHTWARD = 0, 1
F32 = jnp.float32
BF16 = jnp.bfloat16

NT = (((1,), (1,)), ((), ()))
NN = (((1,), (0,)), ((), ()))
TN = (((0,), (0,)), ((), ()))


def dot(a, b, dims):
    return lax.dot_general(a, b, dims, preferred_element_type=F32)


def turned(x, amount):
    amount %= x.shape[1]
    return pltpu.roll(x, amount, 1) if amount else x


def grid(axis):
    return lax.broadcasted_iota(jnp.int32, (BLK, BLK), axis)


def build_bias(table_row, bias_ref, pair, lane):
    def shear(half):
        return pltpu.roll(
            jnp.broadcast_to(half, (BLK, BLK)), 0, 1, stride=1, stride_axis=0
        )

    ahead, behind = shear(table_row[:, CLIP:]), shear(table_row[:, :CLIP])
    flat = jnp.broadcast_to(table_row[:, 2 * CLIP - 1 :], (BLK, BLK))
    key, query = grid(0), grid(1)
    later = query >= key
    cols = pl.ds(lane * BLK, BLK)
    bias_ref[pair, :BLK, cols] = jnp.where((key < SEG) & (query >= SEG), NEG_FILL, flat)
    bias_ref[pair, BLK : 2 * BLK, cols] = jnp.where(later, flat, ahead)
    bias_ref[pair, 2 * BLK :, cols] = jnp.where(
        (key >= SEG) & (query < SEG), NEG_FILL, jnp.where(later, ahead, behind)
    )


def unshear(square, shift):
    parts = [turned(square[8 * g : 8 * g + 8], -8 * g) for g in range(BLK // 8)]
    while len(parts) > 1:
        parts = [a + b for a, b in zip(parts[::2], parts[1::2])]
    row = lax.broadcasted_iota(jnp.int32, (8, BLK), 0)
    result = turned(parts[0], shift)
    for i in range(1, 8):
        result = jnp.where(row == i, turned(parts[0], shift - i), result)
    return jnp.sum(result, axis=0, keepdims=True)


def diagonals(square, shift):
    top, far, near = square[:BLK], square[BLK : 2 * BLK], square[2 * BLK :]
    later = grid(1) >= grid(0)
    beyond = jnp.sum(top + jnp.where(later, far, 0.0), axis=0, keepdims=True)
    spot = lax.broadcasted_iota(jnp.int32, (1, BLK), 1)
    clipped = jnp.where(
        spot == (BLK - 1 + shift) % BLK, jnp.sum(beyond, axis=1, keepdims=True), 0.0
    )
    return (
        unshear(jnp.where(later, 0.0, near), shift),
        unshear(jnp.where(later, near, far), shift) + clipped,
    )


def kernel(
    sp_size, tp_size, moved, direct,
    q_hbm, k_hbm, v_hbm, d_hbm, table_hbm,
    dq_ref, dk_ref, dv_ref, dt_ref,
    qd, got_qd, kv, bias_ref, square_ref, grown_ref, dprob_ref, peak_ref,
    own_k, own_v, own_q, back_q, got_q, back_kv, got_kv,
    local_stats, right_stats, halo_stats, left_stats,
    table_rows, pieces, exchange_a, exchange_b, exchange_c,
    load_sem, hop_sem, send_sem, seq_recv, back_recv, halo_recv, misc_recv,
):
    if direct:
        packs, pack_got, stack = exchange_a, exchange_b, exchange_c
    else:
        piece_got, shares = exchange_a, exchange_b
    rows, width = q_hbm.shape
    pairs = width // LANES
    heads = width // HEAD_DIM
    part = 2 * CLIP // sp_size
    me = lax.axis_index("sp")
    col = lax.axis_index("tp")
    has_left = me > 0
    has_right = me < sp_size - 1
    left = jnp.maximum(me - 1, 0)
    right = jnp.minimum(me + 1, sp_size - 1)
    prev, own = pl.ds(0, rows), pl.ds(rows, rows)

    def columns(p):
        return pl.ds(p * LANES, LANES)

    barrier = pltpu.get_barrier_semaphore()

    def greet(sem, step):
        @pl.when(me >= step)
        def _():
            pl.semaphore_signal(sem, inc=1, device_id=(me - step, col), device_id_type=MESH)

        @pl.when(me + step < sp_size)
        def _():
            pl.semaphore_signal(sem, inc=1, device_id=(me + step, col), device_id_type=MESH)

    def greeters(step):
        return (me >= step).astype(jnp.int32) + (me + step < sp_size).astype(jnp.int32)

    @pl.when(has_right)
    def _():
        pl.semaphore_signal(barrier, inc=1, device_id=(me + 1, col), device_id_type=MESH)

    for k in range(1, tp_size):
        pl.semaphore_signal(
            barrier, inc=1, device_id=(me, lax.rem(col + k, tp_size)), device_id_type=MESH
        )

    def load_queries(p):
        for i, src in enumerate((q_hbm, d_hbm)):
            sem = load_sem.at[2 + (p > 0)]
            pltpu.make_async_copy(src.at[:, columns(p)], qd.at[p, i], sem).start()

    load_queries(0)
    pltpu.make_async_copy(table_hbm, table_rows, load_sem.at[0]).start()

    rounds = hop_sem.shape[0] - 1

    def hop(r):
        if 0 < r <= rounds:
            pl.semaphore_wait(hop_sem.at[r - 1], greeters(1 << (r - 1)))
        if r < rounds:
            greet(hop_sem.at[r], 1 << r)

    def remote(src, dst, send, recv, target):
        return pltpu.make_async_remote_copy(
            src_ref=src,
            dst_ref=dst,
            send_sem=send_sem.at[send],
            recv_sem=recv,
            device_id=(target, col),
            device_id_type=MESH,
        )

    def query_copy(p):
        return remote(qd.at[p], got_qd.at[p], LEFTWARD, seq_recv.at[p], left)

    turn, last = max(moved - 2, 0), pairs - 1

    def query_part(half):
        mine = pl.ds(SEG, rows - SEG) if half else pl.ds(0, SEG)
        recv = seq_recv.at[turn if half else 2 * pairs - moved]
        return remote(qd.at[turn, :, mine], got_qd.at[turn, :, mine], LEFTWARD, recv, left)

    def all_queries():
        return remote(qd.at[pl.ds(0, moved)], got_qd, LEFTWARD, misc_recv.at[0], left)

    def key_copy(p, block):
        return remote(
            kv.at[p, :, pl.ds(rows + block * BLK, BLK)],
            kv.at[p, :, pl.ds(block * BLK, BLK)],
            RIGHTWARD,
            seq_recv.at[p + block * (pairs - moved)],
            right,
        )

    def all_keys():
        keyed = pl.ds(moved, pairs - moved)
        return remote(kv.at[keyed, :, own], kv.at[keyed, :, prev], RIGHTWARD, misc_recv.at[0], right)

    def local_copy():
        return remote(local_stats, right_stats, LEFTWARD, misc_recv.at[0], left)

    def halo_copy(p):
        return remote(halo_stats.at[p], left_stats.at[p], RIGHTWARD, halo_recv.at[p], right)

    def back_copy(p):
        return remote(back_q.at[p], got_q.at[p], RIGHTWARD, back_recv.at[0], right)

    def all_back():
        return remote(back_q, got_q, RIGHTWARD, back_recv.at[0], right)

    def key_back_copy(p):
        i = p - moved
        return remote(back_kv.at[i], got_kv.at[i], LEFTWARD, back_recv.at[1 + i], left)

    def send_queries(p):
        @pl.when(has_left)
        def _():
            if p == turn:
                query_part(1).start()
                query_part(0).start()
            else:
                query_copy(p).start()

    def send_back(p):
        if p < moved:
            @pl.when(has_right)
            def _():
                back_copy(p).start()
        else:
            @pl.when(has_left)
            def _():
                key_back_copy(p).start()

    def load_wait(refs, sem):
        pltpu.make_async_copy(refs, refs, sem).wait()

    pl.semaphore_wait(barrier, has_left.astype(jnp.int32) + tp_size - 1)
    load_wait(qd.at[0], load_sem.at[2])
    send_queries(0)
    for p in range(1, pairs):
        load_queries(p)
    for p in range(pairs):
        for i, src in enumerate((k_hbm, v_hbm)):
            pltpu.make_async_copy(src.at[:, columns(p)], kv.at[p, i, own], load_sem.at[1]).start()

    @pl.when(jnp.logical_not(has_left))
    def _():
        spot = lax.broadcasted_iota(jnp.int32, left_stats.shape, 1)
        left_stats[...] = jnp.where((spot & 2) == 0, NEG_FILL, 0.0)
        kv[moved:, :, prev] = jnp.zeros((pairs - moved, 2, rows, LANES), BF16)

    load_wait(table_rows, load_sem.at[0])
    for h in range(heads):
        row = table_rows[pl.ds(col * heads + h, 1), :] * LOG2E
        build_bias(row, bias_ref, h // 2, h % 2)

    load_wait(qd.at[pl.ds(1, pairs - 1)], load_sem.at[3])
    load_wait(kv.at[:, :, own], load_sem.at[1])

    low = lax.broadcasted_iota(jnp.int32, (BLK, LANES), 1) < HEAD_DIM
    scale = HEAD_DIM ** -0.5
    groups = CLIP // part
    folded = exchange_a.shape[1]
    wide = heads // folded

    def split(x):
        zero = jnp.zeros_like(x)
        return jnp.concatenate([jnp.where(low, x, zero), jnp.where(low, zero, x)], axis=0)

    def queries(ref, p, half):
        mine = pl.ds(half * BLK, BLK)
        return split(ref[p, 0, mine] * jnp.asarray(scale, BF16)), split(ref[p, 1, mine])

    def tile(p, half, halo):
        start, size, row = (
            (half * BLK, REACH - half * BLK, 0)
            if halo
            else (0, (half + 1) * BLK, REACH - half * BLK)
        )
        keys = pl.ds(rows + start, size)
        ref = got_qd if halo else qd
        return kv[p, 0, keys], kv[p, 1, keys], *queries(ref, p, half), pl.ds(row, size)

    def put(stats, p, half, which, value):
        for lane in range(2):
            spot = pl.ds(half * 4 + which * 2 + lane, 1)
            stats[p, spot, :] = value[:, lane * BLK : (lane + 1) * BLK]

    def get(stats, p, half, which):
        spots = [pl.ds(half * 4 + which * 2 + lane, 1) for lane in range(2)]
        return jnp.concatenate([stats[p, spot, :] for spot in spots], axis=1)

    def partial_softmax(p, half, halo, stats):
        k_blk, v_blk, qq, dd, band = tile(p, half, halo)
        scores = dot(k_blk, qq, NT) * LOG2E + bias_ref[p, band]
        dprobs = dot(v_blk, dd, NT)
        peak = jnp.max(scores, axis=0, keepdims=True)
        grown = jnp.exp2(scores - peak)
        total = jnp.sum(grown, axis=0, keepdims=True)
        put(stats, p, half, 0, peak + jnp.log2(total))
        put(stats, p, half, 1, jnp.sum(grown * dprobs, axis=0, keepdims=True) / total)
        return grown, dprobs, peak

    def products(k_blk, qq, dd, probs, dscores):
        ds_half = dscores.astype(BF16)
        flat = dot(k_blk, ds_half, TN)
        both = jnp.concatenate([flat[:HEAD_DIM, :BLK], flat[HEAD_DIM:, BLK:]], axis=0)
        return (
            dot(ds_half, qq, NN),
            dot(probs.astype(BF16), dd, NN),
            jnp.transpose(both) * scale,
        )

    def tile_probs(p, half, grown, dprobs, peak, stats, others):
        n1, i1 = get(stats, p, half, 0), get(stats, p, half, 1)
        n2, i2 = get(others, p, half, 0), get(others, p, half, 1)
        top = jnp.maximum(n1, n2)
        a1, a2 = jnp.exp2(n1 - top), jnp.exp2(n2 - top)
        inverse = 1.0 / (a1 + a2)
        inner = (i1 * a1 + i2 * a2) * inverse
        probs = grown * (jnp.exp2(peak - top) * inverse)
        return probs, probs * (dprobs - inner)

    def tile_grads(p, half, halo, probs, dscores):
        k_blk, _, qq, dd, _ = tile(p, half, halo)
        return products(k_blk, qq, dd, probs, dscores)

    places = (pl.ds(0, BLK), pl.ds(BLK, 2 * BLK))
    for p in range(moved):
        for half in range(2):
            grown, dprobs, peak = partial_softmax(p, half, False, local_stats)
            grown_ref[p, places[half], :] = grown
            dprob_ref[p, places[half], :] = dprobs
            peak_ref[p, pl.ds(half, 1), :] = peak

    @pl.when(has_left)
    def _():
        local_copy().start()

    if moved > 1:
        send_queries(1)

    even = lax.rem(me, 2) == 0
    core = lax.rem(col, 2)
    early = has_right & (even | (core == 0))
    keyed = [(p, block) for p in range(moved, pairs) for block in (1, 0)]

    def send_keys(blocks):
        for p, block in blocks:
            key_copy(p, block).start()

    def first_keys():
        @pl.when(has_right & jnp.logical_not(even) & (core == 0))
        def _():
            pl.semaphore_signal(
                hop_sem.at[rounds], inc=1, device_id=(me, col + 1), device_id_type=MESH
            )

        @pl.when(early)
        def _():
            send_keys(keyed[:1])

    def after_stats(p):
        if p + 2 < moved:
            send_queries(p + 2)
        if p == turn:
            @pl.when(early)
            def _():
                send_keys(keyed[1:])

            @pl.when(has_right & jnp.logical_not(early))
            def _():
                pl.semaphore_wait(hop_sem.at[rounds], 1)
                send_keys(keyed)

        if p == moved - 1:
            for done in range(p):
                send_back(done)

    def halo(p):
        @pl.when(has_right)
        def _():
            if p == turn:
                query_part(1).wait_recv()
                kept = [partial_softmax(p, 1, True, halo_stats)]
                first_keys()
                query_part(0).wait_recv()
                kept.insert(0, partial_softmax(p, 0, True, halo_stats))
            else:
                query_copy(p).wait_recv()
                kept = [partial_softmax(p, half, True, halo_stats) for half in range(2)]
            halo_copy(p).start()
            after_stats(p)
            hop(p)
            if p == 0:
                local_copy().wait_recv()
            (p0, s0), (p1, s1) = (
                tile_probs(p, half, *kept[half], halo_stats, right_stats) for half in range(2)
            )
            k0, v0, q0 = tile_grads(p, 0, True, p0, s0)
            k1, v1, q1 = tile_grads(p, 1, True, p1, s1)
            for ref, a, b in ((own_k, k0, k1), (own_v, v0, v1)):
                ref[p, :BLK, :] = a[:BLK]
                ref[p, BLK:, :] = a[BLK:] + b
            back_q[p, :BLK, :] = q0.astype(BF16)
            back_q[p, BLK:, :] = q1.astype(BF16)
            square_ref[p, :BLK, :] = s0[:BLK] + s1
            square_ref[p, BLK:REACH, :] = s0[BLK:]

        @pl.when(jnp.logical_not(has_right))
        def _():
            after_stats(p)
            hop(p)
            own_k[p] = jnp.zeros((rows, LANES), F32)
            own_v[p] = jnp.zeros((rows, LANES), F32)
            square_ref[p, :REACH, :] = jnp.zeros((REACH, 2 * BLK), F32)

    def tally(p, square):
        for lane in range(2):
            head = 2 * p + lane
            sides = diagonals(
                square[:, lane * BLK : (lane + 1) * BLK],
                part * (head % wide) if direct else 0,
            )
            for side in range(2):
                pieces[side, head : head + 1] = sides[side]

    def local_probs(p):
        @pl.when(has_left)
        def _():
            halo_copy(p).wait_recv()

        (p0, s0), (p1, s1) = (
            tile_probs(
                p, half,
                grown_ref[p, places[half], :], dprob_ref[p, places[half], :],
                peak_ref[p, pl.ds(half, 1), :],
                local_stats, left_stats,
            )
            for half in range(2)
        )
        square = jnp.concatenate(
            [
                square_ref[p, :BLK, :],
                square_ref[p, BLK:REACH, :] + s1[:BLK],
                s0 + s1[BLK:],
            ],
            axis=0,
        )
        tally(p, square)
        return p0, s0, p1, s1

    def local_grads(p, p0, s0, p1, s1):
        cols = columns(p)
        k0, v0, q0 = tile_grads(p, 0, False, p0, s0)
        k1, v1, q1 = tile_grads(p, 1, False, p1, s1)
        for out, ref, a, b in ((dk_ref, own_k, k0, k1), (dv_ref, own_v, v0, v1)):
            out[:BLK, cols] = (ref[p, :BLK, :] + a + b[:BLK]).astype(BF16)
            out[BLK:, cols] = (ref[p, BLK:, :] + b[BLK:]).astype(BF16)
        own_q[p, :BLK, :] = q0
        own_q[p, BLK:, :] = q1

    def local(p):
        local_grads(p, *local_probs(p))

    gate = jnp.where(has_left, 0.0, NEG_FILL)

    def full(p, between=None):
        cols = columns(p)
        i = p - moved

        def arrived(block):
            @pl.when(has_left)
            def _():
                key_copy(p, block).wait_recv()

        def part_of(half, row, size, before):
            keys = pl.ds(half * BLK + row, size)
            qq, dd = queries(qd, p, half)
            scores = dot(kv[p, 0, keys], qq, NT) * LOG2E + bias_ref[p, pl.ds(row, size)]
            scores = (
                jnp.concatenate([scores[:before] + gate, scores[before:]], axis=0)
                if before < size
                else scores + gate
            )
            peak = jnp.max(scores, axis=0, keepdims=True)
            return scores, dot(kv[p, 1, keys], dd, NT), peak

        def moments(grown, dprobs):
            return (
                jnp.sum(grown, axis=0, keepdims=True),
                jnp.sum(grown * dprobs, axis=0, keepdims=True),
            )

        def half_grads(half, probs, dscores):
            qq, dd = queries(qd, p, half)
            return products(kv[p, 0, pl.ds(half * BLK, BAND)], qq, dd, probs, dscores)

        arrived(1)
        scores, dprobs, peak = part_of(1, 0, BAND, BLK)
        grown = jnp.exp2(scores - peak)
        total, inner = moments(grown, dprobs)
        inverse = 1.0 / total
        probs = grown * inverse
        s1 = probs * (dprobs - inner * inverse)
        k1, v1, q1 = half_grads(1, probs, s1)
        scores_a, dprobs_a, peak_a = part_of(0, BLK, 2 * BLK, BLK)
        grown_a = jnp.exp2(scores_a - peak_a)
        total_a, inner_a = moments(grown_a, dprobs_a)

        arrived(0)
        scores_b, dprobs_b, peak_b = part_of(0, 0, BLK, BLK)
        peak = jnp.maximum(peak_a, peak_b)
        grown_b = jnp.exp2(scores_b - peak)
        total_b, inner_b = moments(grown_b, dprobs_b)
        factor = jnp.exp2(peak_a - peak)
        inverse = 1.0 / (total_a * factor + total_b)
        inner = (inner_a * factor + inner_b) * inverse
        probs_a, probs_b = grown_a * (factor * inverse), grown_b * inverse
        p0 = jnp.concatenate([probs_b, probs_a], axis=0)
        s0 = jnp.concatenate(
            [probs_b * (dprobs_b - inner), probs_a * (dprobs_a - inner)], axis=0
        )
        tally(p, s0 + s1)
        if p == pairs - 1:
            send_back(moved - 1)
        if between is not None:
            between()
        k0, v0, q0 = half_grads(0, p0, s0)
        for which, ref, a, b in ((0, own_k, k0, k1), (1, own_v, v0, v1)):
            back_kv[i, which, :BLK, :] = a[:BLK].astype(BF16)
            back_kv[i, which, BLK:, :] = (a[BLK:REACH] + b[:BLK]).astype(BF16)
            ref[p, :BLK, :] = a[REACH:] + b[BLK:REACH]
            ref[p, BLK:, :] = b[REACH:]
        dq_ref[:BLK, cols] = q0.astype(BF16)
        dq_ref[BLK:, cols] = q1.astype(BF16)

    def piece_copy(target, t, k=1):
        if direct:
            src, dst = packs.at[target], pack_got.at[col * sp_size + me]
        else:
            src, dst = pieces.at[target * part // CLIP], piece_got.at[k - 1]
        return pltpu.make_async_remote_copy(
            src_ref=src,
            dst_ref=dst,
            send_sem=send_sem.at[2],
            recv_sem=misc_recv.at[1],
            device_id=(target, lax.rem(col + t, tp_size)),
            device_id_type=MESH,
        )

    def all_pieces():
        ref = pack_got.at[pl.ds(1, sp_size * tp_size - 1)] if direct else piece_got
        return remote(ref, ref, 2, misc_recv.at[1], left)

    def share_copy(k):
        return pltpu.make_async_remote_copy(
            src_ref=shares.at[0],
            dst_ref=shares.at[k],
            send_sem=send_sem.at[3],
            recv_sem=misc_recv.at[2],
            device_id=(me, lax.rem(col + k, tp_size)),
            device_id_type=MESH,
        )

    def all_shares():
        rest = shares.at[pl.ds(1, tp_size - 1)]
        return remote(rest, rest, 3, misc_recv.at[2], left)

    def fold():
        block = lax.broadcasted_iota(jnp.int32, (folded, CLIP), 1) // part
        for side in range(2):
            lines = [pieces[side, pl.ds(j, folded, stride=wide), :] for j in range(wide)]
            for m in range(groups):
                pack = jnp.zeros((folded, CLIP), F32)
                for j in range(wide):
                    pack = jnp.where(block == (m + j) % groups, lines[j], pack)
                packs[side * groups + m] = pack

    def unfold():
        pack_got[col * sp_size + me] = packs[me]
        total = []
        for t in range(tp_size):
            line = pack_got[t * sp_size]
            for k in range(1, sp_size):
                line = line + pack_got[t * sp_size + k]
            total.append(line)
        total = jnp.concatenate(total, axis=0)
        for j in range(wide):
            away = lax.rem(me + j, groups) * part
            stack[pl.ds(j, folded * tp_size, stride=wide), :] = pltpu.roll(
                total, lax.rem(CLIP - away, CLIP), 1
            )
        dt_ref[...] = jnp.transpose(stack[...])[:part]

    def send_pieces():
        for r in range(moved, rounds + 1):
            hop(r)
        if direct:
            fold()
        beside = range(1, tp_size if direct else 1)
        for t in beside:
            piece_copy(0, t).start()
        for k in range(1, sp_size):
            piece_copy(lax.rem(me + k, sp_size), 0, k).start()
        for target in range(1, sp_size):
            for t in beside:
                piece_copy(target, t).start()

    for p in range(moved):
        halo(p)
        if p:
            local(p - 1)
    for p in range(moved, last):
        full(p)
        send_back(p)
        if p == moved:
            local(moved - 1)
    kept = []

    def finish_pieces():
        if moved == last:
            kept.extend(local_probs(moved - 1))
        send_pieces()

    full(last, finish_pieces)
    send_back(last)
    if kept:
        local_grads(moved - 1, *kept)

    def finish(p):
        cols = pl.ds(p * LANES, LANES)
        if p < moved:
            @pl.when(has_left)
            def _():
                if p == 0:
                    all_back().wait_recv()
                dq_ref[:, cols] = (own_q[p] + got_q[p].astype(F32)).astype(BF16)

            @pl.when(jnp.logical_not(has_left))
            def _():
                dq_ref[:, cols] = own_q[p].astype(BF16)
        else:
            i = p - moved

            @pl.when(has_right)
            def _():
                key_back_copy(p).wait_recv()
                dk_ref[:, cols] = (own_k[p] + got_kv[i, 0].astype(F32)).astype(BF16)
                dv_ref[:, cols] = (own_v[p] + got_kv[i, 1].astype(F32)).astype(BF16)

            @pl.when(jnp.logical_not(has_right))
            def _():
                dk_ref[:, cols] = own_k[p].astype(BF16)
                dv_ref[:, cols] = own_v[p].astype(BF16)

    if direct:
        for p in range(pairs):
            finish(p)
    all_pieces().wait_recv()
    if direct:
        unfold()
    else:
        total = pieces[me * part // CLIP]
        for k in range(1, sp_size):
            total = total + piece_got[k - 1]
        shares[0] = pltpu.roll(total, lax.rem(CLIP - lax.rem(me * part, CLIP), CLIP), 1)
        for k in range(1, tp_size):
            share_copy(k).start()
    if not direct:
        for p in range(pairs):
            finish(p)
        all_shares().wait_recv()
        stacked = jnp.concatenate(
            [shares[lax.rem(col + tp_size - t, tp_size)] for t in range(tp_size)], axis=0
        )
        dt_ref[...] = jnp.transpose(stacked)[:part]
        all_shares().wait_send()

    all_pieces().wait_send()

    @pl.when(has_left)
    def _():
        all_queries().wait_send()
        local_copy().wait_send()
        remote(back_kv, got_kv, LEFTWARD, misc_recv.at[0], left).wait_send()

    @pl.when(has_right)
    def _():
        all_keys().wait_send()
        remote(halo_stats, left_stats, RIGHTWARD, misc_recv.at[0], right).wait_send()
        all_back().wait_send()


def shards(sp_size, tp_size, query_rows, key_rows, value_rows, out_grad, rel_bias):
    rows, width = query_rows.shape
    pairs = width // LANES
    heads = width // HEAD_DIM
    part = 2 * CLIP // sp_size
    moved = pairs - 1
    rounds = (sp_size - 1).bit_length()
    direct = sp_size * tp_size <= 64 and part <= CLIP and heads % (CLIP // part) == 0
    folded = heads * part // CLIP
    exchange = [
        pltpu.VMEM(shape, F32)
        for shape in (
            (
                (sp_size, folded, CLIP),
                (sp_size * tp_size, folded, CLIP),
                (tp_size * heads, CLIP),
            )
            if direct
            else ((sp_size - 1, heads, CLIP), (tp_size, heads, CLIP), (8, CLIP))
        )
    ]
    assert rows == REACH and REACH == 2 * BLK and CLIP == BLK
    like = jax.ShapeDtypeStruct((rows, width), BF16)
    dma = pltpu.SemaphoreType.DMA
    shapes = (like, like, like, jax.ShapeDtypeStruct((part, heads * tp_size), F32))
    results = pl.pallas_call(
        partial(kernel, sp_size, tp_size, moved, direct),
        out_shape=shapes,
        in_specs=[pl.BlockSpec(memory_space=pltpu.HBM)] * 5,
        out_specs=tuple([pl.BlockSpec(memory_space=pltpu.VMEM)] * 4),
        scratch_shapes=[
            pltpu.VMEM((pairs, 2, rows, LANES), BF16),
            pltpu.VMEM((moved, 2, rows, LANES), BF16),
            pltpu.VMEM((pairs, 2, 2 * rows, LANES), BF16),
            pltpu.VMEM((pairs, BAND, 2 * BLK), F32),
            pltpu.VMEM((moved, REACH, 2 * BLK), F32),
            pltpu.VMEM((moved, BAND, 2 * BLK), F32),
            pltpu.VMEM((moved, BAND, 2 * BLK), F32),
            pltpu.VMEM((moved, 8, 2 * BLK), F32),
            pltpu.VMEM((pairs, rows, LANES), F32),
            pltpu.VMEM((pairs, rows, LANES), F32),
            pltpu.VMEM((moved, rows, LANES), F32),
            pltpu.VMEM((moved, rows, LANES), BF16),
            pltpu.VMEM((moved, rows, LANES), BF16),
            pltpu.VMEM((pairs - moved, 2, rows, LANES), BF16),
            pltpu.VMEM((pairs - moved, 2, rows, LANES), BF16),
            pltpu.VMEM((moved, 8, BLK), F32),
            pltpu.VMEM((moved, 8, BLK), F32),
            pltpu.VMEM((moved, 8, BLK), F32),
            pltpu.VMEM((moved, 8, BLK), F32),
            pltpu.VMEM(rel_bias.shape[::-1], F32),
            pltpu.VMEM((2, heads, BLK), F32),
            *exchange,
            dma((4,)),
            pltpu.SemaphoreType.REGULAR((rounds + 1,)),
            dma((3 if direct else 4,)),
            dma((2 * pairs - moved + 1,)),
            dma((1 + pairs - moved,)),
            dma((moved,)),
            dma((2 if direct else 3,)),
        ],
        compiler_params=pltpu.CompilerParams(
            collective_id=0, has_side_effects=True, vmem_limit_bytes=48 * 1024 * 1024
        ),
    )(*[pltpu.with_memory_space_constraint(x, pltpu.HBM) for x in (query_rows, key_rows, value_rows, out_grad, jnp.transpose(rel_bias))])
    return pl.pallas_call(
        write_out,
        out_shape=shapes,
        in_specs=[pl.BlockSpec(memory_space=pl.ANY)] * 4,
        out_specs=tuple([pl.BlockSpec(memory_space=pltpu.HBM)] * 4),
        scratch_shapes=[dma((4,))],
        compiler_params=pltpu.CompilerParams(vmem_limit_bytes=1024 * 1024),
    )(*results)


def write_out(*refs):
    sem = refs[-1]
    copies = [pltpu.make_async_copy(refs[i], refs[4 + i], sem.at[i]) for i in range(4)]
    for copy in copies:
        copy.start()
    for copy in copies:
        copy.wait()


def solution(mesh):
    return jax.shard_map(
        partial(shards, mesh.shape["sp"], mesh.shape["tp"]),
        mesh=mesh,
        in_specs=(P("sp", "tp"), P("sp", "tp"), P("sp", "tp"), P("sp", "tp"), P()),
        out_specs=(P("sp", "tp"), P("sp", "tp"), P("sp", "tp"), P("sp", None)),
        check_vma=False,
    )
```

```python
from functools import partial
import math

import jax
import jax.numpy as jnp
from jax import lax
from jax.experimental import pallas as pl
from jax.experimental.pallas import tpu as pltpu
from jax.sharding import PartitionSpec as P

HEAD_DIM = 64
SEG = 64
LEFT = 4
CLIP = 128

LANES = 2 * HEAD_DIM
REACH = LEFT * SEG
BLK = 2 * SEG
BAND = REACH + BLK
WRAP = 3 * BLK
NEG_FILL = -1e30
LOG2E = math.log2(math.e)
MESH = pl.DeviceIdType.MESH
LEFTWARD, RIGHTWARD, PIECES, SHARES = 2, 0, 1, 3
F32 = jnp.float32
BF16 = jnp.bfloat16

NT = (((1,), (1,)), ((), ()))
NN = (((1,), (0,)), ((), ()))
TN = (((0,), (0,)), ((), ()))


def dot(a, b, dims):
    return lax.dot_general(a, b, dims, preferred_element_type=F32)


def turned(x, amount):
    amount %= x.shape[1]
    return pltpu.roll(x, amount, 1) if amount else x


def grid(axis):
    return lax.broadcasted_iota(jnp.int32, (BLK, BLK), axis)


def build_bias(table_row, bias_ref, pair, lane):
    def shear(half):
        return pltpu.roll(
            jnp.broadcast_to(half, (BLK, BLK)), 0, 1, stride=1, stride_axis=0
        )

    ahead, behind = shear(table_row[:, CLIP:]), shear(table_row[:, :CLIP])
    flat = jnp.broadcast_to(table_row[:, 2 * CLIP - 1 :], (BLK, BLK))
    key, query = grid(0), grid(1)
    later = query >= key
    cols = pl.ds(lane * BLK, BLK)
    bias_ref[pair, :BLK, cols] = jnp.where((key < SEG) & (query >= SEG), NEG_FILL, flat)
    bias_ref[pair, BLK : 2 * BLK, cols] = jnp.where(later, flat, ahead)
    bias_ref[pair, 2 * BLK :, cols] = jnp.where(
        (key >= SEG) & (query < SEG), NEG_FILL, jnp.where(later, ahead, behind)
    )


def unshear(square, shift):
    parts = [turned(square[8 * g : 8 * g + 8], -8 * g) for g in range(BLK // 8)]
    while len(parts) > 1:
        parts = [a + b for a, b in zip(parts[::2], parts[1::2])]
    row = lax.broadcasted_iota(jnp.int32, (8, BLK), 0)
    result = turned(parts[0], shift)
    for i in range(1, 8):
        result = jnp.where(row == i, turned(parts[0], shift - i), result)
    return jnp.sum(result, axis=0, keepdims=True)


def diagonals(square, shift):
    top, far, near = square[:BLK], square[BLK : 2 * BLK], square[2 * BLK :]
    later = grid(1) >= grid(0)
    beyond = jnp.sum(top + jnp.where(later, far, 0.0), axis=0, keepdims=True)
    spot = lax.broadcasted_iota(jnp.int32, (1, BLK), 1)
    clipped = jnp.where(
        spot == (BLK - 1 + shift) % BLK, jnp.sum(beyond, axis=1, keepdims=True), 0.0
    )
    return (
        unshear(jnp.where(later, 0.0, near), shift),
        unshear(jnp.where(later, near, far), shift) + clipped,
    )


def kernel(
    sp_size, tp_size, moved, direct,
    q_hbm, k_hbm, v_hbm, d_hbm, table_hbm,
    dq_ref, dk_ref, dv_ref, dt_ref,
    qd, got_qd, kv, bias_ref, square_ref, grown_ref, dprob_ref, peak_ref,
    own_k, own_v, own_q, back_q, got_q, back_kv, got_kv,
    local_stats, right_stats, halo_stats, left_stats,
    table_rows, pieces, exchange_a, exchange_b, exchange_c,
    load_sem, hop_sem, seq_recv, back_recv, halo_recv, misc_recv,
):
    if direct:
        packs, pack_got, stack = exchange_a, exchange_b, exchange_c
    else:
        piece_got, shares = exchange_a, exchange_b
    rows, width = q_hbm.shape
    pairs = width // LANES
    heads = width // HEAD_DIM
    part = 2 * CLIP // sp_size
    me = lax.axis_index("sp")
    col = lax.axis_index("tp")
    has_left = me > 0
    has_right = me < sp_size - 1
    left = jnp.maximum(me - 1, 0)
    right = jnp.minimum(me + 1, sp_size - 1)
    prev, own = pl.ds(0, rows), pl.ds(rows, rows)

    def columns(p):
        return pl.ds(p * LANES, LANES)

    barrier = pltpu.get_barrier_semaphore()

    def greet(sem, step):
        @pl.when(me >= step)
        def _():
            pl.semaphore_signal(sem, inc=1, device_id=(me - step, col), device_id_type=MESH)

        @pl.when(me + step < sp_size)
        def _():
            pl.semaphore_signal(sem, inc=1, device_id=(me + step, col), device_id_type=MESH)

    def greeters(step):
        return (me >= step).astype(jnp.int32) + (me + step < sp_size).astype(jnp.int32)

    @pl.when(has_right)
    def _():
        pl.semaphore_signal(barrier, inc=1, device_id=(me + 1, col), device_id_type=MESH)

    for k in range(1, tp_size):
        pl.semaphore_signal(
            barrier, inc=1, device_id=(me, lax.rem(col + k, tp_size)), device_id_type=MESH
        )

    def load_queries(p):
        for i, src in enumerate((q_hbm, d_hbm)):
            sem = load_sem.at[2 + (p > 0)]
            pltpu.make_async_copy(src.at[:, columns(p)], qd.at[p, i], sem).start()

    load_queries(0)
    pltpu.make_async_copy(table_hbm, table_rows, load_sem.at[0]).start()

    rounds = hop_sem.shape[0] - 1

    def hop(r):
        if 0 < r <= rounds:
            pl.semaphore_wait(hop_sem.at[r - 1], greeters(1 << (r - 1)))
        if r < rounds:
            greet(hop_sem.at[r], 1 << r)

    def remote(src, dst, send, recv, target):
        return pltpu.make_async_remote_copy(
            src_ref=src,
            dst_ref=dst,
            send_sem=load_sem.at[send],
            recv_sem=recv,
            device_id=(target, col),
            device_id_type=MESH,
        )

    def query_copy(p):
        return remote(qd.at[p], got_qd.at[p], LEFTWARD, seq_recv.at[p], left)

    turn, last = max(moved - 2, 0), pairs - 1

    def query_part(half):
        mine = pl.ds(SEG, rows - SEG) if half else pl.ds(0, SEG)
        recv = seq_recv.at[turn if half else 2 * pairs - moved]
        return remote(qd.at[turn, :, mine], got_qd.at[turn, :, mine], LEFTWARD, recv, left)

    def all_queries():
        return remote(qd.at[pl.ds(0, moved)], got_qd, LEFTWARD, misc_recv.at[0], left)

    def key_copy(p, block):
        return remote(
            kv.at[p, :, pl.ds(rows + block * BLK, BLK)],
            kv.at[p, :, pl.ds(block * BLK, BLK)],
            RIGHTWARD,
            seq_recv.at[p + block * (pairs - moved)],
            right,
        )

    def all_keys():
        keyed = pl.ds(moved, pairs - moved)
        return remote(kv.at[keyed, :, own], kv.at[keyed, :, prev], RIGHTWARD, misc_recv.at[0], right)

    def local_copy():
        return remote(local_stats, right_stats, LEFTWARD, misc_recv.at[0], left)

    def halo_copy(p):
        return remote(halo_stats.at[p], left_stats.at[p], RIGHTWARD, halo_recv.at[p], right)

    def back_copy(p):
        return remote(back_q.at[p], got_q.at[p], RIGHTWARD, back_recv.at[0], right)

    def all_back():
        return remote(back_q, got_q, RIGHTWARD, back_recv.at[0], right)

    def key_back_copy(p):
        i = p - moved
        return remote(back_kv.at[i], got_kv.at[i], LEFTWARD, back_recv.at[1 + i], left)

    def send_queries(p):
        @pl.when(has_left)
        def _():
            if p == turn:
                query_part(1).start()
                query_part(0).start()
            else:
                query_copy(p).start()

    def send_back(p):
        if p < moved:
            @pl.when(has_right)
            def _():
                back_copy(p).start()
        else:
            @pl.when(has_left)
            def _():
                key_back_copy(p).start()

    def load_wait(refs, sem):
        pltpu.make_async_copy(refs, refs, sem).wait()

    pl.semaphore_wait(barrier, has_left.astype(jnp.int32) + tp_size - 1)
    load_wait(qd.at[0], load_sem.at[2])
    send_queries(0)
    for p in range(1, pairs):
        load_queries(p)
    for p in range(pairs):
        for i, src in enumerate((k_hbm, v_hbm)):
            pltpu.make_async_copy(src.at[:, columns(p)], kv.at[p, i, own], load_sem.at[1]).start()

    @pl.when(jnp.logical_not(has_left))
    def _():
        spot = lax.broadcasted_iota(jnp.int32, left_stats.shape, 1)
        left_stats[...] = jnp.where((spot & 2) == 0, NEG_FILL, 0.0)
        kv[moved:, :, prev] = jnp.zeros((pairs - moved, 2, rows, LANES), BF16)

    load_wait(table_rows, load_sem.at[0])
    for h in range(heads):
        row = table_rows[pl.ds(col * heads + h, 1), :] * LOG2E
        build_bias(row, bias_ref, h // 2, h % 2)

    load_wait(qd.at[pl.ds(1, pairs - 1)], load_sem.at[3])
    load_wait(kv.at[:, :, own], load_sem.at[1])

    low = lax.broadcasted_iota(jnp.int32, (BLK, LANES), 1) < HEAD_DIM
    scale = HEAD_DIM ** -0.5
    groups = CLIP // part
    folded = exchange_a.shape[1]
    wide = heads // folded

    def split(x):
        zero = jnp.zeros_like(x)
        return jnp.concatenate([jnp.where(low, x, zero), jnp.where(low, zero, x)], axis=0)

    def queries(ref, p, half):
        mine = pl.ds(half * BLK, BLK)
        return split(ref[p, 0, mine] * jnp.asarray(scale, BF16)), split(ref[p, 1, mine])

    def tile(p, half, halo):
        start, size, row = (
            (half * BLK, REACH - half * BLK, 0)
            if halo
            else (0, (half + 1) * BLK, REACH - half * BLK)
        )
        keys = pl.ds(rows + start, size)
        ref = got_qd if halo else qd
        return kv[p, 0, keys], kv[p, 1, keys], *queries(ref, p, half), pl.ds(row, size)

    def put(stats, p, half, which, value):
        for lane in range(2):
            spot = pl.ds(half * 4 + which * 2 + lane, 1)
            stats[p, spot, :] = value[:, lane * BLK : (lane + 1) * BLK]

    def get(stats, p, half, which):
        spots = [pl.ds(half * 4 + which * 2 + lane, 1) for lane in range(2)]
        return jnp.concatenate([stats[p, spot, :] for spot in spots], axis=1)

    def partial_softmax(p, half, halo, stats):
        k_blk, v_blk, qq, dd, band = tile(p, half, halo)
        scores = dot(k_blk, qq, NT) * LOG2E + bias_ref[p, band]
        dprobs = dot(v_blk, dd, NT)
        peak = jnp.max(scores, axis=0, keepdims=True)
        grown = jnp.exp2(scores - peak)
        total = jnp.sum(grown, axis=0, keepdims=True)
        put(stats, p, half, 0, peak + jnp.log2(total))
        put(stats, p, half, 1, jnp.sum(grown * dprobs, axis=0, keepdims=True) / total)
        return grown, dprobs, peak

    def products(k_blk, qq, dd, probs, dscores):
        ds_half = dscores.astype(BF16)
        flat = dot(k_blk, ds_half, TN)
        both = jnp.concatenate([flat[:HEAD_DIM, :BLK], flat[HEAD_DIM:, BLK:]], axis=0)
        return (
            dot(ds_half, qq, NN),
            dot(probs.astype(BF16), dd, NN),
            jnp.transpose(both) * scale,
        )

    def tile_probs(p, half, grown, dprobs, peak, stats, others):
        n1, i1 = get(stats, p, half, 0), get(stats, p, half, 1)
        n2, i2 = get(others, p, half, 0), get(others, p, half, 1)
        top = jnp.maximum(n1, n2)
        a1, a2 = jnp.exp2(n1 - top), jnp.exp2(n2 - top)
        inverse = 1.0 / (a1 + a2)
        inner = (i1 * a1 + i2 * a2) * inverse
        probs = grown * (jnp.exp2(peak - top) * inverse)
        return probs, probs * (dprobs - inner)

    def tile_grads(p, half, halo, probs, dscores):
        k_blk, _, qq, dd, _ = tile(p, half, halo)
        return products(k_blk, qq, dd, probs, dscores)

    places = (pl.ds(0, BLK), pl.ds(BLK, 2 * BLK))
    for p in range(moved):
        for half in range(2):
            grown, dprobs, peak = partial_softmax(p, half, False, local_stats)
            grown_ref[p, places[half], :] = grown
            dprob_ref[p, places[half], :] = dprobs
            peak_ref[p, pl.ds(half, 1), :] = peak

    @pl.when(has_left)
    def _():
        local_copy().start()

    if moved > 1:
        send_queries(1)

    even = lax.rem(me, 2) == 0
    core = lax.rem(col, 2)
    early = has_right & (even | (core == 0))
    keyed = [(p, block) for p in range(moved, pairs) for block in (1, 0)]

    def send_keys(blocks):
        for p, block in blocks:
            key_copy(p, block).start()

    def first_keys():
        @pl.when(has_right & jnp.logical_not(even) & (core == 0))
        def _():
            pl.semaphore_signal(
                hop_sem.at[rounds], inc=1, device_id=(me, col + 1), device_id_type=MESH
            )

        @pl.when(early)
        def _():
            send_keys(keyed[:1])

    def after_stats(p):
        if p + 2 < moved:
            send_queries(p + 2)
        if p == turn:
            @pl.when(early)
            def _():
                send_keys(keyed[1:])

            @pl.when(has_right & jnp.logical_not(early))
            def _():
                pl.semaphore_wait(hop_sem.at[rounds], 1)
                send_keys(keyed)

        if p == moved - 1:
            for done in range(p):
                send_back(done)

    def halo(p):
        @pl.when(has_right)
        def _():
            if p == turn:
                query_part(1).wait_recv()
                kept = [partial_softmax(p, 1, True, halo_stats)]
                first_keys()
                query_part(0).wait_recv()
                kept.insert(0, partial_softmax(p, 0, True, halo_stats))
            else:
                query_copy(p).wait_recv()
                kept = [partial_softmax(p, half, True, halo_stats) for half in range(2)]
            halo_copy(p).start()
            after_stats(p)
            hop(p)
            if p == 0:
                local_copy().wait_recv()
            (p0, s0), (p1, s1) = (
                tile_probs(p, half, *kept[half], halo_stats, right_stats) for half in range(2)
            )
            k0, v0, q0 = tile_grads(p, 0, True, p0, s0)
            k1, v1, q1 = tile_grads(p, 1, True, p1, s1)
            for ref, a, b in ((own_k, k0, k1), (own_v, v0, v1)):
                ref[p, :BLK, :] = a[:BLK]
                ref[p, BLK:, :] = a[BLK:] + b
            back_q[p, :BLK, :] = q0.astype(BF16)
            back_q[p, BLK:, :] = q1.astype(BF16)
            square_ref[p, :BLK, :] = s0[:BLK] + s1
            square_ref[p, BLK:REACH, :] = s0[BLK:]

        @pl.when(jnp.logical_not(has_right))
        def _():
            after_stats(p)
            hop(p)
            own_k[p] = jnp.zeros((rows, LANES), F32)
            own_v[p] = jnp.zeros((rows, LANES), F32)
            square_ref[p, :REACH, :] = jnp.zeros((REACH, 2 * BLK), F32)

    def tally(p, square):
        for lane in range(2):
            head = 2 * p + lane
            sides = diagonals(
                square[:, lane * BLK : (lane + 1) * BLK],
                part * (head % wide) if direct else 0,
            )
            for side in range(2):
                pieces[side, head : head + 1] = sides[side]

    def local_probs(p):
        @pl.when(has_left)
        def _():
            halo_copy(p).wait_recv()

        (p0, s0), (p1, s1) = (
            tile_probs(
                p, half,
                grown_ref[p, places[half], :], dprob_ref[p, places[half], :],
                peak_ref[p, pl.ds(half, 1), :],
                local_stats, left_stats,
            )
            for half in range(2)
        )
        square = jnp.concatenate(
            [
                square_ref[p, :BLK, :],
                square_ref[p, BLK:REACH, :] + s1[:BLK],
                s0 + s1[BLK:],
            ],
            axis=0,
        )
        tally(p, square)
        return p0, s0, p1, s1

    def local_grads(p, p0, s0, p1, s1):
        cols = columns(p)
        k0, v0, q0 = tile_grads(p, 0, False, p0, s0)
        k1, v1, q1 = tile_grads(p, 1, False, p1, s1)
        for out, ref, a, b in ((dk_ref, own_k, k0, k1), (dv_ref, own_v, v0, v1)):
            out[:BLK, cols] = (ref[p, :BLK, :] + a + b[:BLK]).astype(BF16)
            out[BLK:, cols] = (ref[p, BLK:, :] + b[BLK:]).astype(BF16)
        own_q[p, :BLK, :] = q0
        own_q[p, BLK:, :] = q1

    def local(p):
        local_grads(p, *local_probs(p))

    gate = jnp.where(has_left, 0.0, NEG_FILL)

    def full(p, between=None):
        cols = columns(p)
        i = p - moved

        def arrived(block):
            @pl.when(has_left)
            def _():
                key_copy(p, block).wait_recv()

        def part_of(half, row, size, before):
            keys = pl.ds(half * BLK + row, size)
            qq, dd = queries(qd, p, half)
            scores = dot(kv[p, 0, keys], qq, NT) * LOG2E + bias_ref[p, pl.ds(row, size)]
            scores = (
                jnp.concatenate([scores[:before] + gate, scores[before:]], axis=0)
                if before < size
                else scores + gate
            )
            peak = jnp.max(scores, axis=0, keepdims=True)
            return scores, dot(kv[p, 1, keys], dd, NT), peak

        def moments(grown, dprobs):
            return (
                jnp.sum(grown, axis=0, keepdims=True),
                jnp.sum(grown * dprobs, axis=0, keepdims=True),
            )

        def half_grads(half, probs, dscores):
            qq, dd = queries(qd, p, half)
            return products(kv[p, 0, pl.ds(half * BLK, BAND)], qq, dd, probs, dscores)

        arrived(1)
        scores, dprobs, peak = part_of(1, 0, BAND, BLK)
        grown = jnp.exp2(scores - peak)
        total, inner = moments(grown, dprobs)
        inverse = 1.0 / total
        probs = grown * inverse
        s1 = probs * (dprobs - inner * inverse)
        k1, v1, q1 = half_grads(1, probs, s1)
        scores_a, dprobs_a, peak_a = part_of(0, BLK, 2 * BLK, BLK)
        grown_a = jnp.exp2(scores_a - peak_a)
        total_a, inner_a = moments(grown_a, dprobs_a)

        arrived(0)
        scores_b, dprobs_b, peak_b = part_of(0, 0, BLK, BLK)
        peak = jnp.maximum(peak_a, peak_b)
        grown_b = jnp.exp2(scores_b - peak)
        total_b, inner_b = moments(grown_b, dprobs_b)
        factor = jnp.exp2(peak_a - peak)
        inverse = 1.0 / (total_a * factor + total_b)
        inner = (inner_a * factor + inner_b) * inverse
        probs_a, probs_b = grown_a * (factor * inverse), grown_b * inverse
        p0 = jnp.concatenate([probs_b, probs_a], axis=0)
        s0 = jnp.concatenate(
            [probs_b * (dprobs_b - inner), probs_a * (dprobs_a - inner)], axis=0
        )
        tally(p, s0 + s1)
        if p == pairs - 1:
            send_back(moved - 1)
        if between is not None:
            between()
        k0, v0, q0 = half_grads(0, p0, s0)
        for which, ref, a, b in ((0, own_k, k0, k1), (1, own_v, v0, v1)):
            back_kv[i, which, :BLK, :] = a[:BLK].astype(BF16)
            back_kv[i, which, BLK:, :] = (a[BLK:REACH] + b[:BLK]).astype(BF16)
            ref[p, :BLK, :] = a[REACH:] + b[BLK:REACH]
            ref[p, BLK:, :] = b[REACH:]
        dq_ref[:BLK, cols] = q0.astype(BF16)
        dq_ref[BLK:, cols] = q1.astype(BF16)

    def piece_copy(target, t, k=1):
        if direct:
            src, dst = packs.at[target], pack_got.at[col * sp_size + me]
        else:
            src, dst = pieces.at[target * part // CLIP], piece_got.at[k - 1]
        return pltpu.make_async_remote_copy(
            src_ref=src,
            dst_ref=dst,
            send_sem=load_sem.at[PIECES],
            recv_sem=misc_recv.at[1],
            device_id=(target, lax.rem(col + t, tp_size)),
            device_id_type=MESH,
        )

    def all_pieces():
        ref = pack_got.at[pl.ds(1, sp_size * tp_size - 1)] if direct else piece_got
        return remote(ref, ref, PIECES, misc_recv.at[1], left)

    def share_copy(k):
        return pltpu.make_async_remote_copy(
            src_ref=shares.at[0],
            dst_ref=shares.at[k],
            send_sem=load_sem.at[SHARES],
            recv_sem=misc_recv.at[2],
            device_id=(me, lax.rem(col + k, tp_size)),
            device_id_type=MESH,
        )

    def all_shares():
        rest = shares.at[pl.ds(1, tp_size - 1)]
        return remote(rest, rest, SHARES, misc_recv.at[2], left)

    def fold():
        block = lax.broadcasted_iota(jnp.int32, (folded, CLIP), 1) // part
        for side in range(2):
            lines = [pieces[side, pl.ds(j, folded, stride=wide), :] for j in range(wide)]
            for m in range(groups):
                pack = jnp.zeros((folded, CLIP), F32)
                for j in range(wide):
                    pack = jnp.where(block == (m + j) % groups, lines[j], pack)
                packs[side * groups + m] = pack

    def unfold():
        pack_got[col * sp_size + me] = packs[me]
        total = []
        for t in range(tp_size):
            line = pack_got[t * sp_size]
            for k in range(1, sp_size):
                line = line + pack_got[t * sp_size + k]
            total.append(line)
        total = jnp.concatenate(total, axis=0)
        for j in range(wide):
            away = lax.rem(me + j, groups) * part
            stack[pl.ds(j, folded * tp_size, stride=wide), :] = pltpu.roll(
                total, lax.rem(CLIP - away, CLIP), 1
            )
        dt_ref[...] = jnp.transpose(stack[...])[:part]

    def send_pieces():
        for r in range(moved, rounds + 1):
            hop(r)
        if direct:
            fold()
        beside = range(1, tp_size if direct else 1)
        for t in beside:
            piece_copy(0, t).start()
        for k in range(1, sp_size):
            piece_copy(lax.rem(me + k, sp_size), 0, k).start()
        for target in range(1, sp_size):
            for t in beside:
                piece_copy(target, t).start()

    for p in range(moved):
        halo(p)
        if p:
            local(p - 1)
    for p in range(moved, last):
        full(p)
        send_back(p)
        if p == moved:
            local(moved - 1)
    kept = []

    def finish_pieces():
        if moved == last:
            kept.extend(local_probs(moved - 1))
        send_pieces()

    full(last, finish_pieces)
    send_back(last)
    if kept:
        local_grads(moved - 1, *kept)

    def finish(p):
        cols = pl.ds(p * LANES, LANES)
        if p < moved:
            @pl.when(has_left)
            def _():
                if p == 0:
                    all_back().wait_recv()
                dq_ref[:, cols] = (own_q[p] + got_q[p].astype(F32)).astype(BF16)

            @pl.when(jnp.logical_not(has_left))
            def _():
                dq_ref[:, cols] = own_q[p].astype(BF16)
        else:
            i = p - moved

            @pl.when(has_right)
            def _():
                key_back_copy(p).wait_recv()
                dk_ref[:, cols] = (own_k[p] + got_kv[i, 0].astype(F32)).astype(BF16)
                dv_ref[:, cols] = (own_v[p] + got_kv[i, 1].astype(F32)).astype(BF16)

            @pl.when(jnp.logical_not(has_right))
            def _():
                dk_ref[:, cols] = own_k[p].astype(BF16)
                dv_ref[:, cols] = own_v[p].astype(BF16)

    if direct:
        for p in range(pairs):
            finish(p)
    all_pieces().wait_recv()
    if direct:
        unfold()
    else:
        total = pieces[me * part // CLIP]
        for k in range(1, sp_size):
            total = total + piece_got[k - 1]
        shares[0] = pltpu.roll(total, lax.rem(CLIP - lax.rem(me * part, CLIP), CLIP), 1)
        for k in range(1, tp_size):
            share_copy(k).start()
    if not direct:
        for p in range(pairs):
            finish(p)
        all_shares().wait_recv()
        stacked = jnp.concatenate(
            [shares[lax.rem(col + tp_size - t, tp_size)] for t in range(tp_size)], axis=0
        )
        dt_ref[...] = jnp.transpose(stacked)[:part]
        all_shares().wait_send()

    all_pieces().wait_send()

    @pl.when(has_left)
    def _():
        all_queries().wait_send()
        local_copy().wait_send()
        remote(back_kv, got_kv, LEFTWARD, misc_recv.at[0], left).wait_send()

    @pl.when(has_right)
    def _():
        all_keys().wait_send()
        remote(halo_stats, left_stats, RIGHTWARD, misc_recv.at[0], right).wait_send()
        all_back().wait_send()


def shards(sp_size, tp_size, query_rows, key_rows, value_rows, out_grad, rel_bias):
    rows, width = query_rows.shape
    pairs = width // LANES
    heads = width // HEAD_DIM
    part = 2 * CLIP // sp_size
    moved = pairs - 1
    rounds = (sp_size - 1).bit_length()
    direct = sp_size * tp_size <= 64 and part <= CLIP and heads % (CLIP // part) == 0
    folded = heads * part // CLIP
    exchange = [
        pltpu.VMEM(shape, F32)
        for shape in (
            (
                (sp_size, folded, CLIP),
                (sp_size * tp_size, folded, CLIP),
                (tp_size * heads, CLIP),
            )
            if direct
            else ((sp_size - 1, heads, CLIP), (tp_size, heads, CLIP), (8, CLIP))
        )
    ]
    assert rows == REACH and REACH == 2 * BLK and CLIP == BLK
    like = jax.ShapeDtypeStruct((rows, width), BF16)
    dma = pltpu.SemaphoreType.DMA
    shapes = (like, like, like, jax.ShapeDtypeStruct((part, heads * tp_size), F32))
    results = pl.pallas_call(
        partial(kernel, sp_size, tp_size, moved, direct),
        out_shape=shapes,
        in_specs=[pl.BlockSpec(memory_space=pltpu.HBM)] * 5,
        out_specs=tuple([pl.BlockSpec(memory_space=pltpu.VMEM)] * 4),
        scratch_shapes=[
            pltpu.VMEM((pairs, 2, rows, LANES), BF16),
            pltpu.VMEM((moved, 2, rows, LANES), BF16),
            pltpu.VMEM((pairs, 2, 2 * rows, LANES), BF16),
            pltpu.VMEM((pairs, BAND, 2 * BLK), F32),
            pltpu.VMEM((moved, REACH, 2 * BLK), F32),
            pltpu.VMEM((moved, BAND, 2 * BLK), F32),
            pltpu.VMEM((moved, BAND, 2 * BLK), F32),
            pltpu.VMEM((moved, 8, 2 * BLK), F32),
            pltpu.VMEM((pairs, rows, LANES), F32),
            pltpu.VMEM((pairs, rows, LANES), F32),
            pltpu.VMEM((moved, rows, LANES), F32),
            pltpu.VMEM((moved, rows, LANES), BF16),
            pltpu.VMEM((moved, rows, LANES), BF16),
            pltpu.VMEM((pairs - moved, 2, rows, LANES), BF16),
            pltpu.VMEM((pairs - moved, 2, rows, LANES), BF16),
            pltpu.VMEM((moved, 8, BLK), F32),
            pltpu.VMEM((moved, 8, BLK), F32),
            pltpu.VMEM((moved, 8, BLK), F32),
            pltpu.VMEM((moved, 8, BLK), F32),
            pltpu.VMEM(rel_bias.shape[::-1], F32),
            pltpu.VMEM((2, heads, BLK), F32),
            *exchange,
            dma((4,)),
            pltpu.SemaphoreType.REGULAR((rounds + 1,)),
            dma((2 * pairs - moved + 1,)),
            dma((1 + pairs - moved,)),
            dma((moved,)),
            dma((2 if direct else 3,)),
        ],
        compiler_params=pltpu.CompilerParams(
            collective_id=0, has_side_effects=True, vmem_limit_bytes=48 * 1024 * 1024
        ),
    )(*[pltpu.with_memory_space_constraint(x, pltpu.HBM) for x in (query_rows, key_rows, value_rows, out_grad, jnp.transpose(rel_bias))])
    return pl.pallas_call(
        write_out,
        out_shape=shapes,
        in_specs=[pl.BlockSpec(memory_space=pl.ANY)] * 4,
        out_specs=tuple([pl.BlockSpec(memory_space=pltpu.HBM)] * 4),
        scratch_shapes=[dma((4,))],
        compiler_params=pltpu.CompilerParams(vmem_limit_bytes=1024 * 1024),
    )(*results)


def write_out(*refs):
    sem = refs[-1]
    copies = [pltpu.make_async_copy(refs[i], refs[4 + i], sem.at[i]) for i in range(4)]
    for copy in copies:
        copy.start()
    for copy in copies:
        copy.wait()


def solution(mesh):
    return jax.shard_map(
        partial(shards, mesh.shape["sp"], mesh.shape["tp"]),
        mesh=mesh,
        in_specs=(P("sp", "tp"), P("sp", "tp"), P("sp", "tp"), P("sp", "tp"), P()),
        out_specs=(P("sp", "tp"), P("sp", "tp"), P("sp", "tp"), P("sp", None)),
        check_vma=False,
    )
```
